32 devices in a mesh: sp: 16 (over z, y, core), tp: 2 (over x).
Axes of the slice: x: 2, y: 2, z: 4, core: 2. Of those that a mesh axis runs over, the one named last changes fastest.
Arguments:
- queries: bfloat16 [8192, 1024], P('sp', 'tp'), may hold values from -160 to 160
- keys: bfloat16 [8192, 256], P('sp', 'tp'), may hold values from -5 to 5
- values: bfloat16 [8192, 256], P('sp', 'tp'), may hold values from -6 to 6
- doc_ids: int32 [8192], P('sp'), may hold values from 0 to 7, never falling along the last dimension, each value on 1 to 2048 neighbouring positions
- sink_logit: float32 [16], P('tp'), may hold values from 1 to 6
- w_out: bfloat16 [1024, 2048], P('tp'), may hold values from -0.1875 to 0.1875
- residual: bfloat16 [8192, 2048], P(('sp', 'tp')), may hold values from -6 to 6
- ffn_gain: float32 [2048], replicated, may hold values from 0.1 to 1.9
- expert_ids: int32 [8192, 8], P(('sp', 'tp')), may hold values from 0 to 15, all different within a row; in each aligned block of 128 rows (0 to 127, 128 to 255, ...) at most 96 rows name the same one
- expert_weight: float32 [8192, 8], P(('sp', 'tp')), may hold values from 0.2 to 2
- exp_gate: bfloat16 [16, 2048, 512], P('sp'), may hold values from -0.125 to 0.125
- exp_up: bfloat16 [16, 2048, 512], P('sp'), may hold values from -0.125 to 0.125
- exp_down: bfloat16 [16, 512, 2048], P('sp'), may hold values from -0.25 to 0.25
- shared_gate: bfloat16 [2048, 512], P(None, 'tp'), may hold values from -0.125 to 0.125
- shared_up: bfloat16 [2048, 512], P(None, 'tp'), may hold values from -0.125 to 0.125
- shared_down: bfloat16 [512, 2048], P('tp'), may hold values from -0.25 to 0.25
Outputs:
- output: bfloat16 [8192, 2048], P(('sp', 'tp'))
The draws below stay inside these ranges and needn't reach their ends.
Inputs may be any that keep to these rules, and one draw needn't show every extreme that they name: `doc_ids`: never falling along the sequence; every document holds at most 2048 positions, and one holds exactly that many. `expert_ids`: each row names 8 different experts. In each aligned block of 128 rows no expert is named by more than 96 rows, and in some blocks one expert is named by exactly 96 rows.
All inputs are finite; a program needn't handle non-finite values.
Results may differ from the reference program's by a relative error of at most 0.018.
Values may be sent and summed in bfloat16 or wider, within the bound.
A program may use at most 128 MiB of HBM per device.

```python
import math
import jax
import jax.numpy as jnp
import numpy as np
from jax import lax

D = 2048
HQ = 16
KV = 4
HD = 64
WINDOW = 128
FF = 512
SFF = 512
TOP_K = 8
TOK_DEV = 512
ATTN_W = 1024
TOKENS = 8192
HALF = 128
EXPERTS = 16
CAP = 96
DOCS = 8
N_TP = 2


def drawn_pair(key):
    base_keys = jnp.clip(jax.random.normal(jax.random.fold_in(key, 101), (TOKENS, KV, HD), jnp.float32), -5.0, 5.0)
    return base_keys


def draw_keys(key, part):
    base_keys = drawn_pair(key)
    result = base_keys
    return result.reshape(TOKENS, KV * HD).astype(jnp.bfloat16)


def draw_queries(key, part):
    drawn_rows = jnp.clip(jax.random.normal(jax.random.fold_in(key, 105), (TOKENS, HQ * HD), jnp.float32), -5.0, 5.0)
    result = drawn_rows
    return result.astype(jnp.bfloat16)


def block_scale(stream_key, extent, cuts, smallest, high):
    factor_of, own = 1.0, jax.random.fold_in(stream_key, 6)
    for axis_at, parts in cuts:
        heights = jnp.exp(jax.random.uniform(jax.random.fold_in(own, axis_at), (parts,), jnp.float32, smallest / len(cuts), high / len(cuts)))
        factor_of = factor_of * jnp.repeat(heights, extent[axis_at] // parts).reshape([-1 if axis == axis_at else 1 for axis in range(len(extent))])
    return factor_of


def split_up(count, total, bound, lean):
    loads = [(1 << 20) // math.isqrt(rank ** lean) + 1 for rank in range(2, count + 1)]
    rest, given = total - bound - (count - 1), [1] * (count - 1)
    while rest > 0:
        free = [i for i in range(count - 1) if given[i] < bound]
        whole, budget = sum([loads[i] for i in free]), rest
        for i in free:
            extra = min(bound - given[i], max(1, budget * loads[i] // whole), rest)
            given[i] = given[i] + extra
            rest = rest - extra
    return np.array([bound] + given)


def uneven_parts(rng, count, total, limit, lean):
    if count == 2:
        one = jax.random.randint(rng, (), max(1, total - limit), min(limit, total - 1) + 1)
        return jnp.stack([one, total - one])
    lengths = jnp.asarray(split_up(count, total, limit, lean), jnp.int32)
    pairs = (count - 1) // 2
    source_of, receiver = lengths[1:1 + 2 * pairs:2], lengths[2:2 + 2 * pairs:2]
    slack = jnp.minimum(source_of - 1, limit - receiver)
    moved = jax.random.randint(jax.random.fold_in(rng, 1), (pairs,), 0, 1 << 20) % (slack + 1)
    lengths = lengths.at[1:1 + 2 * pairs:2].set(source_of - moved).at[2:2 + 2 * pairs:2].set(receiver + moved)
    return lengths[jax.random.permutation(jax.random.fold_in(rng, 2), count)]


def routed_block(key, own, number, rows, number_of, top, bound, lean):
    ranking = jax.random.permutation(key, number_of)
    packed, common = shares(number_of, rows * top, bound, lean, True), shares(number_of, rows * top, bound, lean, False)
    places = jnp.arange(number_of)

    def named(sizes, turn):
        used = int((sizes > 0).sum())
        fixed = max(1, used // 4)
        passed = fixed + (places - fixed + turn * (used - fixed)) % max(1, number_of - fixed)
        return jnp.zeros((number_of,), jnp.int32).at[ranking[jnp.where(places < fixed, places, passed)]].set(jnp.asarray(sizes, jnp.int32))

    sizes = jnp.where(number % 4 == 0, named(packed, number // 4), named(common, number - number // 4 - 1))
    mixed = jax.random.permutation(jax.random.fold_in(own, 3), number_of)
    donor, sink = mixed[0:number_of // 2 * 2:2], mixed[1:number_of // 2 * 2:2]
    room = jnp.minimum(sizes[donor] - 1, bound - sizes[sink]) // 2
    room = jnp.where((donor == ranking[0]) | (sink == ranking[0]) | (sizes[sink] == 0), 0, jnp.maximum(room, 0))
    passed = jax.random.randint(jax.random.fold_in(own, 4), (number_of // 2,), 0, 1 << 20) % (room + 1)
    sizes = sizes.at[donor].add(-passed).at[sink].add(passed)
    members = jnp.searchsorted(jnp.cumsum(sizes), jnp.arange(rows * top), side="right").astype(jnp.int32)
    listing = members.reshape(top, rows).T
    listing = listing[jax.random.permutation(jax.random.fold_in(own, 1), rows)]
    turn = jax.random.randint(jax.random.fold_in(own, 2), (rows, 1), 0, top)
    return jnp.take_along_axis(listing, (jnp.arange(top)[None, :] + turn) % top, axis=1)


def shares(amount, total, reach, skew, full):
    weights = [(1 << 20) // math.isqrt(grade ** skew) + 1 for grade in range(1, amount + 1)]
    largest = reach if full else min(reach, max(-(-total // amount), total * weights[0] // sum(weights)))
    least = 1 if total - largest >= amount - 1 else 0
    given, surplus = [largest] + [least] * (amount - 1), total - largest - least * (amount - 1)
    while surplus > 0:
        candidates = [i for i in range(1, amount) if given[i] < largest] or [i for i in range(1, amount) if given[i] < reach]
        pool, budget = sum([weights[i] for i in candidates]), surplus
        for i in candidates:
            more = min(reach - given[i], max(1, budget * weights[i] // pool), surplus)
            given[i] = given[i] + more
            surplus = surplus - more
    return np.array(given)


def centred(key, extent, deviation, limit, shards=(), kind=jnp.bfloat16):
    values = deviation * jax.random.normal(key, extent, jnp.float32)
    if shards:
        values = values * block_scale(key, extent, shards, -0.22, 0.18)
    return jnp.clip(values, -limit, limit).astype(kind)


def setup_inputs(seed: int = 0) -> dict:
    splits = jax.random.split(jax.random.key(seed), 17)
    queries = draw_queries(jax.random.fold_in(splits[16], 71), 0)
    keys = draw_keys(jax.random.fold_in(splits[16], 71), 0)
    values = centred(splits[2], (TOKENS, KV * HD), 1.0, 6.0, ((0, 16), (1, 2)))
    doc_ids = jnp.searchsorted(jnp.cumsum(uneven_parts(splits[3], DOCS, TOKENS, 4 * TOK_DEV, 2)), jnp.arange(TOKENS), side="right").astype(jnp.int32)
    sink_logit = jnp.clip(1.0 + 5.0 * jax.random.uniform(splits[4], (HQ,), jnp.float32) ** block_scale(splits[4], (HQ,), ((0, 2),), -0.2, 0.2), 1.0, 6.0)
    w_out = centred(splits[5], (ATTN_W, D), ATTN_W ** -0.5, 0.1875, ((0, 2),))
    residual = centred(splits[6], (TOKENS, D), 1.0, 6.0, ((0, 32),))
    ffn_gain = jnp.clip(1.0 + 0.18 * jax.random.normal(splits[7], (D,), jnp.float32), 0.1, 1.9)
    expert_ids_keys = jax.random.split(jax.random.fold_in(splits[8], 1), TOKENS // HALF)
    expert_ids_turns = jax.random.permutation(jax.random.fold_in(splits[8], 3), TOKENS // HALF)
    expert_ids = jax.vmap(lambda own, number: routed_block(jax.random.fold_in(splits[8], 2), own, number, HALF, EXPERTS, TOP_K, CAP, 2))(expert_ids_keys, expert_ids_turns).reshape((TOKENS, TOP_K))
    expert_weight = jnp.clip(jnp.exp(math.log(2.0) - 2.3025851 * jax.random.uniform(splits[9], (TOKENS, TOP_K), jnp.float32) ** block_scale(splits[9], (TOKENS, TOP_K), ((0, 32),), -0.2, 0.2)), 0.2, 2.0)
    exp_gate = centred(splits[10], (EXPERTS, D, FF), D ** -0.5, 0.125, ((0, 16),))
    exp_up = centred(splits[11], (EXPERTS, D, FF), D ** -0.5, 0.125, ((0, 16),))
    exp_down = centred(splits[12], (EXPERTS, FF, D), FF ** -0.5, 0.25, ((0, 16),))
    shared_gate = centred(splits[13], (D, SFF), D ** -0.5, 0.125, ((1, 2),))
    shared_up = centred(splits[14], (D, SFF), D ** -0.5, 0.125, ((1, 2),))
    shared_down = centred(splits[15], (SFF, D), SFF ** -0.5, 0.25, ((0, 2),))
    return dict(queries=queries, keys=keys, values=values, doc_ids=doc_ids, sink_logit=sink_logit, w_out=w_out, residual=residual, ffn_gain=ffn_gain, expert_ids=expert_ids, expert_weight=expert_weight, exp_gate=exp_gate, exp_up=exp_up, exp_down=exp_down, shared_gate=shared_gate, shared_up=shared_up, shared_down=shared_down)


norm_eps = 1e-06

def band_blocks(padded, width):
    span_count = padded.shape[0] // width - 2
    shaped = padded.reshape((span_count + 2, width) + padded.shape[1:])
    return jnp.concatenate([shaped[0:span_count:2], shaped[1:span_count + 1:2], shaped[2:span_count + 2:2], shaped[3:span_count + 3:2]], axis=1)

def reference(queries, keys, values, doc_ids, sink_logit, w_out, residual, ffn_gain, expert_ids, expert_weight, exp_gate, exp_up, exp_down, shared_gate, shared_up, shared_down):
    group_size = HQ // KV
    query_span = 2 * WINDOW
    block_count = TOKENS // query_span
    pad_rows = ((WINDOW, WINDOW), (0, 0))
    key_blocks = band_blocks(jnp.pad(keys, pad_rows), WINDOW).reshape(block_count, 4 * WINDOW, KV, HD)
    value_blocks = band_blocks(jnp.pad(values, pad_rows), WINDOW).reshape(block_count, 4 * WINDOW, KV, HD)
    marks = (doc_ids + 1).astype(jnp.int32)
    mark_blocks = band_blocks(jnp.pad(marks, (WINDOW, WINDOW)), WINDOW)
    query_blocks = queries.reshape(block_count, query_span, KV, group_size, HD)
    query_marks = marks.reshape(block_count, query_span)
    offset = jnp.arange(query_span, dtype=jnp.int32)[:, None] - jnp.arange(4 * WINDOW, dtype=jnp.int32)[None, :] + WINDOW
    near = jnp.abs(offset) <= WINDOW
    sink_term = sink_logit.astype(jnp.float32).reshape(KV, group_size)[:, :, None, None]

    def attend_block(inputs):
        query_in, key_in, value_in, key_marks, row_marks = inputs
        scores = jnp.einsum('qkgd,mkd->kgqm', query_in.astype(jnp.float32), key_in.astype(jnp.float32)) * HD ** (-0.5)
        allowed = near & (key_marks[None, :] == row_marks[:, None])
        scores = jnp.where(allowed[None, None], scores, -jnp.inf)
        row_max = jnp.maximum(lax.optimization_barrier(jnp.max(scores, axis=-1, keepdims=True)), sink_term)
        exp_scores = jnp.exp(scores - row_max)
        attn_probs = (exp_scores / (lax.optimization_barrier(jnp.sum(exp_scores, axis=-1, keepdims=True)) + jnp.exp(sink_term - row_max))).astype(jnp.bfloat16)
        result = jnp.einsum('kgqm,mkd->qkgd', attn_probs.astype(jnp.float32), value_in.astype(jnp.float32))
        return result.astype(jnp.bfloat16).reshape(query_span, HQ * HD)
    attended = lax.map(attend_block, (query_blocks, key_blocks, value_blocks, mark_blocks, query_marks)).reshape(TOKENS, HQ * HD)
    mixed = jnp.dot(attended, w_out, preferred_element_type=jnp.float32)
    resid = (residual.astype(jnp.float32) + mixed).astype(jnp.bfloat16)
    resid_f = resid.astype(jnp.float32)
    normed = (resid_f * lax.rsqrt(lax.optimization_barrier(jnp.mean(resid_f * resid_f, axis=-1, keepdims=True)) + norm_eps) * ffn_gain.astype(jnp.float32)).astype(jnp.bfloat16)
    shared_hidden = (jax.nn.silu(jnp.dot(normed, shared_gate, preferred_element_type=jnp.float32)) * jnp.dot(normed, shared_up, preferred_element_type=jnp.float32)).astype(jnp.bfloat16)
    block_units = SFF // N_TP
    shared_out = jnp.zeros((TOKENS, D), jnp.float32)
    for unit_block in range(N_TP):
        lower = unit_block * block_units
        partial_out = jnp.dot(shared_hidden[:, lower:lower + block_units], shared_down[lower:lower + block_units], preferred_element_type=jnp.float32)
        shared_out = shared_out + lax.optimization_barrier(partial_out.astype(jnp.bfloat16)).astype(jnp.float32)
    assign_count = TOKENS * TOP_K
    row_block = 512
    flat_ids = expert_ids.reshape(assign_count).astype(jnp.int32)
    order = jnp.argsort(flat_ids, stable=True).astype(jnp.int32)
    sorted_ids = flat_ids[order]
    counts = jnp.bincount(flat_ids, length=EXPERTS).astype(jnp.int32)
    starts = (jnp.cumsum(counts) - counts).astype(jnp.int32)
    padded = ((counts + row_block - 1) // row_block * row_block).astype(jnp.int32)
    ends = jnp.cumsum(padded).astype(jnp.int32)
    pad_starts = (ends - padded).astype(jnp.int32)
    dest = (pad_starts[sorted_ids] + jnp.arange(assign_count, dtype=jnp.int32) - starts[sorted_ids]).astype(jnp.int32)
    block_total = -(-assign_count // row_block) + EXPERTS
    row_source = jnp.full((block_total * row_block,), assign_count, jnp.int32).at[dest].set(order)
    block_expert = jnp.minimum(jnp.searchsorted(ends, jnp.arange(block_total, dtype=jnp.int32) * row_block, side='right'), EXPERTS - 1).astype(jnp.int32)
    flat_weight = expert_weight.reshape(assign_count).astype(jnp.float32)

    def expert_step(running, inputs):
        sources, expert_index = inputs
        live = sources < assign_count
        safe = jnp.minimum(sources, assign_count - 1)
        token_rows = (safe // TOP_K).astype(jnp.int32)
        gathered = normed[token_rows]
        hidden = (jax.nn.silu(jnp.dot(gathered, exp_gate[expert_index], preferred_element_type=jnp.float32)) * jnp.dot(gathered, exp_up[expert_index], preferred_element_type=jnp.float32)).astype(jnp.bfloat16)
        produced = jnp.dot(hidden, exp_down[expert_index], preferred_element_type=jnp.float32).astype(jnp.bfloat16)
        scale = jnp.where(live, flat_weight[safe], jnp.zeros_like(flat_weight[safe]))
        return (running.at[token_rows].add(scale[:, None] * produced.astype(jnp.float32)), None)
    routed, _ = lax.scan(expert_step, jnp.zeros((TOKENS, D), jnp.float32), (row_source.reshape(block_total, row_block), block_expert))
    return (resid.astype(jnp.float32) + shared_out + routed).astype(jnp.bfloat16)
```

```python
import math

import jax
import jax.numpy as jnp
from jax import lax
from jax.experimental import pallas as pl
from jax.experimental.pallas import tpu as pltpu
from jax.sharding import PartitionSpec as P

HD = 64
WINDOW = 128
PARTS = 2


norm_eps = 1e-06


def extended(cells, sides, width):
    for axis, dim in sides:
        count = lax.axis_size(axis)
        ends = count - 1
        head = lax.slice_in_dim(cells, 0, width, axis=dim)
        tail = lax.slice_in_dim(cells, cells.shape[dim] - width, cells.shape[dim], axis=dim)
        cells = jnp.concatenate(
            [
                lax.ppermute(tail, axis, [(i, (i + 1) % count) for i in range(ends)]),
                cells,
                lax.ppermute(head, axis, [((i + 1) % count, i) for i in range(ends)]),
            ],
            axis=dim,
        )
    return cells


def band_blocks(padded, width):
    span_count = padded.shape[0] // width - 2
    shaped = padded.reshape((span_count + 2, width) + padded.shape[1:])
    return jnp.concatenate(
        [
            shaped[0:span_count:2],
            shaped[1 : span_count + 1 : 2],
            shaped[2 : span_count + 2 : 2],
            shaped[3 : span_count + 3 : 2],
        ],
        axis=1,
    )


def attend(queries, ext_keys, ext_values, ext_marks, own_marks, sink_logit):
    tok_count = queries.shape[0]
    head_count = sink_logit.shape[0]
    key_heads = ext_keys.shape[1] // HD
    group_size = head_count // key_heads
    query_span = 2 * WINDOW
    block_count = tok_count // query_span
    query_blocks = queries.reshape(block_count, query_span, key_heads, group_size, HD)
    key_blocks = band_blocks(ext_keys, WINDOW).reshape(block_count, 4 * WINDOW, key_heads, HD)
    value_blocks = band_blocks(ext_values, WINDOW).reshape(block_count, 4 * WINDOW, key_heads, HD)
    mark_blocks = band_blocks(ext_marks, WINDOW)
    query_marks = own_marks.reshape(block_count, query_span)
    scores = jnp.einsum(
        "nqkgd,nmkd->nkgqm", query_blocks, key_blocks, preferred_element_type=jnp.float32
    ) * HD ** (-0.5)
    offset = (
        jnp.arange(query_span, dtype=jnp.int32)[:, None]
        - jnp.arange(4 * WINDOW, dtype=jnp.int32)[None, :]
        + WINDOW
    )
    allowed = (jnp.abs(offset) <= WINDOW)[None] & (
        mark_blocks[:, None, :] == query_marks[:, :, None]
    )
    scores = jnp.where(allowed[:, None, None], scores, -jnp.inf)
    sink_term = sink_logit.reshape(key_heads, group_size)[None, :, :, None, None]
    row_max = jnp.maximum(jnp.max(scores, axis=-1, keepdims=True), sink_term)
    exp_scores = jnp.exp(scores - row_max)
    attn_probs = (
        exp_scores / (jnp.sum(exp_scores, axis=-1, keepdims=True) + jnp.exp(sink_term - row_max))
    ).astype(jnp.bfloat16)
    result = jnp.einsum(
        "nkgqm,nmkd->nqkgd", attn_probs, value_blocks, preferred_element_type=jnp.float32
    )
    return result.astype(jnp.bfloat16).reshape(tok_count, head_count * HD)


def expert_kernel(rows_ref, scale_ref, gate_ref, up_ref, down_ref, side_ref, side_down_ref, out_ref):
    rows = rows_ref[...]
    gated = jnp.dot(rows, gate_ref[...], preferred_element_type=jnp.float32)
    lifted = jnp.dot(rows, up_ref[...], preferred_element_type=jnp.float32)
    hidden = (gated / (1.0 + jnp.exp(-gated)) * lifted).astype(jnp.bfloat16)
    produced = jnp.dot(hidden, down_ref[...], preferred_element_type=jnp.float32)
    side = jnp.dot(rows, side_ref[...], preferred_element_type=jnp.float32)
    width = side.shape[1] // 2
    side_gate, side_up = side[:, :width], side[:, width:]
    side_hidden = (side_gate / (1.0 + jnp.exp(-side_gate)) * side_up).astype(jnp.bfloat16)
    shared = jnp.dot(side_hidden, side_down_ref[...], preferred_element_type=jnp.float32)
    out_ref[...] = (
        scale_ref[...] * produced.astype(jnp.bfloat16).astype(jnp.float32) + shared
    ).astype(jnp.bfloat16)


def run_experts(rows, scale, gate_w, up_w, down_w, side_w, side_down):
    count, width = rows.shape
    tile = math.gcd(count, 256)
    whole = lambda w: pl.BlockSpec(w.shape, lambda i: (0, 0))
    units = gate_w.shape[1] + side_w.shape[1] // 2
    return pl.pallas_call(
        expert_kernel,
        grid=(count // tile,),
        in_specs=[
            pl.BlockSpec((tile, width), lambda i: (i, 0)),
            pl.BlockSpec((tile, 1), lambda i: (i, 0)),
            whole(gate_w),
            whole(up_w),
            whole(down_w),
            whole(side_w),
            whole(side_down),
        ],
        out_specs=pl.BlockSpec((tile, width), lambda i: (i, 0)),
        out_shape=jax.ShapeDtypeStruct((count, width), jnp.bfloat16),
        compiler_params=pltpu.CompilerParams(
            dimension_semantics=("arbitrary",), vmem_limit_bytes=48 * 1024 * 1024
        ),
        cost_estimate=pl.CostEstimate(
            flops=6 * count * width * units,
            bytes_accessed=4 * count * width + 6 * units * width,
            transcendentals=count * units,
        ),
    )(rows, scale, gate_w, up_w, down_w, side_w, side_down)


def shared_slice(shared_gate, shared_up, shared_down):
    sp_count, tp_count = lax.axis_size("sp"), lax.axis_size("tp")
    own, side = lax.axis_index("tp"), lax.axis_index("sp")
    units = shared_gate.shape[1] * tp_count // sp_count
    per_owner = sp_count // tp_count
    owner, offset = side // per_owner, (side % per_owner) * units
    held = jnp.concatenate(
        [
            lax.dynamic_slice_in_dim(shared_gate, offset, units, axis=1).T,
            lax.dynamic_slice_in_dim(shared_up, offset, units, axis=1).T,
            lax.dynamic_slice_in_dim(shared_down, offset, units, axis=0),
        ],
        axis=0,
    )
    chosen = held
    for shift in range(1, tp_count):
        came = lax.ppermute(held, "tp", [(i, (i + shift) % tp_count) for i in range(tp_count)])
        chosen = jnp.where((own - shift) % tp_count == owner, came, chosen)
    padded = -(-units // 128) * 128
    grown = [
        jnp.pad(chosen[i * units : (i + 1) * units], ((0, padded - units), (0, 0))) for i in range(3)
    ]
    return jnp.concatenate(grown[:2], axis=0).T, grown[2]


def shards(
    queries,
    keys,
    values,
    doc_ids,
    sink_logit,
    w_out,
    residual,
    ffn_gain,
    expert_ids,
    expert_weight,
    exp_gate,
    exp_up,
    exp_down,
    shared_gate,
    shared_up,
    shared_down,
):
    marks = (doc_ids + 1).astype(jnp.bfloat16)
    kv = keys.shape[1]
    joined = jnp.concatenate(
        [keys, values, jnp.broadcast_to(marks[:, None], (marks.shape[0], 128))], axis=1
    )
    extended_all = extended(joined, (("sp", 0),), WINDOW)
    ext_keys, ext_values, ext_marks = (
        extended_all[:, :kv],
        extended_all[:, kv : 2 * kv],
        extended_all[:, 2 * kv],
    )
    attended = attend(queries, ext_keys, ext_values, ext_marks, marks, sink_logit)
    row_count = residual.shape[0]
    mixed = lax.psum_scatter(
        jnp.dot(attended, w_out, preferred_element_type=jnp.float32).astype(jnp.bfloat16),
        "tp",
        scatter_dimension=0,
        tiled=True,
    ).astype(jnp.float32)
    resid = (residual.astype(jnp.float32) + mixed).astype(jnp.bfloat16)
    resid_f = resid.astype(jnp.float32)
    normed = (
        resid_f
        * lax.rsqrt(jnp.mean(resid_f * resid_f, axis=-1, keepdims=True) + norm_eps)
        * ffn_gain
    ).astype(jnp.bfloat16)
    side_w, side_down = shared_slice(shared_gate, shared_up, shared_down)
    sp_count = lax.axis_size("sp")
    chosen = expert_ids[:, :, None] == jnp.arange(sp_count, dtype=jnp.int32)
    table = jnp.sum(jnp.where(chosen, expert_weight[:, :, None], 0.0), axis=1)
    scales = lax.all_to_all(table.T, "sp", split_axis=0, concat_axis=0, tiled=True)
    part_rows = row_count // PARTS
    sums = []
    for part in range(PARTS):
        begin = part * part_rows
        gathered = lax.all_gather(normed[begin : begin + part_rows], "sp", axis=0, tiled=True)
        scale = scales[:, begin : begin + part_rows].reshape(-1, 1)
        produced = run_experts(
            gathered, scale, exp_gate[0], exp_up[0], exp_down[0], side_w, side_down
        )
        sums.append(lax.psum_scatter(produced, "sp", scatter_dimension=0, tiled=True))
    added = jnp.concatenate(sums, axis=0)
    return (resid.astype(jnp.float32) + added.astype(jnp.float32)).astype(jnp.bfloat16)


MESH = pl.DeviceIdType.MESH
QB = 128
NEG = -1e30
LINE = 4


def layer_kernel(
    tab_in, marks_in, sink_ref, q_in, k_in, v_in, wo_in, res_in, gain_ref,
    eg_in, eu_in, ed_in, sg_in, su_in, sd_in,
    out_ref,
    q_s, kx, vx, marks, kk, vv, a_out, a_own, a_in, wo_own, wo_oth, res, tok, tab, tabt,
    gs, us, ds, hid, acc, stage, rbuf, sg, su, sd, sh, ost,
    loc, halo_s, halo_r, tab_s, tab_r, wo_s, wo_r, att_s, att_r,
    sib_s, sib_r, y_s, y_r, x_s, x_r, fy_s, fy_r, fx_s, fx_r,
    ag_s, ag_r, rs_s, rs_r, sx_s, sx_r, ss_s, ss_r, out_sem,
):
    f32, bf16 = jnp.float32, jnp.bfloat16
    sp_count, tp_count = lax.axis_size("sp"), lax.axis_size("tp")
    s, x = lax.axis_index("sp"), lax.axis_index("tp")
    z, y, c = s // 4, lax.rem(s // 2, 2), lax.rem(s, 2)
    ox, oy, oc = 1 - x, 1 - y, 1 - c
    at = lambda zz, yy, cc: (zz * 2 + yy) * 2 + cc
    dev = lambda sp, tp: {"sp": sp, "tp": tp}
    sib, ypar, xpar = dev(at(z, y, oc), x), dev(at(z, oy, c), x), dev(s, ox)
    nxt, prv = dev(lax.rem(s + 1, sp_count), x), dev(lax.rem(s + sp_count - 1, sp_count), x)
    low = z < 2
    w = jnp.where(low, z, 3 - z)
    inner = w == 1
    zf = jnp.where(low, z + 1, z - 1)
    zb = jnp.clip(jnp.where(low, z - 1, z + 1), 0, 3)
    fwd, bck = dev(at(zf, y, c), x), dev(at(zb, y, c), x)
    line = lambda ob: jnp.where(low, ob, 3 - ob)
    tokens = q_in.shape[0]
    half = tokens // 2
    width = res_in.shape[1]
    ff = eg_in.shape[2]
    part = width // 4

    def send(src, dst, ss, rs, to):
        cp = pltpu.make_async_remote_copy(
            src_ref=src, dst_ref=dst, send_sem=ss, recv_sem=rs, device_id=to, device_id_type=MESH
        )
        cp.start()
        return cp

    def got(view, rs):
        pltpu.make_async_remote_copy(
            src_ref=view, dst_ref=view, send_sem=rs, recv_sem=rs, device_id=sib, device_id_type=MESH
        ).wait_recv()

    def sent(view, ss):
        pltpu.make_async_remote_copy(
            src_ref=view, dst_ref=view, send_sem=ss, recv_sem=ss, device_id=sib, device_id_type=MESH
        ).wait_send()

    def load(src, dst, sem):
        cp = pltpu.make_async_copy(src, dst, sem)
        cp.start()
        return cp

    rows_own = pl.ds(QB, tokens)
    loads_a = [
        load(q_in, q_s, loc.at[0]),
        load(k_in, kx.at[rows_own], loc.at[1]),
        load(v_in, vx.at[rows_own], loc.at[2]),
        load(marks_in, marks.at[pl.ds(1, tokens // QB)], loc.at[3]),
    ]
    loads_b = [
        load(wo_in, wo_own, loc.at[4]),
        load(res_in, res, loc.at[5]),
        load(tab_in, tab.at[z], loc.at[6]),
        load(eg_in.at[0], gs.at[0], loc.at[7]),
        load(eu_in.at[0], us.at[0], loc.at[8]),
        load(sg_in, sg.at[0], loc.at[9]),
        load(su_in, su.at[0], loc.at[10]),
        load(sd_in, sd.at[pl.ds(0, sd_in.shape[0])], loc.at[11]),
    ]
    for n in range(4):
        loads_b.append(
            load(ed_in.at[0, :, pl.ds(n * part, part)], ds.at[n, pl.ds(0, ff)], loc.at[12 + n])
        )

    barrier = pltpu.get_barrier_semaphore()
    zs = [lax.rem(z + i, LINE) for i in range(1, LINE)]
    partners = [nxt, prv, sib, ypar, xpar] + [dev(at(zz, y, c), x) for zz in zs]
    for to in partners:
        pl.semaphore_signal(barrier, inc=1, device_id=to, device_id_type=MESH)
    pl.semaphore_wait(barrier, len(partners))

    pend = []
    last, first = pl.ds(tokens - QB, QB), pl.ds(0, QB)
    after = pl.ds(QB + tokens, QB)
    nb = tokens // QB
    for i, (src, dst, lo, hi, a, b) in enumerate(
        [(k_in, kx, first, after, last, first), (v_in, vx, first, after, last, first)]
    ):
        pend.append(send(src.at[a], dst.at[lo], halo_s.at[2 * i], halo_r.at[2 * i], nxt))
        pend.append(send(src.at[b], dst.at[hi], halo_s.at[2 * i + 1], halo_r.at[2 * i + 1], prv))
    pend.append(send(marks_in.at[nb - 1], marks.at[0], halo_s.at[4], halo_r.at[4], nxt))
    pend.append(send(marks_in.at[0], marks.at[nb + 1], halo_s.at[5], halo_r.at[5], prv))
    for i, zz in enumerate(zs):
        pend.append(send(tab_in, tab.at[z], tab_s.at[i], tab_r.at[LINE - 2 - i], dev(at(zz, y, c), x)))

    wrows = wo_in.shape[0] // 2
    wmine, woth = pl.ds(c * wrows, wrows), pl.ds(oc * wrows, wrows)
    pend.append(send(wo_in.at[wmine], wo_oth.at[wmine], wo_s.at[0], wo_r.at[0], xpar))

    quarter = width // 4

    def piece(refs, kind, i, slot):
        g, u, d = refs
        if kind == "g":
            return g.at[slot, pl.ds(i * quarter, quarter)]
        if kind == "u":
            return u.at[slot, pl.ds(i * quarter, quarter)]
        if slot is None:
            return d.at[0, :, pl.ds(i * part, part)]
        return d.at[i, pl.ds(slot * ff, ff)]

    def hbm_piece(kind, i):
        if kind == "g":
            return eg_in.at[0, pl.ds(i * quarter, quarter)]
        if kind == "u":
            return eu_in.at[0, pl.ds(i * quarter, quarter)]
        return ed_in.at[0, :, pl.ds(pl.multiple_of(i * part, part), part)]

    held = (gs, us, ds)
    own_only = lambda v: [("g", 2 * v), ("g", 2 * v + 1), ("u", v), ("d", v), ("d", 2 + v)]
    y_list = own_only(x)[:3] + [("u", 2), ("u", 3)] + own_only(x)[3:]
    x_list = own_only(ox)
    y_to_x = {0: 0, 1: 1, 2: 2, 5: 3, 6: 4}
    for i, (kind, j) in enumerate(y_list):
        pend.append(send(hbm_piece(kind, j), piece(held, kind, j, 2), y_s.at[i], y_r.at[i], ypar))
    pend.append(send(eg_in.at[0], gs.at[1], sib_s.at[0], sib_r.at[0], sib))
    pend.append(send(eu_in.at[0], us.at[1], sib_s.at[1], sib_r.at[1], sib))
    for n in range(4):
        pend.append(
            send(hbm_piece("d", n), piece(held, "d", n, 1), sib_s.at[2 + n], sib_r.at[2 + n], sib)
        )

    def y_event(i):
        kind, j = y_list[i]
        view = piece(held, kind, j, 2)
        got(view, y_r.at[i])
        if i in y_to_x:
            pend.append(send(view, view, x_s.at[y_to_x[i]], x_r.at[y_to_x[i]], xpar))
        pend.append(send(view, piece(held, kind, j, 3), fy_s.at[i], fy_r.at[i], sib))

    def x_event(i):
        kind, j = x_list[i]
        view = piece(held, kind, j, 2)
        got(view, x_r.at[i])
        pend.append(send(view, piece(held, kind, j, 3), fx_s.at[i], fx_r.at[i], sib))

    for cp in loads_a:
        cp.wait()
    for i in range(2):
        dst = (kx, vx)[i]
        got(dst.at[first], halo_r.at[2 * i])
        got(dst.at[after], halo_r.at[2 * i + 1])
    got(marks.at[0], halo_r.at[4])
    got(marks.at[nb + 1], halo_r.at[5])

    @pl.when(s == 0)
    def _():
        marks[0] = jnp.full(marks.shape[1:], -1, jnp.int32)

    @pl.when(s == sp_count - 1)
    def _():
        marks[nb + 1] = jnp.full(marks.shape[1:], -1, jnp.int32)

    ri = lax.broadcasted_iota(jnp.int32, (QB, QB), 0)
    ci = lax.broadcasted_iota(jnp.int32, (QB, QB), 1)
    swap = jnp.where(ci == lax.rem(ri + HD, QB), 1.0, 0.0).astype(bf16)

    def spread(t, carry):
        rows = pl.ds(pl.multiple_of(t * QB, QB), QB)
        for src, dst in ((kx, kk), (vx, vv)):
            cur = src[rows]
            turned = jnp.dot(cur, swap, preferred_element_type=f32)
            cur = cur.astype(f32)
            zero = jnp.zeros_like(cur)
            left = ci < HD
            dst[0, rows] = jnp.where(left, cur, zero).astype(bf16)
            dst[1, rows] = jnp.where(left, zero, turned).astype(bf16)
            dst[2, rows] = jnp.where(left, turned, zero).astype(bf16)
            dst[3, rows] = jnp.where(left, zero, cur).astype(bf16)
        return carry

    lax.fori_loop(0, nb + 2, spread, 0)

    def attend_rows(blk, dst, drow):
        rows = pl.ds(pl.multiple_of(blk * QB, QB), QB)
        span = pl.ds(pl.multiple_of(blk * QB, QB), 3 * QB)
        mine = jnp.broadcast_to(marks[blk + 1][0:1], (QB, QB)).T
        biases = []
        for t in range(3):
            same = mine == jnp.broadcast_to(marks[blk + t][0:1], (QB, QB))
            if t == 0:
                same = same & (ri <= ci)
            if t == 2:
                same = same & (ci <= ri)
            biases.append(jnp.where(same, 0.0, NEG).astype(f32))
        bias = jnp.concatenate(biases, axis=1)
        for j in range(q_s.shape[1] // QB):
            g = j // 2
            keys2 = jnp.concatenate([kk[2 * g, span], kk[2 * g + 1, span]], axis=0)
            vals2 = jnp.concatenate([vv[2 * g, span], vv[2 * g + 1, span]], axis=0)
            sc = lax.dot_general(
                q_s[rows, j * QB : (j + 1) * QB], keys2, (((1,), (1,)), ((), ())),
                preferred_element_type=f32,
            ) * HD ** (-0.5)
            probs = []
            for h in range(2):
                sink = sink_ref[2 * j + h]
                own = sc[:, h * 3 * QB : (h + 1) * 3 * QB] + bias
                top = jnp.maximum(jnp.max(own, axis=-1, keepdims=True), sink)
                e = jnp.exp(own - top)
                total = jnp.sum(e, axis=-1, keepdims=True) + jnp.exp(sink - top)
                probs.append((e * (1.0 / total)).astype(bf16))
            o = jnp.dot(jnp.concatenate(probs, axis=1), vals2, preferred_element_type=f32)
            dst[pl.ds(pl.multiple_of(drow, QB), QB), j * QB : (j + 1) * QB] = o.astype(bf16)

    hb = half // QB

    def other_rows(i, carry):
        attend_rows(ox * hb + i, a_out, i * QB)
        piece_rows = pl.ds(pl.multiple_of(i * QB, QB), QB)
        send(a_out.at[piece_rows], a_in.at[piece_rows], att_s.at[i], att_r.at[i], xpar)
        return carry

    lax.fori_loop(0, hb, other_rows, 0)

    def own_rows(i, carry):
        attend_rows(x * hb + i, a_own, i * QB)
        return carry

    lax.fori_loop(0, hb, own_rows, 0)

    for cp in loads_b:
        cp.wait()
    y_event(0)
    got(wo_oth.at[wmine], wo_r.at[0])
    pend.append(send(wo_oth.at[wmine], wo_oth.at[wmine], wo_s.at[1], wo_r.at[1], sib))
    for i in range(hb):
        got(a_in.at[pl.ds(i * QB, QB)], att_r.at[i])
    got(wo_oth.at[woth], wo_r.at[1])
    square = jnp.zeros((half, 1), f32)
    for n in range(4):
        cols = slice(n * part, (n + 1) * part)
        mixed = jnp.dot(a_own[...], wo_own[:, cols], preferred_element_type=f32)
        mixed = mixed + jnp.dot(a_in[...], wo_oth[:, cols], preferred_element_type=f32)
        r = (res[:, cols].astype(f32) + mixed).astype(bf16)
        res[:, cols] = r
        rf = r.astype(f32)
        square = square + jnp.sum(rf * rf, axis=-1, keepdims=True)
    inv = lax.rsqrt(square * (1.0 / width) + norm_eps)
    for n in range(4):
        cols = slice(n * part, (n + 1) * part)
        tok[z, :, cols] = (res[:, cols].astype(f32) * inv * gain_ref[:, cols]).astype(bf16)

    hr = half // 2
    rows_of = lambda r: pl.ds(r * hr, hr)

    def ag_send(b, r, direction, to):
        view = tok.at[b, rows_of(r)]
        send(view, view, ag_s.at[direction, b, r], ag_r.at[b, r], to)

    def ag_sent(b, r, direction):
        sent(tok.at[b, rows_of(r)], ag_s.at[direction, b, r])

    def ag_got(b, r):
        got(tok.at[b, rows_of(r)], ag_r.at[b, r])

    for r in range(2):
        ag_send(z, r, 0, fwd)

        @pl.when(inner)
        def _():
            ag_send(z, r, 1, bck)

    def relay(ob, r):
        b = line(ob)

        @pl.when(inner)
        def _():
            ag_got(b, r)
            if ob == 0:
                ag_send(b, r, 0, fwd)
            else:
                ag_send(b, r, 1, bck)

    def table_columns(b, carry):
        t = tab[b]
        grown = jnp.concatenate([t, jnp.zeros((QB - t.shape[0], t.shape[1]), f32)], axis=0)
        tabt[b] = grown.T
        return carry

    lanes = lax.broadcasted_iota(jnp.int32, (half, QB), 1)

    def gated(rows, gate, up):
        a = jnp.dot(rows, gate, preferred_element_type=f32)
        b = jnp.dot(rows, up, preferred_element_type=f32)
        return a / (1.0 + jnp.exp(-a)) * b

    def hidden(b, lo, hi):
        def one(slot, carry):
            e = at(z, jnp.where(slot >= 2, oy, y), jnp.where(lax.rem(slot, 2) == 1, oc, c))
            scale = jnp.sum(jnp.where(lanes == e, tabt[b], 0.0), axis=-1, keepdims=True)
            for h in range(2):
                cols = slice(h * (ff // 2), (h + 1) * (ff // 2))
                v = gated(tok[b], gs[slot, :, cols], us[slot, :, cols]) * scale
                to = pl.ds(pl.multiple_of(slot * ff + h * (ff // 2), ff // 2), ff // 2)
                hid[b, :, to] = v.astype(bf16)
            return carry

        lax.fori_loop(lo, hi, one, 0)

    y_event(1)
    for i in range(LINE - 1):
        got(tab.at[z], tab_r.at[i])
    lax.fori_loop(0, LINE, table_columns, 0)
    got(gs.at[1], sib_r.at[0])
    got(us.at[1], sib_r.at[1])
    hidden(z, 0, 2)
    y_event(2)
    relay(0, 0)
    relay(2, 0)
    x_event(0)
    y_event(3)
    relay(0, 1)
    relay(2, 1)
    x_event(1)
    y_event(4)
    near = line(1 - w)

    @pl.when(w == 0)
    def _():
        ag_got(near, 0)
        ag_got(near, 1)

    hidden(near, 0, 2)
    relay(3, 0)
    x_event(2)
    y_event(5)
    relay(3, 1)
    srow, drow = sg_in.shape[0] // 2, sd_in.shape[0] // 2
    shared_views = lambda core: [
        sg.at[1, pl.ds(core * srow, srow)],
        su.at[1, pl.ds(core * srow, srow)],
        sd.at[pl.ds(sd_in.shape[0] + core * drow, drow)],
    ]
    for g in (2, 3):
        pass
    far2 = line(2)

    @pl.when(w == 0)
    def _():
        ag_got(far2, 0)
        ag_got(far2, 1)

    for i in range(5):
        kind, j = y_list[i]
        got(piece(held, kind, j, 3), fy_r.at[i])
    for i in range(3):
        kind, j = x_list[i]
        got(piece(held, kind, j, 3), fx_r.at[i])
    hidden(far2, 0, 4)
    for n in range(4):
        got(piece(held, "d", n, 1), sib_r.at[2 + n])
    y_event(6)
    for i, (src, dst) in enumerate(
        zip(
            [
                sg_in.at[pl.ds(c * srow, srow)],
                su_in.at[pl.ds(c * srow, srow)],
                sd_in.at[pl.ds(c * drow, drow)],
            ],
            shared_views(c),
        )
    ):
        pend.append(send(src, dst, sx_s.at[i], sx_r.at[i], xpar))

    order = [x, 2 + x, ox, 2 + ox]
    tile = lambda slot, n: rbuf.at[slot, n]

    def down(b, n):
        return jnp.dot(hid[b], ds[n], preferred_element_type=f32)

    def reduce_piece(step, n):
        b = jnp.where(step == 2, near, line(2 + step))
        slot = jnp.where(step == 0, 3 * w, jnp.where(step == 1, 1 + w, 4 - w))
        zt = jnp.where((step == 2) & inner, zb, zf)
        acc[...] = down(b, n)

        @pl.when(inner)
        def _():
            got(tile(step, n), rs_r.at[step, n])
            acc[...] = acc[...] + rbuf[step, n].astype(f32)

        stage[step, n] = acc[...].astype(bf16)
        send(
            stage.at[step, n], tile(slot, n), rs_s.at[step, n], rs_r.at[slot, n], dev(at(zt, y, c), x)
        )

    for k in range(4):
        kind, j = (y_list[5], y_list[6], x_list[3], x_list[4])[k]
        if k >= 2:
            x_event(k + 1)
        got(piece(held, kind, j, 3), (fy_r.at[5], fy_r.at[6], fx_r.at[3], fx_r.at[4])[k])
        reduce_piece(0, order[k])

    def nth(k):
        base = jnp.where(k < 2, x, ox)
        return base + 2 * lax.rem(k, 2)

    far3 = line(3)

    @pl.when(w == 0)
    def _():
        ag_got(far3, 0)
        ag_got(far3, 1)

    hidden(far3, 0, 4)

    def step_b(k, carry):
        reduce_piece(1, nth(k))
        return carry

    lax.fori_loop(0, 4, step_b, 0)
    hidden(near, 2, 4)

    def step_c(k, carry):
        reduce_piece(2, nth(k))
        return carry

    lax.fori_loop(0, 4, step_c, 0)

    hidden(z, 2, 4)
    for i, view in enumerate(shared_views(c)):
        got(view, sx_r.at[i])
        pend.append(send(view, view, ss_s.at[i], ss_r.at[i], sib))
    for i, view in enumerate(shared_views(oc)):
        got(view, ss_r.at[i])
    units = sg_in.shape[1]
    for h in range(2):
        sh[:, h * units : (h + 1) * units] = gated(tok[z], sg[h], su[h]).astype(bf16)

    def final(k, carry):
        n = nth(k)
        cols = pl.ds(pl.multiple_of(n * part, part), part)
        acc[...] = (
            res[:, cols].astype(f32)
            + down(z, n)
            + jnp.dot(sh[...], sd[:, cols], preferred_element_type=f32)
        )
        got(tile(3, n), rs_r.at[3, n])
        acc[...] = acc[...] + rbuf[3, n].astype(f32)

        @pl.when(inner)
        def _():
            got(tile(4, n), rs_r.at[4, n])
            acc[...] = acc[...] + rbuf[4, n].astype(f32)

        ost[n] = acc[...].astype(bf16)
        load(ost.at[n], out_ref.at[:, cols], out_sem.at[n])
        return carry

    lax.fori_loop(0, 4, final, 0)

    for cp in pend:
        cp.wait_send()
    for i in range(hb):
        sent(a_out.at[pl.ds(i * QB, QB)], att_s.at[i])
    for r in range(2):
        ag_sent(z, r, 0)

        @pl.when(inner)
        def _():
            ag_sent(z, r, 1)
            ag_sent(line(0), r, 0)
            ag_sent(line(2), r, 1)
            ag_sent(line(3), r, 1)

    for step in range(3):
        for n in range(4):
            sent(stage.at[step, n], rs_s.at[step, n])
    for n in range(4):
        pltpu.make_async_copy(ost.at[n], out_ref.at[:, pl.ds(n * part, part)], out_sem.at[n]).wait()


def fused_shards(
    queries, keys, values, doc_ids, sink_logit, w_out, residual, ffn_gain, expert_ids,
    expert_weight, exp_gate, exp_up, exp_down, shared_gate, shared_up, shared_down,
):
    bf16, f32 = jnp.bfloat16, jnp.float32
    experts = lax.axis_size("sp")
    chosen = expert_ids.T[:, None, :] == jnp.arange(experts, dtype=jnp.int32)[None, :, None]
    table = jnp.sum(jnp.where(chosen, expert_weight.T[:, None, :], 0.0), axis=0)
    tokens = queries.shape[0]
    nb = tokens // QB
    marks = jnp.broadcast_to(doc_ids.reshape(nb, 1, QB), (nb, 8, QB))
    half, width = residual.shape
    ff = exp_gate.shape[2]
    part = width // 4
    units = shared_gate.shape[1]
    heads = queries.shape[1]
    vm = pltpu.VMEM
    dma = pltpu.SemaphoreType.DMA
    anyspace = pl.BlockSpec(memory_space=pl.ANY)
    scratch = [
        vm((tokens, heads), bf16),
        vm((tokens + 2 * QB, QB), bf16),
        vm((tokens + 2 * QB, QB), bf16),
        vm((nb + 2, 8, QB), jnp.int32),
        vm((4, tokens + 2 * QB, QB), bf16),
        vm((4, tokens + 2 * QB, QB), bf16),
        vm((half, heads), bf16),
        vm((half, heads), bf16),
        vm((half, heads), bf16),
        vm(w_out.shape, bf16),
        vm(w_out.shape, bf16),
        vm((half, width), bf16),
        vm((LINE, half, width), bf16),
        vm((LINE, experts, half), f32),
        vm((LINE, half, QB), f32),
        vm((4, width, ff), bf16),
        vm((4, width, ff), bf16),
        vm((4, 4 * ff, part), bf16),
        vm((LINE, half, 4 * ff), bf16),
        vm((half, part), f32),
        vm((3, 4, half, part), bf16),
        vm((5, 4, half, part), bf16),
        vm((2, width, units), bf16),
        vm((2, width, units), bf16),
        vm((2 * units, width), bf16),
        vm((half, 2 * units), bf16),
        vm((4, half, part), bf16),
        dma((16,)), dma((6,)), dma((6,)), dma((3,)), dma((3,)), dma((2,)), dma((2,)),
        dma((2,)), dma((2,)),
        dma((6,)), dma((6,)), dma((7,)), dma((7,)), dma((5,)), dma((5,)), dma((7,)), dma((7,)),
        dma((5,)), dma((5,)),
        dma((2, LINE, 2)), dma((LINE, 2)), dma((3, 4)), dma((5, 4)),
        dma((3,)), dma((3,)), dma((3,)), dma((3,)), dma((4,)),
    ]
    rows = LINE * half
    return pl.pallas_call(
        layer_kernel,
        out_shape=jax.ShapeDtypeStruct((half, width), bf16),
        in_specs=[anyspace, anyspace, pl.BlockSpec(memory_space=pltpu.SMEM)]
        + [anyspace] * 5
        + [pl.BlockSpec(memory_space=pltpu.VMEM)]
        + [anyspace] * 6,
        out_specs=anyspace,
        scratch_shapes=scratch,
        compiler_params=pltpu.CompilerParams(
            collective_id=0, has_side_effects=True, vmem_limit_bytes=63 * 1024 * 1024
        ),
        cost_estimate=pl.CostEstimate(
            flops=24 * rows * width * ff, bytes_accessed=32 * width * ff, transcendentals=rows * ff
        ),
    )(
        table, marks, sink_logit, queries, keys, values, w_out, residual, ffn_gain.reshape(1, -1),
        exp_gate, exp_up, exp_down, shared_gate, shared_up, shared_down,
    )


def solution(mesh):
    fits = mesh.shape["tp"] == 2 and mesh.shape["sp"] == 4 * LINE
    placed = (
        P("sp", "tp"),
        P("sp", "tp"),
        P("sp", "tp"),
        P("sp"),
        P("tp"),
        P("tp", None),
        P(("sp", "tp"), None),
        P(),
        P(("sp", "tp"), None),
        P(("sp", "tp"), None),
        P("sp", None, None),
        P("sp", None, None),
        P("sp", None, None),
        P(None, "tp"),
        P(None, "tp"),
        P("tp", None),
    )
    return jax.shard_map(
        fused_shards if fits else shards, mesh=mesh, in_specs=placed, out_specs=P(("sp", "tp"), None), check_vma=False
    )
```

```python
import math

import jax
import jax.numpy as jnp
from jax import lax
from jax.experimental import pallas as pl
from jax.experimental.pallas import tpu as pltpu
from jax.sharding import PartitionSpec as P

HD = 64
WINDOW = 128
PARTS = 2


norm_eps = 1e-06


def extended(cells, sides, width):
    for axis, dim in sides:
        count = lax.axis_size(axis)
        ends = count - 1
        head = lax.slice_in_dim(cells, 0, width, axis=dim)
        tail = lax.slice_in_dim(cells, cells.shape[dim] - width, cells.shape[dim], axis=dim)
        cells = jnp.concatenate(
            [
                lax.ppermute(tail, axis, [(i, (i + 1) % count) for i in range(ends)]),
                cells,
                lax.ppermute(head, axis, [((i + 1) % count, i) for i in range(ends)]),
            ],
            axis=dim,
        )
    return cells


def band_blocks(padded, width):
    span_count = padded.shape[0] // width - 2
    shaped = padded.reshape((span_count + 2, width) + padded.shape[1:])
    return jnp.concatenate(
        [
            shaped[0:span_count:2],
            shaped[1 : span_count + 1 : 2],
            shaped[2 : span_count + 2 : 2],
            shaped[3 : span_count + 3 : 2],
        ],
        axis=1,
    )


def attend(queries, ext_keys, ext_values, ext_marks, own_marks, sink_logit):
    tok_count = queries.shape[0]
    head_count = sink_logit.shape[0]
    key_heads = ext_keys.shape[1] // HD
    group_size = head_count // key_heads
    query_span = 2 * WINDOW
    block_count = tok_count // query_span
    query_blocks = queries.reshape(block_count, query_span, key_heads, group_size, HD)
    key_blocks = band_blocks(ext_keys, WINDOW).reshape(block_count, 4 * WINDOW, key_heads, HD)
    value_blocks = band_blocks(ext_values, WINDOW).reshape(block_count, 4 * WINDOW, key_heads, HD)
    mark_blocks = band_blocks(ext_marks, WINDOW)
    query_marks = own_marks.reshape(block_count, query_span)
    scores = jnp.einsum(
        "nqkgd,nmkd->nkgqm", query_blocks, key_blocks, preferred_element_type=jnp.float32
    ) * HD ** (-0.5)
    offset = (
        jnp.arange(query_span, dtype=jnp.int32)[:, None]
        - jnp.arange(4 * WINDOW, dtype=jnp.int32)[None, :]
        + WINDOW
    )
    allowed = (jnp.abs(offset) <= WINDOW)[None] & (
        mark_blocks[:, None, :] == query_marks[:, :, None]
    )
    scores = jnp.where(allowed[:, None, None], scores, -jnp.inf)
    sink_term = sink_logit.reshape(key_heads, group_size)[None, :, :, None, None]
    row_max = jnp.maximum(jnp.max(scores, axis=-1, keepdims=True), sink_term)
    exp_scores = jnp.exp(scores - row_max)
    attn_probs = (
        exp_scores / (jnp.sum(exp_scores, axis=-1, keepdims=True) + jnp.exp(sink_term - row_max))
    ).astype(jnp.bfloat16)
    result = jnp.einsum(
        "nkgqm,nmkd->nqkgd", attn_probs, value_blocks, preferred_element_type=jnp.float32
    )
    return result.astype(jnp.bfloat16).reshape(tok_count, head_count * HD)


def expert_kernel(rows_ref, scale_ref, gate_ref, up_ref, down_ref, side_ref, side_down_ref, out_ref):
    rows = rows_ref[...]
    gated = jnp.dot(rows, gate_ref[...], preferred_element_type=jnp.float32)
    lifted = jnp.dot(rows, up_ref[...], preferred_element_type=jnp.float32)
    hidden = (gated / (1.0 + jnp.exp(-gated)) * lifted).astype(jnp.bfloat16)
    produced = jnp.dot(hidden, down_ref[...], preferred_element_type=jnp.float32)
    side = jnp.dot(rows, side_ref[...], preferred_element_type=jnp.float32)
    width = side.shape[1] // 2
    side_gate, side_up = side[:, :width], side[:, width:]
    side_hidden = (side_gate / (1.0 + jnp.exp(-side_gate)) * side_up).astype(jnp.bfloat16)
    shared = jnp.dot(side_hidden, side_down_ref[...], preferred_element_type=jnp.float32)
    out_ref[...] = (
        scale_ref[...] * produced.astype(jnp.bfloat16).astype(jnp.float32) + shared
    ).astype(jnp.bfloat16)


def run_experts(rows, scale, gate_w, up_w, down_w, side_w, side_down):
    count, width = rows.shape
    tile = math.gcd(count, 256)
    whole = lambda w: pl.BlockSpec(w.shape, lambda i: (0, 0))
    units = gate_w.shape[1] + side_w.shape[1] // 2
    return pl.pallas_call(
        expert_kernel,
        grid=(count // tile,),
        in_specs=[
            pl.BlockSpec((tile, width), lambda i: (i, 0)),
            pl.BlockSpec((tile, 1), lambda i: (i, 0)),
            whole(gate_w),
            whole(up_w),
            whole(down_w),
            whole(side_w),
            whole(side_down),
        ],
        out_specs=pl.BlockSpec((tile, width), lambda i: (i, 0)),
        out_shape=jax.ShapeDtypeStruct((count, width), jnp.bfloat16),
        compiler_params=pltpu.CompilerParams(
            dimension_semantics=("arbitrary",), vmem_limit_bytes=48 * 1024 * 1024
        ),
        cost_estimate=pl.CostEstimate(
            flops=6 * count * width * units,
            bytes_accessed=4 * count * width + 6 * units * width,
            transcendentals=count * units,
        ),
    )(rows, scale, gate_w, up_w, down_w, side_w, side_down)


def shared_slice(shared_gate, shared_up, shared_down):
    sp_count, tp_count = lax.axis_size("sp"), lax.axis_size("tp")
    own, side = lax.axis_index("tp"), lax.axis_index("sp")
    units = shared_gate.shape[1] * tp_count // sp_count
    per_owner = sp_count // tp_count
    owner, offset = side // per_owner, (side % per_owner) * units
    held = jnp.concatenate(
        [
            lax.dynamic_slice_in_dim(shared_gate, offset, units, axis=1).T,
            lax.dynamic_slice_in_dim(shared_up, offset, units, axis=1).T,
            lax.dynamic_slice_in_dim(shared_down, offset, units, axis=0),
        ],
        axis=0,
    )
    chosen = held
    for shift in range(1, tp_count):
        came = lax.ppermute(held, "tp", [(i, (i + shift) % tp_count) for i in range(tp_count)])
        chosen = jnp.where((own - shift) % tp_count == owner, came, chosen)
    padded = -(-units // 128) * 128
    grown = [
        jnp.pad(chosen[i * units : (i + 1) * units], ((0, padded - units), (0, 0))) for i in range(3)
    ]
    return jnp.concatenate(grown[:2], axis=0).T, grown[2]


def shards(
    queries,
    keys,
    values,
    doc_ids,
    sink_logit,
    w_out,
    residual,
    ffn_gain,
    expert_ids,
    expert_weight,
    exp_gate,
    exp_up,
    exp_down,
    shared_gate,
    shared_up,
    shared_down,
):
    marks = (doc_ids + 1).astype(jnp.bfloat16)
    kv = keys.shape[1]
    joined = jnp.concatenate(
        [keys, values, jnp.broadcast_to(marks[:, None], (marks.shape[0], 128))], axis=1
    )
    extended_all = extended(joined, (("sp", 0),), WINDOW)
    ext_keys, ext_values, ext_marks = (
        extended_all[:, :kv],
        extended_all[:, kv : 2 * kv],
        extended_all[:, 2 * kv],
    )
    attended = attend(queries, ext_keys, ext_values, ext_marks, marks, sink_logit)
    row_count = residual.shape[0]
    mixed = lax.psum_scatter(
        jnp.dot(attended, w_out, preferred_element_type=jnp.float32).astype(jnp.bfloat16),
        "tp",
        scatter_dimension=0,
        tiled=True,
    ).astype(jnp.float32)
    resid = (residual.astype(jnp.float32) + mixed).astype(jnp.bfloat16)
    resid_f = resid.astype(jnp.float32)
    normed = (
        resid_f
        * lax.rsqrt(jnp.mean(resid_f * resid_f, axis=-1, keepdims=True) + norm_eps)
        * ffn_gain
    ).astype(jnp.bfloat16)
    side_w, side_down = shared_slice(shared_gate, shared_up, shared_down)
    sp_count = lax.axis_size("sp")
    chosen = expert_ids[:, :, None] == jnp.arange(sp_count, dtype=jnp.int32)
    table = jnp.sum(jnp.where(chosen, expert_weight[:, :, None], 0.0), axis=1)
    scales = lax.all_to_all(table.T, "sp", split_axis=0, concat_axis=0, tiled=True)
    part_rows = row_count // PARTS
    sums = []
    for part in range(PARTS):
        begin = part * part_rows
        gathered = lax.all_gather(normed[begin : begin + part_rows], "sp", axis=0, tiled=True)
        scale = scales[:, begin : begin + part_rows].reshape(-1, 1)
        produced = run_experts(
            gathered, scale, exp_gate[0], exp_up[0], exp_down[0], side_w, side_down
        )
        sums.append(lax.psum_scatter(produced, "sp", scatter_dimension=0, tiled=True))
    added = jnp.concatenate(sums, axis=0)
    return (resid.astype(jnp.float32) + added.astype(jnp.float32)).astype(jnp.bfloat16)


MESH = pl.DeviceIdType.MESH
QB = 128
NEG = -1e30
LINE = 4


def layer_kernel(
    ids_in, wts_in, marks_in, sink_ref, q_in, k_in, v_in, wo_in, res_in, gain_ref,
    eg_in, eu_in, ed_in, sg_in, su_in, sd_in,
    out_ref,
    q_s, kx, vx, marks, kk, vv, a_out, a_own, a_in, wo_own, wo_oth, res, tok, ids, wts, tab, tabt,
    gs, us, ds, hid, acc, base, stage, rbuf, sg, su, sd, sh, ost,
    loc, halo_s, halo_r, tab_s, tab_r, wx_s, wx_r, wz_s, wz_r, wf_s, wf_r, wg_s, wg_r, att_s, att_r,
    sib_s, sib_r, y_s, y_r, x_s, x_r, fy_s, fy_r, fx_s, fx_r,
    ag_s, ag_r, rs_s, rs_r, sx_s, sx_r, ss_s, ss_r, out_sem,
):
    f32, bf16 = jnp.float32, jnp.bfloat16
    sp_count, tp_count = lax.axis_size("sp"), lax.axis_size("tp")
    s, x = lax.axis_index("sp"), lax.axis_index("tp")
    z, y, c = s // 4, lax.rem(s // 2, 2), lax.rem(s, 2)
    ox, oy, oc = 1 - x, 1 - y, 1 - c
    at = lambda zz, yy, cc: (zz * 2 + yy) * 2 + cc
    dev = lambda sp, tp: {"sp": sp, "tp": tp}
    sib, ypar, xpar = dev(at(z, y, oc), x), dev(at(z, oy, c), x), dev(s, ox)
    nxt, prv = dev(lax.rem(s + 1, sp_count), x), dev(lax.rem(s + sp_count - 1, sp_count), x)
    low = z < 2
    w = jnp.where(low, z, 3 - z)
    inner = w == 1
    zf = jnp.where(low, z + 1, z - 1)
    zb = jnp.clip(jnp.where(low, z - 1, z + 1), 0, 3)
    fwd, bck = dev(at(zf, y, c), x), dev(at(zb, y, c), x)
    line = lambda ob: jnp.where(low, ob, 3 - ob)
    tokens = q_in.shape[0]
    half = tokens // 2
    width = res_in.shape[1]
    ff = eg_in.shape[2]
    part = width // 4

    def send(src, dst, ss, rs, to):
        cp = pltpu.make_async_remote_copy(
            src_ref=src, dst_ref=dst, send_sem=ss, recv_sem=rs, device_id=to, device_id_type=MESH
        )
        cp.start()
        return cp

    def got(view, rs):
        pltpu.make_async_remote_copy(
            src_ref=view, dst_ref=view, send_sem=rs, recv_sem=rs, device_id=sib, device_id_type=MESH
        ).wait_recv()

    def sent(view, ss):
        pltpu.make_async_remote_copy(
            src_ref=view, dst_ref=view, send_sem=ss, recv_sem=ss, device_id=sib, device_id_type=MESH
        ).wait_send()

    def load(src, dst, sem):
        cp = pltpu.make_async_copy(src, dst, sem)
        cp.start()
        return cp

    rows_own = pl.ds(QB, tokens)
    loads_a = [
        load(q_in, q_s, loc.at[0]),
        load(k_in, kx.at[rows_own], loc.at[1]),
        load(v_in, vx.at[rows_own], loc.at[2]),
        load(marks_in, marks.at[pl.ds(1, tokens // QB)], loc.at[3]),
        load(ids_in, ids, loc.at[6]),
        load(wts_in, wts, loc.at[16]),
    ]
    loads_b = [
        load(wo_in, wo_own, loc.at[4]),
        load(res_in, res, loc.at[5]),
        load(eg_in.at[0], gs.at[0], loc.at[7]),
        load(eu_in.at[0], us.at[0], loc.at[8]),
        load(sg_in, sg.at[0], loc.at[9]),
        load(su_in, su.at[0], loc.at[10]),
        load(sd_in, sd.at[pl.ds(0, sd_in.shape[0])], loc.at[11]),
    ]
    for n in range(4):
        loads_b.append(
            load(ed_in.at[0, :, pl.ds(n * part, part)], ds.at[n, pl.ds(0, ff)], loc.at[12 + n])
        )

    barrier = pltpu.get_barrier_semaphore()
    zs = [lax.rem(z + i, LINE) for i in range(1, LINE)]
    partners = [nxt, prv, sib, ypar, xpar] + [dev(at(zz, y, c), x) for zz in zs]
    for to in partners:
        pl.semaphore_signal(barrier, inc=1, device_id=to, device_id_type=MESH)
    pl.semaphore_wait(barrier, len(partners))

    pend = []
    last, first = pl.ds(tokens - QB, QB), pl.ds(0, QB)
    after = pl.ds(QB + tokens, QB)
    nb = tokens // QB
    for i, (src, dst, lo, hi, a, b) in enumerate(
        [(k_in, kx, first, after, last, first), (v_in, vx, first, after, last, first)]
    ):
        pend.append(send(src.at[a], dst.at[lo], halo_s.at[2 * i], halo_r.at[2 * i], nxt))
        pend.append(send(src.at[b], dst.at[hi], halo_s.at[2 * i + 1], halo_r.at[2 * i + 1], prv))
    pend.append(send(marks_in.at[nb - 1], marks.at[0], halo_s.at[4], halo_r.at[4], nxt))
    pend.append(send(marks_in.at[0], marks.at[nb + 1], halo_s.at[5], halo_r.at[5], prv))

    pair = dev(at(jnp.where(inner, zb, zf), y, c), x)
    wrows = wo_in.shape[0] // 8
    wpiece = lambda pos, core, i: pl.ds(pl.multiple_of(((pos * 2 + core) * 2 + i) * wrows, wrows), wrows)
    for i in range(2):
        rows = wpiece(w, c, i)
        pend.append(send(wo_in.at[rows], wo_oth.at[rows], wx_s.at[i], wx_r.at[i], xpar))

    def wx_event(i):
        view = wo_oth.at[wpiece(w, c, i)]
        got(view, wx_r.at[i])
        pend.append(send(view, view, wz_s.at[i], wz_r.at[i], pair))
        pend.append(send(view, view, wf_s.at[i], wf_r.at[i], sib))

    def wz_event(i):
        view = wo_oth.at[wpiece(1 - w, c, i)]
        got(view, wz_r.at[i])
        pend.append(send(view, view, wg_s.at[i], wg_r.at[i], sib))

    quarter = width // 4

    def piece(refs, kind, i, slot):
        g, u, d = refs
        if kind == "g":
            return g.at[slot, pl.ds(i * quarter, quarter)]
        if kind == "u":
            return u.at[slot, pl.ds(i * quarter, quarter)]
        if slot is None:
            return d.at[0, :, pl.ds(i * part, part)]
        return d.at[i, pl.ds(slot * ff, ff)]

    def hbm_piece(kind, i):
        if kind == "g":
            return eg_in.at[0, pl.ds(i * quarter, quarter)]
        if kind == "u":
            return eu_in.at[0, pl.ds(i * quarter, quarter)]
        return ed_in.at[0, :, pl.ds(pl.multiple_of(i * part, part), part)]

    held = (gs, us, ds)
    own_only = lambda v: [
        ("g", 2 * v), ("g", 2 * v + 1), ("u", 2 * v), ("u", 2 * v + 1), ("d", v), ("d", 2 + v)
    ]
    y_list, x_list = own_only(x), own_only(ox)
    for i, (kind, j) in enumerate(y_list):
        pend.append(send(hbm_piece(kind, j), piece(held, kind, j, 2), y_s.at[i], y_r.at[i], ypar))
    pend.append(send(eg_in.at[0], gs.at[1], sib_s.at[0], sib_r.at[0], sib))
    pend.append(send(eu_in.at[0], us.at[1], sib_s.at[1], sib_r.at[1], sib))
    for n in range(4):
        pend.append(
            send(hbm_piece("d", n), piece(held, "d", n, 1), sib_s.at[2 + n], sib_r.at[2 + n], sib)
        )

    def y_event(i):
        kind, j = y_list[i]
        view = piece(held, kind, j, 2)
        got(view, y_r.at[i])
        pend.append(send(view, view, x_s.at[i], x_r.at[i], xpar))
        pend.append(send(view, piece(held, kind, j, 3), fy_s.at[i], fy_r.at[i], sib))

    def x_event(i):
        kind, j = x_list[i]
        view = piece(held, kind, j, 2)
        got(view, x_r.at[i])
        pend.append(send(view, piece(held, kind, j, 3), fx_s.at[i], fx_r.at[i], sib))

    for cp in loads_a:
        cp.wait()
    lanes = lax.broadcasted_iota(jnp.int32, (half, QB), 1)
    table = jnp.zeros((half, QB), f32)
    for k in range(ids.shape[1]):
        table = table + jnp.where(lanes == ids[:, k : k + 1], wts[:, k : k + 1], 0.0)
    tabt[z] = table
    tab[z] = table.T[: tab.shape[1]]
    for i, zz in enumerate(zs):
        pend.append(
            send(tab.at[z], tab.at[z], tab_s.at[i], tab_r.at[LINE - 2 - i], dev(at(zz, y, c), x))
        )
    for i in range(2):
        dst = (kx, vx)[i]
        got(dst.at[first], halo_r.at[2 * i])
        got(dst.at[after], halo_r.at[2 * i + 1])
    got(marks.at[0], halo_r.at[4])
    got(marks.at[nb + 1], halo_r.at[5])

    @pl.when(s == 0)
    def _():
        marks[0] = jnp.full(marks.shape[1:], -1, jnp.int32)

    @pl.when(s == sp_count - 1)
    def _():
        marks[nb + 1] = jnp.full(marks.shape[1:], -1, jnp.int32)

    ri = lax.broadcasted_iota(jnp.int32, (QB, QB), 0)
    ci = lax.broadcasted_iota(jnp.int32, (QB, QB), 1)
    swap = jnp.where(ci == lax.rem(ri + HD, QB), 1.0, 0.0).astype(bf16)

    def spread(t, carry):
        rows = pl.ds(pl.multiple_of(t * QB, QB), QB)
        for src, dst in ((kx, kk), (vx, vv)):
            cur = src[rows]
            turned = jnp.dot(cur, swap, preferred_element_type=f32)
            cur = cur.astype(f32)
            zero = jnp.zeros_like(cur)
            left = ci < HD
            dst[0, rows] = jnp.where(left, cur, zero).astype(bf16)
            dst[1, rows] = jnp.where(left, zero, turned).astype(bf16)
            dst[2, rows] = jnp.where(left, turned, zero).astype(bf16)
            dst[3, rows] = jnp.where(left, zero, cur).astype(bf16)
        return carry

    lax.fori_loop(0, nb + 2, spread, 0)

    def attend_rows(blk, dst, drow):
        rows = pl.ds(pl.multiple_of(blk * QB, QB), QB)
        span = pl.ds(pl.multiple_of(blk * QB, QB), 3 * QB)
        mine = jnp.broadcast_to(marks[blk + 1][0:1], (QB, QB)).T
        biases = []
        for t in range(3):
            same = mine == jnp.broadcast_to(marks[blk + t][0:1], (QB, QB))
            if t == 0:
                same = same & (ri <= ci)
            if t == 2:
                same = same & (ci <= ri)
            biases.append(jnp.where(same, 0.0, NEG).astype(f32))
        bias = jnp.concatenate(biases, axis=1)
        for j in range(q_s.shape[1] // QB):
            g = j // 2
            keys2 = jnp.concatenate([kk[2 * g, span], kk[2 * g + 1, span]], axis=0)
            vals2 = jnp.concatenate([vv[2 * g, span], vv[2 * g + 1, span]], axis=0)
            sc = lax.dot_general(
                q_s[rows, j * QB : (j + 1) * QB], keys2, (((1,), (1,)), ((), ())),
                preferred_element_type=f32,
            ) * HD ** (-0.5)
            probs = []
            for h in range(2):
                sink = sink_ref[2 * j + h]
                own = sc[:, h * 3 * QB : (h + 1) * 3 * QB] + bias
                top = jnp.maximum(jnp.max(own, axis=-1, keepdims=True), sink)
                e = jnp.exp(own - top)
                total = jnp.sum(e, axis=-1, keepdims=True) + jnp.exp(sink - top)
                probs.append((e * (1.0 / total)).astype(bf16))
            o = jnp.dot(jnp.concatenate(probs, axis=1), vals2, preferred_element_type=f32)
            dst[pl.ds(pl.multiple_of(drow, QB), QB), j * QB : (j + 1) * QB] = o.astype(bf16)

    hb = half // QB

    for i in range(hb):
        attend_rows(ox * hb + i, a_out, i * QB)
        rows = pl.ds(i * QB, QB)
        pend.append(send(a_out.at[rows], a_in.at[rows], att_s.at[i], att_r.at[i], xpar))
        if i == 0:
            wx_event(0)
    for i in range(hb):
        attend_rows(x * hb + i, a_own, i * QB)

    wx_event(1)
    y_event(0)
    for cp in loads_b:
        cp.wait()
    for n in range(4):
        cols = slice(n * part, (n + 1) * part)
        base[n] = res[:, cols].astype(f32) + jnp.dot(
            a_own[...], wo_own[:, cols], preferred_element_type=f32
        )
    wz_event(0)
    for i in range(hb):
        got(a_in.at[pl.ds(i * QB, QB)], att_r.at[i])
    wz_event(1)
    for i in range(2):
        got(wo_oth.at[wpiece(w, oc, i)], wf_r.at[i])
        got(wo_oth.at[wpiece(1 - w, oc, i)], wg_r.at[i])
    square = jnp.zeros((half, 1), f32)
    for n in range(4):
        cols = slice(n * part, (n + 1) * part)
        r = (
            base[n] + jnp.dot(a_in[...], wo_oth[:, cols], preferred_element_type=f32)
        ).astype(bf16)
        res[:, cols] = r
        rf = r.astype(f32)
        square = square + jnp.sum(rf * rf, axis=-1, keepdims=True)
    inv = lax.rsqrt(square * (1.0 / width) + norm_eps)
    for n in range(4):
        cols = slice(n * part, (n + 1) * part)
        tok[z, :, cols] = (res[:, cols].astype(f32) * inv * gain_ref[:, cols]).astype(bf16)

    hr = half // 2
    rows_of = lambda r: pl.ds(r * hr, hr)

    def ag_send(b, r, direction, to):
        view = tok.at[b, rows_of(r)]
        send(view, view, ag_s.at[direction, b, r], ag_r.at[b, r], to)

    def ag_sent(b, r, direction):
        sent(tok.at[b, rows_of(r)], ag_s.at[direction, b, r])

    def ag_got(b, r):
        got(tok.at[b, rows_of(r)], ag_r.at[b, r])

    for r in range(2):
        ag_send(z, r, 0, fwd)

        @pl.when(inner)
        def _():
            ag_send(z, r, 1, bck)

    def relay(ob, r):
        b = line(ob)

        @pl.when(inner)
        def _():
            ag_got(b, r)
            if ob == 0:
                ag_send(b, r, 0, fwd)
            else:
                ag_send(b, r, 1, bck)

    def table_columns(i, carry):
        b = lax.rem(z + i, LINE)
        t = tab[b]
        grown = jnp.concatenate([t, jnp.zeros((QB - t.shape[0], t.shape[1]), f32)], axis=0)
        tabt[b] = grown.T
        return carry

    def gated(rows, gate, up):
        a = jnp.dot(rows, gate, preferred_element_type=f32)
        b = jnp.dot(rows, up, preferred_element_type=f32)
        return a / (1.0 + jnp.exp(-a)) * b

    def hidden(b, lo, hi):
        def one(slot, carry):
            e = at(z, jnp.where(slot >= 2, oy, y), jnp.where(lax.rem(slot, 2) == 1, oc, c))
            scale = jnp.sum(jnp.where(lanes == e, tabt[b], 0.0), axis=-1, keepdims=True)
            for h in range(2):
                cols = slice(h * (ff // 2), (h + 1) * (ff // 2))
                v = gated(tok[b], gs[slot, :, cols], us[slot, :, cols]) * scale
                to = pl.ds(pl.multiple_of(slot * ff + h * (ff // 2), ff // 2), ff // 2)
                hid[b, :, to] = v.astype(bf16)
            return carry

        lax.fori_loop(lo, hi, one, 0)

    y_event(1)
    for i in range(LINE - 1):
        got(tab.at[z], tab_r.at[i])
    lax.fori_loop(1, LINE, table_columns, 0)
    got(gs.at[1], sib_r.at[0])
    got(us.at[1], sib_r.at[1])
    hidden(z, 0, 2)
    relay(0, 0)
    relay(2, 0)
    x_event(0)
    y_event(2)
    x_event(1)
    relay(0, 1)
    relay(2, 1)
    y_event(3)
    near, far2, far3 = line(1 - w), line(2), line(3)

    def end_got(b):
        @pl.when(w == 0)
        def _():
            ag_got(b, 0)
            ag_got(b, 1)

    end_got(near)
    hidden(near, 0, 2)
    x_event(2)
    relay(3, 0)
    y_event(4)
    x_event(3)
    relay(3, 1)
    for i in range(4):
        kind, j = y_list[i]
        got(piece(held, kind, j, 3), fy_r.at[i])
        kind, j = x_list[i]
        got(piece(held, kind, j, 3), fx_r.at[i])
    hidden(near, 2, 4)
    for n in range(4):
        got(piece(held, "d", n, 1), sib_r.at[2 + n])
    srow, drow = sg_in.shape[0] // 2, sd_in.shape[0] // 2
    shared_views = lambda core: [
        sg.at[1, pl.ds(core * srow, srow)],
        su.at[1, pl.ds(core * srow, srow)],
        sd.at[pl.ds(sd_in.shape[0] + core * drow, drow)],
    ]
    shared_parts = [
        sg_in.at[pl.ds(c * srow, srow)],
        su_in.at[pl.ds(c * srow, srow)],
        sd_in.at[pl.ds(c * drow, drow)],
    ]

    order = [x, 2 + x, ox, 2 + ox]
    tile = lambda slot, n: rbuf.at[slot, n]

    def down(b, n):
        return jnp.dot(hid[b], ds[n], preferred_element_type=f32)

    def reduce_piece(step, n):
        b = jnp.where(step == 2, near, line(2 + step))
        slot = jnp.where(step == 0, 3 * w, jnp.where(step == 1, 1 + w, 4 - w))
        zt = jnp.where((step == 2) & inner, zb, zf)
        acc[...] = down(b, n)

        @pl.when(inner)
        def _():
            got(tile(step, n), rs_r.at[step, n])
            acc[...] = acc[...] + rbuf[step, n].astype(f32)

        stage[step, n] = acc[...].astype(bf16)
        send(
            stage.at[step, n], tile(slot, n), rs_s.at[step, n], rs_r.at[slot, n], dev(at(zt, y, c), x)
        )

    def nth(k):
        base_n = jnp.where(k < 2, x, ox)
        return base_n + 2 * lax.rem(k, 2)

    def down_got(k):
        lst, sem = (y_list, fy_r) if k < 2 else (x_list, fx_r)
        kind, j = lst[4 + k % 2]
        got(piece(held, kind, j, 3), sem.at[4 + k % 2])

    def near_early(k):
        @pl.when(w == 0)
        def _():
            reduce_piece(2, order[k])

    down_got(0)
    near_early(0)
    end_got(far2)
    hidden(far2, 0, 4)
    y_event(5)
    for i, (src, dst) in enumerate(zip(shared_parts, shared_views(c))):
        pend.append(send(src, dst, sx_s.at[i], sx_r.at[i], xpar))
    down_got(1)
    near_early(1)
    reduce_piece(0, order[0])
    reduce_piece(0, order[1])
    x_event(4)
    down_got(2)
    reduce_piece(0, order[2])
    hidden(z, 2, 4)
    x_event(5)
    down_got(3)
    reduce_piece(0, order[3])
    end_got(far3)
    hidden(far3, 0, 4)

    def later(i, carry):
        even = lax.rem(i, 2) == 0
        step = jnp.where(inner, jnp.where(even, 1, 2), jnp.where(i < 4, 1, 2))
        k = jnp.where(inner, i // 2, jnp.where(i < 4, i, i - 2))
        reduce_piece(step, nth(k))
        return carry

    def own_sum(n, carry):
        cols = pl.ds(pl.multiple_of(n * part, part), part)
        base[n] = res[:, cols].astype(f32) + down(z, n)
        return carry

    lax.fori_loop(0, 2, later, 0)
    lax.fori_loop(0, 4, own_sum, 0)
    lax.fori_loop(2, 6, later, 0)

    for i, view in enumerate(shared_views(c)):
        got(view, sx_r.at[i])
        pend.append(send(view, view, ss_s.at[i], ss_r.at[i], sib))
    for i, view in enumerate(shared_views(oc)):
        got(view, ss_r.at[i])
    units = sg_in.shape[1]
    for h in range(2):
        sh[:, h * units : (h + 1) * units] = gated(tok[z], sg[h], su[h]).astype(bf16)

    def shared_sum(n, carry):
        cols = pl.ds(pl.multiple_of(n * part, part), part)
        base[n] = base[n] + jnp.dot(sh[...], sd[:, cols], preferred_element_type=f32)
        return carry

    lax.fori_loop(0, 4, shared_sum, 0)
    lax.fori_loop(6, 6 + 2 * w, later, 0)

    def final(k, carry):
        n = nth(k)
        cols = pl.ds(pl.multiple_of(n * part, part), part)
        got(tile(3, n), rs_r.at[3, n])
        acc[...] = base[n] + rbuf[3, n].astype(f32)

        @pl.when(inner)
        def _():
            got(tile(4, n), rs_r.at[4, n])
            acc[...] = acc[...] + rbuf[4, n].astype(f32)

        ost[n] = acc[...].astype(bf16)
        load(ost.at[n], out_ref.at[:, cols], out_sem.at[n])
        return carry

    lax.fori_loop(0, 4, final, 0)

    for cp in pend:
        cp.wait_send()
    for r in range(2):
        ag_sent(z, r, 0)

        @pl.when(inner)
        def _():
            ag_sent(z, r, 1)
            ag_sent(line(0), r, 0)
            ag_sent(line(2), r, 1)
            ag_sent(line(3), r, 1)

    for step in range(3):
        for n in range(4):
            sent(stage.at[step, n], rs_s.at[step, n])
    for n in range(4):
        pltpu.make_async_copy(ost.at[n], out_ref.at[:, pl.ds(n * part, part)], out_sem.at[n]).wait()


def fused_shards(
    queries, keys, values, doc_ids, sink_logit, w_out, residual, ffn_gain, expert_ids,
    expert_weight, exp_gate, exp_up, exp_down, shared_gate, shared_up, shared_down,
):
    bf16, f32 = jnp.bfloat16, jnp.float32
    experts = lax.axis_size("sp")
    tokens = queries.shape[0]
    nb = tokens // QB
    marks = doc_ids.reshape(nb, 1, QB)
    half, width = residual.shape
    ff = exp_gate.shape[2]
    part = width // 4
    units = shared_gate.shape[1]
    heads = queries.shape[1]
    vm = pltpu.VMEM
    dma = pltpu.SemaphoreType.DMA
    anyspace = pl.BlockSpec(memory_space=pl.ANY)
    scratch = [
        vm((tokens, heads), bf16),
        vm((tokens + 2 * QB, QB), bf16),
        vm((tokens + 2 * QB, QB), bf16),
        vm((nb + 2, 1, QB), jnp.int32),
        vm((4, tokens + 2 * QB, QB), bf16),
        vm((4, tokens + 2 * QB, QB), bf16),
        vm((half, heads), bf16),
        vm((half, heads), bf16),
        vm((half, heads), bf16),
        vm(w_out.shape, bf16),
        vm(w_out.shape, bf16),
        vm((half, width), bf16),
        vm((LINE, half, width), bf16),
        vm(expert_ids.shape, jnp.int32),
        vm(expert_weight.shape, f32),
        vm((LINE, experts, half), f32),
        vm((LINE, half, QB), f32),
        vm((4, width, ff), bf16),
        vm((4, width, ff), bf16),
        vm((4, 4 * ff, part), bf16),
        vm((LINE, half, 4 * ff), bf16),
        vm((half, part), f32),
        vm((4, half, part), f32),
        vm((3, 4, half, part), bf16),
        vm((5, 4, half, part), bf16),
        vm((2, width, units), bf16),
        vm((2, width, units), bf16),
        vm((2 * units, width), bf16),
        vm((half, 2 * units), bf16),
        vm((4, half, part), bf16),
        dma((17,)), dma((6,)), dma((6,)), dma((3,)), dma((3,)),
        *[dma((2,)) for _ in range(10)],
        *[dma((6,)) for _ in range(10)],
        dma((2, LINE, 2)), dma((LINE, 2)), dma((3, 4)), dma((5, 4)),
        dma((3,)), dma((3,)), dma((3,)), dma((3,)), dma((4,)),
    ]
    rows = LINE * half
    return pl.pallas_call(
        layer_kernel,
        out_shape=jax.ShapeDtypeStruct((half, width), bf16),
        in_specs=[anyspace] * 3 + [pl.BlockSpec(memory_space=pltpu.SMEM)]
        + [anyspace] * 5
        + [pl.BlockSpec(memory_space=pltpu.VMEM)]
        + [anyspace] * 6,
        out_specs=anyspace,
        scratch_shapes=scratch,
        compiler_params=pltpu.CompilerParams(
            collective_id=0, has_side_effects=True, vmem_limit_bytes=63 * 1024 * 1024
        ),
        cost_estimate=pl.CostEstimate(
            flops=24 * rows * width * ff, bytes_accessed=32 * width * ff, transcendentals=rows * ff
        ),
    )(
        expert_ids, expert_weight, marks, sink_logit, queries, keys, values, w_out, residual, ffn_gain.reshape(1, -1),
        exp_gate, exp_up, exp_down, shared_gate, shared_up, shared_down,
    )


def solution(mesh):
    fits = mesh.shape["tp"] == 2 and mesh.shape["sp"] == 4 * LINE
    placed = (
        P("sp", "tp"),
        P("sp", "tp"),
        P("sp", "tp"),
        P("sp"),
        P("tp"),
        P("tp", None),
        P(("sp", "tp"), None),
        P(),
        P(("sp", "tp"), None),
        P(("sp", "tp"), None),
        P("sp", None, None),
        P("sp", None, None),
        P("sp", None, None),
        P(None, "tp"),
        P(None, "tp"),
        P("tp", None),
    )
    return jax.shard_map(
        fused_shards if fits else shards, mesh=mesh, in_specs=placed, out_specs=P(("sp", "tp"), None), check_vma=False
    )
```

```python
import math

import jax
import jax.numpy as jnp
from jax import lax
from jax.experimental import pallas as pl
from jax.experimental.pallas import tpu as pltpu
from jax.sharding import PartitionSpec as P

HD = 64
WINDOW = 128
PARTS = 2


norm_eps = 1e-06


def extended(cells, sides, width):
    for axis, dim in sides:
        count = lax.axis_size(axis)
        ends = count - 1
        head = lax.slice_in_dim(cells, 0, width, axis=dim)
        tail = lax.slice_in_dim(cells, cells.shape[dim] - width, cells.shape[dim], axis=dim)
        cells = jnp.concatenate(
            [
                lax.ppermute(tail, axis, [(i, (i + 1) % count) for i in range(ends)]),
                cells,
                lax.ppermute(head, axis, [((i + 1) % count, i) for i in range(ends)]),
            ],
            axis=dim,
        )
    return cells


def band_blocks(padded, width):
    span_count = padded.shape[0] // width - 2
    shaped = padded.reshape((span_count + 2, width) + padded.shape[1:])
    return jnp.concatenate(
        [
            shaped[0:span_count:2],
            shaped[1 : span_count + 1 : 2],
            shaped[2 : span_count + 2 : 2],
            shaped[3 : span_count + 3 : 2],
        ],
        axis=1,
    )


def attend(queries, ext_keys, ext_values, ext_marks, own_marks, sink_logit):
    tok_count = queries.shape[0]
    head_count = sink_logit.shape[0]
    key_heads = ext_keys.shape[1] // HD
    group_size = head_count // key_heads
    query_span = 2 * WINDOW
    block_count = tok_count // query_span
    query_blocks = queries.reshape(block_count, query_span, key_heads, group_size, HD)
    key_blocks = band_blocks(ext_keys, WINDOW).reshape(block_count, 4 * WINDOW, key_heads, HD)
    value_blocks = band_blocks(ext_values, WINDOW).reshape(block_count, 4 * WINDOW, key_heads, HD)
    mark_blocks = band_blocks(ext_marks, WINDOW)
    query_marks = own_marks.reshape(block_count, query_span)
    scores = jnp.einsum(
        "nqkgd,nmkd->nkgqm", query_blocks, key_blocks, preferred_element_type=jnp.float32
    ) * HD ** (-0.5)
    offset = (
        jnp.arange(query_span, dtype=jnp.int32)[:, None]
        - jnp.arange(4 * WINDOW, dtype=jnp.int32)[None, :]
        + WINDOW
    )
    allowed = (jnp.abs(offset) <= WINDOW)[None] & (
        mark_blocks[:, None, :] == query_marks[:, :, None]
    )
    scores = jnp.where(allowed[:, None, None], scores, -jnp.inf)
    sink_term = sink_logit.reshape(key_heads, group_size)[None, :, :, None, None]
    row_max = jnp.maximum(jnp.max(scores, axis=-1, keepdims=True), sink_term)
    exp_scores = jnp.exp(scores - row_max)
    attn_probs = (
        exp_scores / (jnp.sum(exp_scores, axis=-1, keepdims=True) + jnp.exp(sink_term - row_max))
    ).astype(jnp.bfloat16)
    result = jnp.einsum(
        "nkgqm,nmkd->nqkgd", attn_probs, value_blocks, preferred_element_type=jnp.float32
    )
    return result.astype(jnp.bfloat16).reshape(tok_count, head_count * HD)


def expert_kernel(rows_ref, scale_ref, gate_ref, up_ref, down_ref, side_ref, side_down_ref, out_ref):
    rows = rows_ref[...]
    gated = jnp.dot(rows, gate_ref[...], preferred_element_type=jnp.float32)
    lifted = jnp.dot(rows, up_ref[...], preferred_element_type=jnp.float32)
    hidden = (gated / (1.0 + jnp.exp(-gated)) * lifted).astype(jnp.bfloat16)
    produced = jnp.dot(hidden, down_ref[...], preferred_element_type=jnp.float32)
    side = jnp.dot(rows, side_ref[...], preferred_element_type=jnp.float32)
    width = side.shape[1] // 2
    side_gate, side_up = side[:, :width], side[:, width:]
    side_hidden = (side_gate / (1.0 + jnp.exp(-side_gate)) * side_up).astype(jnp.bfloat16)
    shared = jnp.dot(side_hidden, side_down_ref[...], preferred_element_type=jnp.float32)
    out_ref[...] = (
        scale_ref[...] * produced.astype(jnp.bfloat16).astype(jnp.float32) + shared
    ).astype(jnp.bfloat16)


def run_experts(rows, scale, gate_w, up_w, down_w, side_w, side_down):
    count, width = rows.shape
    tile = math.gcd(count, 256)
    whole = lambda w: pl.BlockSpec(w.shape, lambda i: (0, 0))
    units = gate_w.shape[1] + side_w.shape[1] // 2
    return pl.pallas_call(
        expert_kernel,
        grid=(count // tile,),
        in_specs=[
            pl.BlockSpec((tile, width), lambda i: (i, 0)),
            pl.BlockSpec((tile, 1), lambda i: (i, 0)),
            whole(gate_w),
            whole(up_w),
            whole(down_w),
            whole(side_w),
            whole(side_down),
        ],
        out_specs=pl.BlockSpec((tile, width), lambda i: (i, 0)),
        out_shape=jax.ShapeDtypeStruct((count, width), jnp.bfloat16),
        compiler_params=pltpu.CompilerParams(
            dimension_semantics=("arbitrary",), vmem_limit_bytes=48 * 1024 * 1024
        ),
        cost_estimate=pl.CostEstimate(
            flops=6 * count * width * units,
            bytes_accessed=4 * count * width + 6 * units * width,
            transcendentals=count * units,
        ),
    )(rows, scale, gate_w, up_w, down_w, side_w, side_down)


def shared_slice(shared_gate, shared_up, shared_down):
    sp_count, tp_count = lax.axis_size("sp"), lax.axis_size("tp")
    own, side = lax.axis_index("tp"), lax.axis_index("sp")
    units = shared_gate.shape[1] * tp_count // sp_count
    per_owner = sp_count // tp_count
    owner, offset = side // per_owner, (side % per_owner) * units
    held = jnp.concatenate(
        [
            lax.dynamic_slice_in_dim(shared_gate, offset, units, axis=1).T,
            lax.dynamic_slice_in_dim(shared_up, offset, units, axis=1).T,
            lax.dynamic_slice_in_dim(shared_down, offset, units, axis=0),
        ],
        axis=0,
    )
    chosen = held
    for shift in range(1, tp_count):
        came = lax.ppermute(held, "tp", [(i, (i + shift) % tp_count) for i in range(tp_count)])
        chosen = jnp.where((own - shift) % tp_count == owner, came, chosen)
    padded = -(-units // 128) * 128
    grown = [
        jnp.pad(chosen[i * units : (i + 1) * units], ((0, padded - units), (0, 0))) for i in range(3)
    ]
    return jnp.concatenate(grown[:2], axis=0).T, grown[2]


def shards(
    queries,
    keys,
    values,
    doc_ids,
    sink_logit,
    w_out,
    residual,
    ffn_gain,
    expert_ids,
    expert_weight,
    exp_gate,
    exp_up,
    exp_down,
    shared_gate,
    shared_up,
    shared_down,
):
    marks = (doc_ids + 1).astype(jnp.bfloat16)
    kv = keys.shape[1]
    joined = jnp.concatenate(
        [keys, values, jnp.broadcast_to(marks[:, None], (marks.shape[0], 128))], axis=1
    )
    extended_all = extended(joined, (("sp", 0),), WINDOW)
    ext_keys, ext_values, ext_marks = (
        extended_all[:, :kv],
        extended_all[:, kv : 2 * kv],
        extended_all[:, 2 * kv],
    )
    attended = attend(queries, ext_keys, ext_values, ext_marks, marks, sink_logit)
    row_count = residual.shape[0]
    mixed = lax.psum_scatter(
        jnp.dot(attended, w_out, preferred_element_type=jnp.float32).astype(jnp.bfloat16),
        "tp",
        scatter_dimension=0,
        tiled=True,
    ).astype(jnp.float32)
    resid = (residual.astype(jnp.float32) + mixed).astype(jnp.bfloat16)
    resid_f = resid.astype(jnp.float32)
    normed = (
        resid_f
        * lax.rsqrt(jnp.mean(resid_f * resid_f, axis=-1, keepdims=True) + norm_eps)
        * ffn_gain
    ).astype(jnp.bfloat16)
    side_w, side_down = shared_slice(shared_gate, shared_up, shared_down)
    sp_count = lax.axis_size("sp")
    chosen = expert_ids[:, :, None] == jnp.arange(sp_count, dtype=jnp.int32)
    table = jnp.sum(jnp.where(chosen, expert_weight[:, :, None], 0.0), axis=1)
    scales = lax.all_to_all(table.T, "sp", split_axis=0, concat_axis=0, tiled=True)
    part_rows = row_count // PARTS
    sums = []
    for part in range(PARTS):
        begin = part * part_rows
        gathered = lax.all_gather(normed[begin : begin + part_rows], "sp", axis=0, tiled=True)
        scale = scales[:, begin : begin + part_rows].reshape(-1, 1)
        produced = run_experts(
            gathered, scale, exp_gate[0], exp_up[0], exp_down[0], side_w, side_down
        )
        sums.append(lax.psum_scatter(produced, "sp", scatter_dimension=0, tiled=True))
    added = jnp.concatenate(sums, axis=0)
    return (resid.astype(jnp.float32) + added.astype(jnp.float32)).astype(jnp.bfloat16)


MESH = pl.DeviceIdType.MESH
QB = 128
NEG = -1e30
LINE = 4


def layer_kernel(
    ids_in, wts_in, marks_in, sink_ref, q_in, k_in, v_in, wo_in, res_in, gain_ref,
    eg_in, eu_in, ed_in, sg_in, su_in, sd_in,
    out_ref,
    q_s, kx, vx, marks, kk, vv, a_out, a_own, a_in, wo_own, wo_oth, res, tok, ids, wts, tab, tabt,
    gs, us, ds, hid, acc, base, stage, rbuf, sg, su, sd, sh, ost,
    loc, halo_s, halo_r, tab_s, tab_r, wx_s, wx_r, wz_s, wz_r, wf_s, wf_r, wg_s, wg_r, att_s, att_r,
    sib_s, sib_r, y_s, y_r, x_s, x_r, fy_s, fy_r, fx_s, fx_r,
    ag_s, ag_r, rs_s, rs_r, sx_s, sx_r, ss_s, ss_r, out_sem,
):
    f32, bf16 = jnp.float32, jnp.bfloat16
    sp_count, tp_count = lax.axis_size("sp"), lax.axis_size("tp")
    s, x = lax.axis_index("sp"), lax.axis_index("tp")
    z, y, c = s // 4, lax.rem(s // 2, 2), lax.rem(s, 2)
    ox, oy, oc = 1 - x, 1 - y, 1 - c
    at = lambda zz, yy, cc: (zz * 2 + yy) * 2 + cc
    dev = lambda sp, tp: {"sp": sp, "tp": tp}
    sib, ypar, xpar = dev(at(z, y, oc), x), dev(at(z, oy, c), x), dev(s, ox)
    nxt, prv = dev(lax.rem(s + 1, sp_count), x), dev(lax.rem(s + sp_count - 1, sp_count), x)
    low = z < 2
    w = jnp.where(low, z, 3 - z)
    inner = w == 1
    zf = jnp.where(low, z + 1, z - 1)
    zb = jnp.clip(jnp.where(low, z - 1, z + 1), 0, 3)
    fwd, bck = dev(at(zf, y, c), x), dev(at(zb, y, c), x)
    line = lambda ob: jnp.where(low, ob, 3 - ob)
    tokens = q_in.shape[0]
    half = tokens // 2
    width = res_in.shape[1]
    ff = eg_in.shape[2]
    part = width // 4

    def send(src, dst, ss, rs, to):
        cp = pltpu.make_async_remote_copy(
            src_ref=src, dst_ref=dst, send_sem=ss, recv_sem=rs, device_id=to, device_id_type=MESH
        )
        cp.start()
        return cp

    def got(view, rs):
        pltpu.make_async_remote_copy(
            src_ref=view, dst_ref=view, send_sem=rs, recv_sem=rs, device_id=sib, device_id_type=MESH
        ).wait_recv()

    def sent(view, ss):
        pltpu.make_async_remote_copy(
            src_ref=view, dst_ref=view, send_sem=ss, recv_sem=ss, device_id=sib, device_id_type=MESH
        ).wait_send()

    def load(src, dst, sem):
        cp = pltpu.make_async_copy(src, dst, sem)
        cp.start()
        return cp

    rows_own = pl.ds(QB, tokens)
    loads_a = [
        load(q_in, q_s, loc.at[0]),
        load(k_in, kx.at[rows_own], loc.at[1]),
        load(v_in, vx.at[rows_own], loc.at[2]),
        load(marks_in, marks.at[pl.ds(1, tokens // QB)], loc.at[3]),
        load(ids_in, ids, loc.at[6]),
        load(wts_in, wts, loc.at[16]),
    ]
    loads_b = [
        load(wo_in, wo_own, loc.at[4]),
        load(res_in, res, loc.at[5]),
        load(eg_in.at[0], gs.at[0], loc.at[7]),
        load(eu_in.at[0], us.at[0], loc.at[8]),
        load(sg_in, sg.at[0], loc.at[9]),
        load(su_in, su.at[0], loc.at[10]),
        load(sd_in, sd.at[pl.ds(0, sd_in.shape[0])], loc.at[11]),
    ]
    for n in range(4):
        loads_b.append(
            load(ed_in.at[0, :, pl.ds(n * part, part)], ds.at[n, pl.ds(0, ff)], loc.at[12 + n])
        )

    barrier = pltpu.get_barrier_semaphore()
    zs = [lax.rem(z + i, LINE) for i in range(1, LINE)]
    partners = [nxt, prv, sib, ypar, xpar] + [dev(at(zz, y, c), x) for zz in zs]
    for to in partners:
        pl.semaphore_signal(barrier, inc=1, device_id=to, device_id_type=MESH)
    pl.semaphore_wait(barrier, len(partners))

    pend = []
    last, first = pl.ds(tokens - QB, QB), pl.ds(0, QB)
    after = pl.ds(QB + tokens, QB)
    nb = tokens // QB
    for i, (src, dst, lo, hi, a, b) in enumerate(
        [(k_in, kx, first, after, last, first), (v_in, vx, first, after, last, first)]
    ):
        pend.append(send(src.at[a], dst.at[lo], halo_s.at[2 * i], halo_r.at[2 * i], nxt))
        pend.append(send(src.at[b], dst.at[hi], halo_s.at[2 * i + 1], halo_r.at[2 * i + 1], prv))
    pend.append(send(marks_in.at[nb - 1], marks.at[0], halo_s.at[4], halo_r.at[4], nxt))
    pend.append(send(marks_in.at[0], marks.at[nb + 1], halo_s.at[5], halo_r.at[5], prv))

    pair = dev(at(jnp.where(inner, zb, zf), y, c), x)
    wrows = wo_in.shape[0] // 8
    wpiece = lambda pos, core, i: pl.ds(pl.multiple_of(((pos * 2 + core) * 2 + i) * wrows, wrows), wrows)
    for i in range(2):
        rows = wpiece(w, c, i)
        pend.append(send(wo_in.at[rows], wo_oth.at[rows], wx_s.at[i], wx_r.at[i], xpar))

    def wx_event(i):
        view = wo_oth.at[wpiece(w, c, i)]
        got(view, wx_r.at[i])
        pend.append(send(view, view, wz_s.at[i], wz_r.at[i], pair))
        pend.append(send(view, view, wf_s.at[i], wf_r.at[i], sib))

    def wz_event(i):
        view = wo_oth.at[wpiece(1 - w, c, i)]
        got(view, wz_r.at[i])
        pend.append(send(view, view, wg_s.at[i], wg_r.at[i], sib))

    quarter = width // 4

    def piece(refs, kind, i, slot):
        g, u, d = refs
        if kind == "g":
            return g.at[slot, pl.ds(i * quarter, quarter)]
        if kind == "u":
            return u.at[slot, pl.ds(i * quarter, quarter)]
        if slot is None:
            return d.at[0, :, pl.ds(i * part, part)]
        return d.at[i, pl.ds(slot * ff, ff)]

    def hbm_piece(kind, i):
        if kind == "g":
            return eg_in.at[0, pl.ds(i * quarter, quarter)]
        if kind == "u":
            return eu_in.at[0, pl.ds(i * quarter, quarter)]
        return ed_in.at[0, :, pl.ds(pl.multiple_of(i * part, part), part)]

    held = (gs, us, ds)
    own_only = lambda v: [
        ("g", 2 * v), ("g", 2 * v + 1), ("u", 2 * v), ("u", 2 * v + 1), ("d", v), ("d", 2 + v)
    ]
    y_list, x_list = own_only(x), own_only(ox)
    for i, (kind, j) in enumerate(y_list):
        pend.append(send(hbm_piece(kind, j), piece(held, kind, j, 2), y_s.at[i], y_r.at[i], ypar))
    pend.append(send(eg_in.at[0], gs.at[1], sib_s.at[0], sib_r.at[0], sib))
    pend.append(send(eu_in.at[0], us.at[1], sib_s.at[1], sib_r.at[1], sib))
    for n in range(4):
        pend.append(
            send(hbm_piece("d", n), piece(held, "d", n, 1), sib_s.at[2 + n], sib_r.at[2 + n], sib)
        )

    def y_event(i):
        kind, j = y_list[i]
        view = piece(held, kind, j, 2)
        got(view, y_r.at[i])
        pend.append(send(view, view, x_s.at[i], x_r.at[i], xpar))
        pend.append(send(view, piece(held, kind, j, 3), fy_s.at[i], fy_r.at[i], sib))

    def x_event(i):
        kind, j = x_list[i]
        view = piece(held, kind, j, 2)
        got(view, x_r.at[i])
        pend.append(send(view, piece(held, kind, j, 3), fx_s.at[i], fx_r.at[i], sib))

    for cp in loads_a:
        cp.wait()
    lanes = lax.broadcasted_iota(jnp.int32, (half, QB), 1)
    table = jnp.zeros((half, QB), f32)
    for k in range(ids.shape[1]):
        table = table + jnp.where(lanes == ids[:, k : k + 1], wts[:, k : k + 1], 0.0)
    tabt[z] = table
    tab[z] = table.T[: tab.shape[1]]
    for i, zz in enumerate(zs):
        pend.append(
            send(tab.at[z], tab.at[z], tab_s.at[i], tab_r.at[LINE - 2 - i], dev(at(zz, y, c), x))
        )
    for i in range(2):
        dst = (kx, vx)[i]
        got(dst.at[first], halo_r.at[2 * i])
        got(dst.at[after], halo_r.at[2 * i + 1])
    got(marks.at[0], halo_r.at[4])
    got(marks.at[nb + 1], halo_r.at[5])

    @pl.when(s == 0)
    def _():
        marks[0] = jnp.full(marks.shape[1:], -1, jnp.int32)

    @pl.when(s == sp_count - 1)
    def _():
        marks[nb + 1] = jnp.full(marks.shape[1:], -1, jnp.int32)

    ri = lax.broadcasted_iota(jnp.int32, (QB, QB), 0)
    ci = lax.broadcasted_iota(jnp.int32, (QB, QB), 1)
    swap = jnp.where(ci == lax.rem(ri + HD, QB), 1.0, 0.0).astype(bf16)

    def spread(t, carry):
        rows = pl.ds(pl.multiple_of(t * QB, QB), QB)
        for src, dst in ((kx, kk), (vx, vv)):
            cur = src[rows]
            turned = jnp.dot(cur, swap, preferred_element_type=f32)
            cur = cur.astype(f32)
            zero = jnp.zeros_like(cur)
            left = ci < HD
            dst[0, rows] = jnp.where(left, cur, zero).astype(bf16)
            dst[1, rows] = jnp.where(left, zero, turned).astype(bf16)
            dst[2, rows] = jnp.where(left, turned, zero).astype(bf16)
            dst[3, rows] = jnp.where(left, zero, cur).astype(bf16)
        return carry

    lax.fori_loop(0, nb + 2, spread, 0)

    def attend_rows(blk, dst, drow):
        rows = pl.ds(pl.multiple_of(blk * QB, QB), QB)
        span = pl.ds(pl.multiple_of(blk * QB, QB), 3 * QB)
        mine = jnp.broadcast_to(marks[blk + 1][0:1], (QB, QB)).T
        biases = []
        for t in range(3):
            same = mine == jnp.broadcast_to(marks[blk + t][0:1], (QB, QB))
            if t == 0:
                same = same & (ri <= ci)
            if t == 2:
                same = same & (ci <= ri)
            biases.append(jnp.where(same, 0.0, NEG).astype(f32))
        bias = jnp.concatenate(biases, axis=1)
        for j in range(q_s.shape[1] // QB):
            g = j // 2
            keys2 = jnp.concatenate([kk[2 * g, span], kk[2 * g + 1, span]], axis=0)
            vals2 = jnp.concatenate([vv[2 * g, span], vv[2 * g + 1, span]], axis=0)
            sc = lax.dot_general(
                q_s[rows, j * QB : (j + 1) * QB], keys2, (((1,), (1,)), ((), ())),
                preferred_element_type=f32,
            ) * HD ** (-0.5)
            probs = []
            for h in range(2):
                sink = sink_ref[2 * j + h]
                own = sc[:, h * 3 * QB : (h + 1) * 3 * QB] + bias
                top = jnp.maximum(jnp.max(own, axis=-1, keepdims=True), sink)
                e = jnp.exp(own - top)
                total = jnp.sum(e, axis=-1, keepdims=True) + jnp.exp(sink - top)
                probs.append((e * (1.0 / total)).astype(bf16))
            o = jnp.dot(jnp.concatenate(probs, axis=1), vals2, preferred_element_type=f32)
            dst[pl.ds(pl.multiple_of(drow, QB), QB), j * QB : (j + 1) * QB] = o.astype(bf16)

    hb = half // QB

    for i in range(hb):
        attend_rows(ox * hb + i, a_out, i * QB)
        rows = pl.ds(i * QB, QB)
        pend.append(send(a_out.at[rows], a_in.at[rows], att_s.at[i], att_r.at[i], xpar))
        if i == 0:
            wx_event(0)
    for i in range(hb):
        attend_rows(x * hb + i, a_own, i * QB)

    wx_event(1)
    y_event(0)
    for cp in loads_b:
        cp.wait()
    for n in range(4):
        cols = slice(n * part, (n + 1) * part)
        base[n] = res[:, cols].astype(f32) + jnp.dot(
            a_own[...], wo_own[:, cols], preferred_element_type=f32
        )
    wz_event(0)
    for i in range(hb):
        got(a_in.at[pl.ds(i * QB, QB)], att_r.at[i])
    wz_event(1)
    for i in range(2):
        got(wo_oth.at[wpiece(w, oc, i)], wf_r.at[i])
        got(wo_oth.at[wpiece(1 - w, oc, i)], wg_r.at[i])
    square = jnp.zeros((half, 1), f32)
    for n in range(4):
        cols = slice(n * part, (n + 1) * part)
        r = (
            base[n] + jnp.dot(a_in[...], wo_oth[:, cols], preferred_element_type=f32)
        ).astype(bf16)
        res[:, cols] = r
        rf = r.astype(f32)
        square = square + jnp.sum(rf * rf, axis=-1, keepdims=True)
    inv = lax.rsqrt(square * (1.0 / width) + norm_eps)
    for n in range(4):
        cols = slice(n * part, (n + 1) * part)
        tok[z, :, cols] = (res[:, cols].astype(f32) * inv * gain_ref[:, cols]).astype(bf16)

    hr = half // 2
    rows_of = lambda r: pl.ds(r * hr, hr)

    def ag_send(b, r, direction, to):
        view = tok.at[b, rows_of(r)]
        send(view, view, ag_s.at[direction, b, r], ag_r.at[b, r], to)

    def ag_sent(b, r, direction):
        sent(tok.at[b, rows_of(r)], ag_s.at[direction, b, r])

    def ag_got(b, r):
        got(tok.at[b, rows_of(r)], ag_r.at[b, r])

    for r in range(2):
        ag_send(z, r, 0, fwd)

        @pl.when(inner)
        def _():
            ag_send(z, r, 1, bck)

    def relay(ob, r):
        b = line(ob)

        @pl.when(inner)
        def _():
            ag_got(b, r)
            if ob == 0:
                ag_send(b, r, 0, fwd)
            else:
                ag_send(b, r, 1, bck)

    def table_columns(i, carry):
        b = lax.rem(z + i, LINE)
        t = tab[b]
        grown = jnp.concatenate([t, jnp.zeros((QB - t.shape[0], t.shape[1]), f32)], axis=0)
        tabt[b] = grown.T
        return carry

    def gated(rows, gate, up):
        a = jnp.dot(rows, gate, preferred_element_type=f32)
        b = jnp.dot(rows, up, preferred_element_type=f32)
        return a / (1.0 + jnp.exp(-a)) * b

    def hidden(b, lo, hi):
        def one(slot, carry):
            e = at(z, jnp.where(slot >= 2, oy, y), jnp.where(lax.rem(slot, 2) == 1, oc, c))
            scale = jnp.sum(jnp.where(lanes == e, tabt[b], 0.0), axis=-1, keepdims=True)
            for h in range(2):
                cols = slice(h * (ff // 2), (h + 1) * (ff // 2))
                v = gated(tok[b], gs[slot, :, cols], us[slot, :, cols]) * scale
                to = pl.ds(pl.multiple_of(slot * ff + h * (ff // 2), ff // 2), ff // 2)
                hid[b, :, to] = v.astype(bf16)
            return carry

        lax.fori_loop(lo, hi, one, 0)

    y_event(1)
    for i in range(LINE - 1):
        got(tab.at[z], tab_r.at[i])
    lax.fori_loop(1, LINE, table_columns, 0)
    got(gs.at[1], sib_r.at[0])
    got(us.at[1], sib_r.at[1])
    hidden(z, 0, 2)
    relay(0, 0)
    relay(2, 0)
    x_event(0)
    y_event(2)
    x_event(1)
    relay(0, 1)
    relay(2, 1)
    y_event(3)
    near, far2, far3 = line(1 - w), line(2), line(3)

    def end_got(b):
        @pl.when(w == 0)
        def _():
            ag_got(b, 0)
            ag_got(b, 1)

    end_got(near)
    hidden(near, 0, 2)
    x_event(2)
    relay(3, 0)
    y_event(4)
    x_event(3)
    relay(3, 1)
    for i in range(4):
        kind, j = y_list[i]
        got(piece(held, kind, j, 3), fy_r.at[i])
        kind, j = x_list[i]
        got(piece(held, kind, j, 3), fx_r.at[i])
    hidden(near, 2, 4)
    for n in range(4):
        got(piece(held, "d", n, 1), sib_r.at[2 + n])
    srow, drow = sg_in.shape[0] // 2, sd_in.shape[0] // 2
    shared_views = lambda core: [
        sg.at[1, pl.ds(core * srow, srow)],
        su.at[1, pl.ds(core * srow, srow)],
        sd.at[pl.ds(sd_in.shape[0] + core * drow, drow)],
    ]
    shared_parts = [
        sg_in.at[pl.ds(c * srow, srow)],
        su_in.at[pl.ds(c * srow, srow)],
        sd_in.at[pl.ds(c * drow, drow)],
    ]

    order = [x, 2 + x, ox, 2 + ox]
    tile = lambda slot, n: rbuf.at[slot, n]

    def down(b, n):
        return jnp.dot(hid[b], ds[n], preferred_element_type=f32)

    def reduce_piece(step, n, place=None):
        b = jnp.where(step == 2, near, line(2 + step))
        slot = jnp.where(step == 0, 3 * w, jnp.where(step == 1, 1 + w, 4 - w))
        zt = jnp.where((step == 2) & inner, zb, zf)

        def add():
            got(tile(step, n), rs_r.at[step, n])
            stage[step, n] = (acc[...] + rbuf[step, n].astype(f32)).astype(bf16)

        if place == "end":
            stage[step, n] = down(b, n).astype(bf16)
        else:
            acc[...] = down(b, n)
            if place == "inner":
                add()
            else:
                pl.when(inner)(add)

                @pl.when(w == 0)
                def _():
                    stage[step, n] = acc[...].astype(bf16)

        send(
            stage.at[step, n], tile(slot, n), rs_s.at[step, n], rs_r.at[slot, n], dev(at(zt, y, c), x)
        )

    def nth(k):
        base_n = jnp.where(k < 2, x, ox)
        return base_n + 2 * lax.rem(k, 2)

    def down_got(k):
        lst, sem = (y_list, fy_r) if k < 2 else (x_list, fx_r)
        kind, j = lst[4 + k % 2]
        got(piece(held, kind, j, 3), sem.at[4 + k % 2])

    def at_end(step, k):
        @pl.when(w == 0)
        def _():
            reduce_piece(step, order[k], "end")

    down_got(0)
    at_end(2, 0)
    end_got(far2)
    hidden(far2, 0, 4)
    at_end(0, 0)
    y_event(5)
    for i, (src, dst) in enumerate(zip(shared_parts, shared_views(c))):
        pend.append(send(src, dst, sx_s.at[i], sx_r.at[i], xpar))

    @pl.when(inner)
    def _():
        hidden(far3, 0, 4)

    down_got(1)
    at_end(0, 1)
    x_event(4)
    down_got(2)
    at_end(0, 2)
    hidden(z, 2, 4)
    x_event(5)
    down_got(3)
    at_end(0, 3)

    @pl.when(w == 0)
    def _():
        ag_got(far3, 0)
        ag_got(far3, 1)
        hidden(far3, 0, 4)

    @pl.when(inner)
    def _():
        def inner_a(k, carry):
            reduce_piece(0, nth(k), "inner")
            return carry

        lax.fori_loop(0, 4, inner_a, 0)

    def later(i, carry):
        first_two, odd = i < 2, (lax.rem(i, 2) == 1) & (i < 7)
        in_step = jnp.where(first_two | odd, 1, 2)
        in_k = jnp.where(first_two, i, jnp.where(odd, (i + 1) // 2, (i - 1) // 2))
        step = jnp.where(inner, in_step, jnp.where(i < 4, 1, 2))
        k = jnp.where(inner, in_k, jnp.where(i < 4, i, i - 3))
        reduce_piece(step, nth(k))
        return carry

    def own_sum(n, carry):
        cols = pl.ds(pl.multiple_of(n * part, part), part)
        base[n] = res[:, cols].astype(f32) + down(z, n)
        return carry

    lax.fori_loop(0, 1, later, 0)
    lax.fori_loop(0, 4, own_sum, 0)
    lax.fori_loop(1, 6, later, 0)

    for i, view in enumerate(shared_views(c)):
        got(view, sx_r.at[i])
        pend.append(send(view, view, ss_s.at[i], ss_r.at[i], sib))
    for i, view in enumerate(shared_views(oc)):
        got(view, ss_r.at[i])
    units = sg_in.shape[1]
    for h in range(2):
        sh[:, h * units : (h + 1) * units] = gated(tok[z], sg[h], su[h]).astype(bf16)

    def shared_sum(n, carry):
        cols = pl.ds(pl.multiple_of(n * part, part), part)
        base[n] = base[n] + jnp.dot(sh[...], sd[:, cols], preferred_element_type=f32)
        return carry

    lax.fori_loop(0, 4, shared_sum, 0)
    lax.fori_loop(6, 7 + w, later, 0)

    def final(k, carry):
        n = nth(k)
        cols = pl.ds(pl.multiple_of(n * part, part), part)
        got(tile(3, n), rs_r.at[3, n])
        acc[...] = base[n] + rbuf[3, n].astype(f32)

        @pl.when(inner)
        def _():
            got(tile(4, n), rs_r.at[4, n])
            acc[...] = acc[...] + rbuf[4, n].astype(f32)

        ost[n] = acc[...].astype(bf16)
        load(ost.at[n], out_ref.at[:, cols], out_sem.at[n])
        return carry

    lax.fori_loop(0, 4, final, 0)

    for cp in pend:
        cp.wait_send()
    for r in range(2):
        ag_sent(z, r, 0)

        @pl.when(inner)
        def _():
            ag_sent(z, r, 1)
            ag_sent(line(0), r, 0)
            ag_sent(line(2), r, 1)
            ag_sent(line(3), r, 1)

    for step in range(3):
        for n in range(4):
            sent(stage.at[step, n], rs_s.at[step, n])
    for n in range(4):
        pltpu.make_async_copy(ost.at[n], out_ref.at[:, pl.ds(n * part, part)], out_sem.at[n]).wait()


def fused_shards(
    queries, keys, values, doc_ids, sink_logit, w_out, residual, ffn_gain, expert_ids,
    expert_weight, exp_gate, exp_up, exp_down, shared_gate, shared_up, shared_down,
):
    bf16, f32 = jnp.bfloat16, jnp.float32
    experts = lax.axis_size("sp")
    tokens = queries.shape[0]
    nb = tokens // QB
    marks = doc_ids.reshape(nb, 1, QB)
    half, width = residual.shape
    ff = exp_gate.shape[2]
    part = width // 4
    units = shared_gate.shape[1]
    heads = queries.shape[1]
    vm = pltpu.VMEM
    dma = pltpu.SemaphoreType.DMA
    anyspace = pl.BlockSpec(memory_space=pl.ANY)
    scratch = [
        vm((tokens, heads), bf16),
        vm((tokens + 2 * QB, QB), bf16),
        vm((tokens + 2 * QB, QB), bf16),
        vm((nb + 2, 1, QB), jnp.int32),
        vm((4, tokens + 2 * QB, QB), bf16),
        vm((4, tokens + 2 * QB, QB), bf16),
        vm((half, heads), bf16),
        vm((half, heads), bf16),
        vm((half, heads), bf16),
        vm(w_out.shape, bf16),
        vm(w_out.shape, bf16),
        vm((half, width), bf16),
        vm((LINE, half, width), bf16),
        vm(expert_ids.shape, jnp.int32),
        vm(expert_weight.shape, f32),
        vm((LINE, experts, half), f32),
        vm((LINE, half, QB), f32),
        vm((4, width, ff), bf16),
        vm((4, width, ff), bf16),
        vm((4, 4 * ff, part), bf16),
        vm((LINE, half, 4 * ff), bf16),
        vm((half, part), f32),
        vm((4, half, part), f32),
        vm((3, 4, half, part), bf16),
        vm((5, 4, half, part), bf16),
        vm((2, width, units), bf16),
        vm((2, width, units), bf16),
        vm((2 * units, width), bf16),
        vm((half, 2 * units), bf16),
        vm((4, half, part), bf16),
        dma((17,)), dma((6,)), dma((6,)), dma((3,)), dma((3,)),
        *[dma((2,)) for _ in range(10)],
        *[dma((6,)) for _ in range(10)],
        dma((2, LINE, 2)), dma((LINE, 2)), dma((3, 4)), dma((5, 4)),
        dma((3,)), dma((3,)), dma((3,)), dma((3,)), dma((4,)),
    ]
    rows = LINE * half
    return pl.pallas_call(
        layer_kernel,
        out_shape=jax.ShapeDtypeStruct((half, width), bf16),
        in_specs=[anyspace] * 3 + [pl.BlockSpec(memory_space=pltpu.SMEM)]
        + [anyspace] * 5
        + [pl.BlockSpec(memory_space=pltpu.VMEM)]
        + [anyspace] * 6,
        out_specs=anyspace,
        scratch_shapes=scratch,
        compiler_params=pltpu.CompilerParams(
            collective_id=0, has_side_effects=True, vmem_limit_bytes=63 * 1024 * 1024
        ),
        cost_estimate=pl.CostEstimate(
            flops=24 * rows * width * ff, bytes_accessed=32 * width * ff, transcendentals=rows * ff
        ),
    )(
        expert_ids, expert_weight, marks, sink_logit, queries, keys, values, w_out, residual, ffn_gain.reshape(1, -1),
        exp_gate, exp_up, exp_down, shared_gate, shared_up, shared_down,
    )


def solution(mesh):
    fits = mesh.shape["tp"] == 2 and mesh.shape["sp"] == 4 * LINE
    placed = (
        P("sp", "tp"),
        P("sp", "tp"),
        P("sp", "tp"),
        P("sp"),
        P("tp"),
        P("tp", None),
        P(("sp", "tp"), None),
        P(),
        P(("sp", "tp"), None),
        P(("sp", "tp"), None),
        P("sp", None, None),
        P("sp", None, None),
        P("sp", None, None),
        P(None, "tp"),
        P(None, "tp"),
        P("tp", None),
    )
    return jax.shard_map(
        fused_shards if fits else shards, mesh=mesh, in_specs=placed, out_specs=P(("sp", "tp"), None), check_vma=False
    )
```

```python
import math

import jax
import jax.numpy as jnp
from jax import lax
from jax.experimental import pallas as pl
from jax.experimental.pallas import tpu as pltpu
from jax.sharding import PartitionSpec as P

HD = 64
WINDOW = 128
PARTS = 2


norm_eps = 1e-06


def extended(cells, sides, width):
    for axis, dim in sides:
        count = lax.axis_size(axis)
        ends = count - 1
        head = lax.slice_in_dim(cells, 0, width, axis=dim)
        tail = lax.slice_in_dim(cells, cells.shape[dim] - width, cells.shape[dim], axis=dim)
        cells = jnp.concatenate(
            [
                lax.ppermute(tail, axis, [(i, (i + 1) % count) for i in range(ends)]),
                cells,
                lax.ppermute(head, axis, [((i + 1) % count, i) for i in range(ends)]),
            ],
            axis=dim,
        )
    return cells


def band_blocks(padded, width):
    span_count = padded.shape[0] // width - 2
    shaped = padded.reshape((span_count + 2, width) + padded.shape[1:])
    return jnp.concatenate(
        [
            shaped[0:span_count:2],
            shaped[1 : span_count + 1 : 2],
            shaped[2 : span_count + 2 : 2],
            shaped[3 : span_count + 3 : 2],
        ],
        axis=1,
    )


def attend(queries, ext_keys, ext_values, ext_marks, own_marks, sink_logit):
    tok_count = queries.shape[0]
    head_count = sink_logit.shape[0]
    key_heads = ext_keys.shape[1] // HD
    group_size = head_count // key_heads
    query_span = 2 * WINDOW
    block_count = tok_count // query_span
    query_blocks = queries.reshape(block_count, query_span, key_heads, group_size, HD)
    key_blocks = band_blocks(ext_keys, WINDOW).reshape(block_count, 4 * WINDOW, key_heads, HD)
    value_blocks = band_blocks(ext_values, WINDOW).reshape(block_count, 4 * WINDOW, key_heads, HD)
    mark_blocks = band_blocks(ext_marks, WINDOW)
    query_marks = own_marks.reshape(block_count, query_span)
    scores = jnp.einsum(
        "nqkgd,nmkd->nkgqm", query_blocks, key_blocks, preferred_element_type=jnp.float32
    ) * HD ** (-0.5)
    offset = (
        jnp.arange(query_span, dtype=jnp.int32)[:, None]
        - jnp.arange(4 * WINDOW, dtype=jnp.int32)[None, :]
        + WINDOW
    )
    allowed = (jnp.abs(offset) <= WINDOW)[None] & (
        mark_blocks[:, None, :] == query_marks[:, :, None]
    )
    scores = jnp.where(allowed[:, None, None], scores, -jnp.inf)
    sink_term = sink_logit.reshape(key_heads, group_size)[None, :, :, None, None]
    row_max = jnp.maximum(jnp.max(scores, axis=-1, keepdims=True), sink_term)
    exp_scores = jnp.exp(scores - row_max)
    attn_probs = (
        exp_scores / (jnp.sum(exp_scores, axis=-1, keepdims=True) + jnp.exp(sink_term - row_max))
    ).astype(jnp.bfloat16)
    result = jnp.einsum(
        "nkgqm,nmkd->nqkgd", attn_probs, value_blocks, preferred_element_type=jnp.float32
    )
    return result.astype(jnp.bfloat16).reshape(tok_count, head_count * HD)


def expert_kernel(rows_ref, scale_ref, gate_ref, up_ref, down_ref, side_ref, side_down_ref, out_ref):
    rows = rows_ref[...]
    gated = jnp.dot(rows, gate_ref[...], preferred_element_type=jnp.float32)
    lifted = jnp.dot(rows, up_ref[...], preferred_element_type=jnp.float32)
    hidden = (gated / (1.0 + jnp.exp(-gated)) * lifted).astype(jnp.bfloat16)
    produced = jnp.dot(hidden, down_ref[...], preferred_element_type=jnp.float32)
    side = jnp.dot(rows, side_ref[...], preferred_element_type=jnp.float32)
    width = side.shape[1] // 2
    side_gate, side_up = side[:, :width], side[:, width:]
    side_hidden = (side_gate / (1.0 + jnp.exp(-side_gate)) * side_up).astype(jnp.bfloat16)
    shared = jnp.dot(side_hidden, side_down_ref[...], preferred_element_type=jnp.float32)
    out_ref[...] = (
        scale_ref[...] * produced.astype(jnp.bfloat16).astype(jnp.float32) + shared
    ).astype(jnp.bfloat16)


def run_experts(rows, scale, gate_w, up_w, down_w, side_w, side_down):
    count, width = rows.shape
    tile = math.gcd(count, 256)
    whole = lambda w: pl.BlockSpec(w.shape, lambda i: (0, 0))
    units = gate_w.shape[1] + side_w.shape[1] // 2
    return pl.pallas_call(
        expert_kernel,
        grid=(count // tile,),
        in_specs=[
            pl.BlockSpec((tile, width), lambda i: (i, 0)),
            pl.BlockSpec((tile, 1), lambda i: (i, 0)),
            whole(gate_w),
            whole(up_w),
            whole(down_w),
            whole(side_w),
            whole(side_down),
        ],
        out_specs=pl.BlockSpec((tile, width), lambda i: (i, 0)),
        out_shape=jax.ShapeDtypeStruct((count, width), jnp.bfloat16),
        compiler_params=pltpu.CompilerParams(
            dimension_semantics=("arbitrary",), vmem_limit_bytes=48 * 1024 * 1024
        ),
        cost_estimate=pl.CostEstimate(
            flops=6 * count * width * units,
            bytes_accessed=4 * count * width + 6 * units * width,
            transcendentals=count * units,
        ),
    )(rows, scale, gate_w, up_w, down_w, side_w, side_down)


def shared_slice(shared_gate, shared_up, shared_down):
    sp_count, tp_count = lax.axis_size("sp"), lax.axis_size("tp")
    own, side = lax.axis_index("tp"), lax.axis_index("sp")
    units = shared_gate.shape[1] * tp_count // sp_count
    per_owner = sp_count // tp_count
    owner, offset = side // per_owner, (side % per_owner) * units
    held = jnp.concatenate(
        [
            lax.dynamic_slice_in_dim(shared_gate, offset, units, axis=1).T,
            lax.dynamic_slice_in_dim(shared_up, offset, units, axis=1).T,
            lax.dynamic_slice_in_dim(shared_down, offset, units, axis=0),
        ],
        axis=0,
    )
    chosen = held
    for shift in range(1, tp_count):
        came = lax.ppermute(held, "tp", [(i, (i + shift) % tp_count) for i in range(tp_count)])
        chosen = jnp.where((own - shift) % tp_count == owner, came, chosen)
    padded = -(-units // 128) * 128
    grown = [
        jnp.pad(chosen[i * units : (i + 1) * units], ((0, padded - units), (0, 0))) for i in range(3)
    ]
    return jnp.concatenate(grown[:2], axis=0).T, grown[2]


def shards(
    queries,
    keys,
    values,
    doc_ids,
    sink_logit,
    w_out,
    residual,
    ffn_gain,
    expert_ids,
    expert_weight,
    exp_gate,
    exp_up,
    exp_down,
    shared_gate,
    shared_up,
    shared_down,
):
    marks = (doc_ids + 1).astype(jnp.bfloat16)
    kv = keys.shape[1]
    joined = jnp.concatenate(
        [keys, values, jnp.broadcast_to(marks[:, None], (marks.shape[0], 128))], axis=1
    )
    extended_all = extended(joined, (("sp", 0),), WINDOW)
    ext_keys, ext_values, ext_marks = (
        extended_all[:, :kv],
        extended_all[:, kv : 2 * kv],
        extended_all[:, 2 * kv],
    )
    attended = attend(queries, ext_keys, ext_values, ext_marks, marks, sink_logit)
    row_count = residual.shape[0]
    mixed = lax.psum_scatter(
        jnp.dot(attended, w_out, preferred_element_type=jnp.float32).astype(jnp.bfloat16),
        "tp",
        scatter_dimension=0,
        tiled=True,
    ).astype(jnp.float32)
    resid = (residual.astype(jnp.float32) + mixed).astype(jnp.bfloat16)
    resid_f = resid.astype(jnp.float32)
    normed = (
        resid_f
        * lax.rsqrt(jnp.mean(resid_f * resid_f, axis=-1, keepdims=True) + norm_eps)
        * ffn_gain
    ).astype(jnp.bfloat16)
    side_w, side_down = shared_slice(shared_gate, shared_up, shared_down)
    sp_count = lax.axis_size("sp")
    chosen = expert_ids[:, :, None] == jnp.arange(sp_count, dtype=jnp.int32)
    table = jnp.sum(jnp.where(chosen, expert_weight[:, :, None], 0.0), axis=1)
    scales = lax.all_to_all(table.T, "sp", split_axis=0, concat_axis=0, tiled=True)
    part_rows = row_count // PARTS
    sums = []
    for part in range(PARTS):
        begin = part * part_rows
        gathered = lax.all_gather(normed[begin : begin + part_rows], "sp", axis=0, tiled=True)
        scale = scales[:, begin : begin + part_rows].reshape(-1, 1)
        produced = run_experts(
            gathered, scale, exp_gate[0], exp_up[0], exp_down[0], side_w, side_down
        )
        sums.append(lax.psum_scatter(produced, "sp", scatter_dimension=0, tiled=True))
    added = jnp.concatenate(sums, axis=0)
    return (resid.astype(jnp.float32) + added.astype(jnp.float32)).astype(jnp.bfloat16)


MESH = pl.DeviceIdType.MESH
QB = 128
NEG = -1e30
LINE = 4


def layer_kernel(
    ids_in, wts_in, marks_in, sink_ref, q_in, k_in, v_in, wo_in, res_in, gain_ref,
    eg_in, eu_in, ed_in, sg_in, su_in, sd_in,
    out_ref,
    q_s, kx, vx, marks, kk, vv, a_out, a_own, a_in, wo_own, wo_oth, res, tok, ids, wts, tab, tabt,
    gs, us, ds, hid, acc, base, stage, rbuf, sg, su, sd, sh, ost,
    loc, halo_s, halo_r, tab_s, tab_r, wx_s, wx_r, wz_s, wz_r, wf_s, wf_r, wg_s, wg_r, att_s, att_r,
    sib_s, sib_r, y_s, y_r, x_s, x_r, fy_s, fy_r, fx_s, fx_r,
    ag_s, ag_r, rs_s, rs_r, sx_s, sx_r, ss_s, ss_r, out_sem,
):
    f32, bf16 = jnp.float32, jnp.bfloat16
    sp_count, tp_count = lax.axis_size("sp"), lax.axis_size("tp")
    s, x = lax.axis_index("sp"), lax.axis_index("tp")
    z, y, c = s // 4, lax.rem(s // 2, 2), lax.rem(s, 2)
    ox, oy, oc = 1 - x, 1 - y, 1 - c
    at = lambda zz, yy, cc: (zz * 2 + yy) * 2 + cc
    dev = lambda sp, tp: {"sp": sp, "tp": tp}
    sib, ypar, xpar = dev(at(z, y, oc), x), dev(at(z, oy, c), x), dev(s, ox)
    nxt, prv = dev(lax.rem(s + 1, sp_count), x), dev(lax.rem(s + sp_count - 1, sp_count), x)
    low = z < 2
    w = jnp.where(low, z, 3 - z)
    inner = w == 1
    zf = jnp.where(low, z + 1, z - 1)
    zb = jnp.clip(jnp.where(low, z - 1, z + 1), 0, 3)
    fwd, bck = dev(at(zf, y, c), x), dev(at(zb, y, c), x)
    line = lambda ob: jnp.where(low, ob, 3 - ob)
    tokens = q_in.shape[0]
    half = tokens // 2
    width = res_in.shape[1]
    ff = eg_in.shape[2]
    part = width // 4

    def send(src, dst, ss, rs, to):
        cp = pltpu.make_async_remote_copy(
            src_ref=src, dst_ref=dst, send_sem=ss, recv_sem=rs, device_id=to, device_id_type=MESH
        )
        cp.start()
        return cp

    def got(view, rs):
        pltpu.make_async_remote_copy(
            src_ref=view, dst_ref=view, send_sem=rs, recv_sem=rs, device_id=sib, device_id_type=MESH
        ).wait_recv()

    def sent(view, ss):
        pltpu.make_async_remote_copy(
            src_ref=view, dst_ref=view, send_sem=ss, recv_sem=ss, device_id=sib, device_id_type=MESH
        ).wait_send()

    def load(src, dst, sem):
        cp = pltpu.make_async_copy(src, dst, sem)
        cp.start()
        return cp

    rows_own = pl.ds(QB, tokens)
    loads_a = [
        load(q_in, q_s, loc.at[0]),
        load(k_in, kx.at[rows_own], loc.at[1]),
        load(v_in, vx.at[rows_own], loc.at[2]),
        load(marks_in, marks.at[pl.ds(1, tokens // QB)], loc.at[3]),
        load(ids_in, ids, loc.at[6]),
        load(wts_in, wts, loc.at[16]),
    ]
    loads_b = [
        load(wo_in, wo_own, loc.at[4]),
        load(res_in, res, loc.at[5]),
        load(eg_in.at[0], gs.at[0], loc.at[7]),
        load(eu_in.at[0], us.at[0], loc.at[8]),
        load(sg_in, sg.at[0], loc.at[9]),
        load(su_in, su.at[0], loc.at[10]),
        load(sd_in, sd.at[pl.ds(0, sd_in.shape[0])], loc.at[11]),
    ]
    for n in range(4):
        loads_b.append(
            load(ed_in.at[0, :, pl.ds(n * part, part)], ds.at[n, pl.ds(0, ff)], loc.at[12 + n])
        )

    barrier = pltpu.get_barrier_semaphore()
    zs = [lax.rem(z + i, LINE) for i in range(1, LINE)]
    partners = [nxt, prv, sib, ypar, xpar] + [dev(at(zz, y, c), x) for zz in zs]
    for to in partners:
        pl.semaphore_signal(barrier, inc=1, device_id=to, device_id_type=MESH)
    pl.semaphore_wait(barrier, len(partners))

    pend = []
    last, first = pl.ds(tokens - QB, QB), pl.ds(0, QB)
    after = pl.ds(QB + tokens, QB)
    nb = tokens // QB
    for i, (src, dst, lo, hi, a, b) in enumerate(
        [(k_in, kx, first, after, last, first), (v_in, vx, first, after, last, first)]
    ):
        pend.append(send(src.at[a], dst.at[lo], halo_s.at[2 * i], halo_r.at[2 * i], nxt))
        pend.append(send(src.at[b], dst.at[hi], halo_s.at[2 * i + 1], halo_r.at[2 * i + 1], prv))
    pend.append(send(marks_in.at[nb - 1], marks.at[0], halo_s.at[4], halo_r.at[4], nxt))
    pend.append(send(marks_in.at[0], marks.at[nb + 1], halo_s.at[5], halo_r.at[5], prv))

    pair = dev(at(jnp.where(inner, zb, zf), y, c), x)
    wrows = wo_in.shape[0] // 8
    wpiece = lambda pos, core, i: pl.ds(pl.multiple_of(((pos * 2 + core) * 2 + i) * wrows, wrows), wrows)
    for i in range(2):
        rows = wpiece(w, c, i)
        pend.append(send(wo_in.at[rows], wo_oth.at[rows], wx_s.at[i], wx_r.at[i], xpar))

    def wx_event(i):
        view = wo_oth.at[wpiece(w, c, i)]
        got(view, wx_r.at[i])
        pend.append(send(view, view, wz_s.at[i], wz_r.at[i], pair))
        pend.append(send(view, view, wf_s.at[i], wf_r.at[i], sib))

    def wz_event(i):
        view = wo_oth.at[wpiece(1 - w, c, i)]
        got(view, wz_r.at[i])
        pend.append(send(view, view, wg_s.at[i], wg_r.at[i], sib))

    quarter = width // 4

    def piece(refs, kind, i, slot):
        g, u, d = refs
        if kind == "g":
            return g.at[slot, pl.ds(i * quarter, quarter)]
        if kind == "u":
            return u.at[slot, pl.ds(i * quarter, quarter)]
        if slot is None:
            return d.at[0, :, pl.ds(i * part, part)]
        return d.at[i, pl.ds(slot * ff, ff)]

    def hbm_piece(kind, i):
        if kind == "g":
            return eg_in.at[0, pl.ds(i * quarter, quarter)]
        if kind == "u":
            return eu_in.at[0, pl.ds(i * quarter, quarter)]
        return ed_in.at[0, :, pl.ds(pl.multiple_of(i * part, part), part)]

    held = (gs, us, ds)
    own_only = lambda v: [
        ("g", 2 * v), ("g", 2 * v + 1), ("u", 2 * v), ("u", 2 * v + 1), ("d", v), ("d", 2 + v)
    ]
    y_list, x_list = own_only(x), own_only(ox)
    for i, (kind, j) in enumerate(y_list):
        pend.append(send(hbm_piece(kind, j), piece(held, kind, j, 2), y_s.at[i], y_r.at[i], ypar))
    pend.append(send(eg_in.at[0], gs.at[1], sib_s.at[0], sib_r.at[0], sib))
    pend.append(send(eu_in.at[0], us.at[1], sib_s.at[1], sib_r.at[1], sib))
    for n in range(4):
        pend.append(
            send(hbm_piece("d", n), piece(held, "d", n, 1), sib_s.at[2 + n], sib_r.at[2 + n], sib)
        )

    def y_event(i):
        kind, j = y_list[i]
        view = piece(held, kind, j, 2)
        got(view, y_r.at[i])
        pend.append(send(view, view, x_s.at[i], x_r.at[i], xpar))
        pend.append(send(view, piece(held, kind, j, 3), fy_s.at[i], fy_r.at[i], sib))

    def x_event(i):
        kind, j = x_list[i]
        view = piece(held, kind, j, 2)
        got(view, x_r.at[i])
        pend.append(send(view, piece(held, kind, j, 3), fx_s.at[i], fx_r.at[i], sib))

    for cp in loads_a:
        cp.wait()
    lanes = lax.broadcasted_iota(jnp.int32, (half, QB), 1)
    named = lax.broadcasted_iota(jnp.int32, tab.shape[1:], 0)
    table = jnp.zeros(tab.shape[1:], f32)
    for k in range(ids.shape[0]):
        table = table + jnp.where(named == ids[k : k + 1], wts[k : k + 1], 0.0)
    tab[z] = table
    for i, zz in enumerate(zs):
        pend.append(
            send(tab.at[z], tab.at[z], tab_s.at[i], tab_r.at[LINE - 2 - i], dev(at(zz, y, c), x))
        )
    for i in range(2):
        dst = (kx, vx)[i]
        got(dst.at[first], halo_r.at[2 * i])
        got(dst.at[after], halo_r.at[2 * i + 1])
    got(marks.at[0], halo_r.at[4])
    got(marks.at[nb + 1], halo_r.at[5])

    @pl.when(s == 0)
    def _():
        marks[0] = jnp.full(marks.shape[1:], -1, jnp.int32)

    @pl.when(s == sp_count - 1)
    def _():
        marks[nb + 1] = jnp.full(marks.shape[1:], -1, jnp.int32)

    ri = lax.broadcasted_iota(jnp.int32, (QB, QB), 0)
    ci = lax.broadcasted_iota(jnp.int32, (QB, QB), 1)
    swap = jnp.where(ci == lax.rem(ri + HD, QB), 1.0, 0.0).astype(bf16)

    def spread(t, carry):
        rows = pl.ds(pl.multiple_of(t * QB, QB), QB)
        for src, dst in ((kx, kk), (vx, vv)):
            cur = src[rows]
            turned = jnp.dot(cur, swap, preferred_element_type=f32)
            cur = cur.astype(f32)
            zero = jnp.zeros_like(cur)
            left = ci < HD
            dst[0, rows] = jnp.where(left, cur, zero).astype(bf16)
            dst[1, rows] = jnp.where(left, zero, turned).astype(bf16)
            dst[2, rows] = jnp.where(left, turned, zero).astype(bf16)
            dst[3, rows] = jnp.where(left, zero, cur).astype(bf16)
        return carry

    lax.fori_loop(0, nb + 2, spread, 0)

    def attend_rows(blk, dst, drow):
        rows = pl.ds(pl.multiple_of(blk * QB, QB), QB)
        span = pl.ds(pl.multiple_of(blk * QB, QB), 3 * QB)
        mine = jnp.broadcast_to(marks[blk + 1][0:1], (QB, QB)).T
        biases = []
        for t in range(3):
            same = mine == jnp.broadcast_to(marks[blk + t][0:1], (QB, QB))
            if t == 0:
                same = same & (ri <= ci)
            if t == 2:
                same = same & (ci <= ri)
            biases.append(jnp.where(same, 0.0, NEG).astype(f32))
        bias = jnp.concatenate(biases, axis=1)
        for j in range(q_s.shape[1] // QB):
            g = j // 2
            keys2 = jnp.concatenate([kk[2 * g, span], kk[2 * g + 1, span]], axis=0)
            vals2 = jnp.concatenate([vv[2 * g, span], vv[2 * g + 1, span]], axis=0)
            sc = lax.dot_general(
                q_s[rows, j * QB : (j + 1) * QB], keys2, (((1,), (1,)), ((), ())),
                preferred_element_type=f32,
            ) * HD ** (-0.5)
            probs = []
            for h in range(2):
                sink = sink_ref[2 * j + h]
                own = sc[:, h * 3 * QB : (h + 1) * 3 * QB] + bias
                top = jnp.maximum(jnp.max(own, axis=-1, keepdims=True), sink)
                e = jnp.exp(own - top)
                total = jnp.sum(e, axis=-1, keepdims=True) + jnp.exp(sink - top)
                probs.append((e * (1.0 / total)).astype(bf16))
            o = jnp.dot(jnp.concatenate(probs, axis=1), vals2, preferred_element_type=f32)
            dst[pl.ds(pl.multiple_of(drow, QB), QB), j * QB : (j + 1) * QB] = o.astype(bf16)

    hb = half // QB

    for i in range(hb):
        attend_rows(ox * hb + i, a_out, i * QB)
        rows = pl.ds(i * QB, QB)
        pend.append(send(a_out.at[rows], a_in.at[rows], att_s.at[i], att_r.at[i], xpar))
        if i == 0:
            wx_event(0)
    for i in range(hb):
        attend_rows(x * hb + i, a_own, i * QB)

    wx_event(1)
    y_event(0)
    for cp in loads_b:
        cp.wait()
    for n in range(4):
        cols = slice(n * part, (n + 1) * part)
        base[n] = res[:, cols].astype(f32) + jnp.dot(
            a_own[...], wo_own[:, cols], preferred_element_type=f32
        )
    wz_event(0)
    for i in range(hb):
        got(a_in.at[pl.ds(i * QB, QB)], att_r.at[i])
    wz_event(1)
    for i in range(2):
        got(wo_oth.at[wpiece(w, oc, i)], wf_r.at[i])
        got(wo_oth.at[wpiece(1 - w, oc, i)], wg_r.at[i])
    square = jnp.zeros((half, 1), f32)
    for n in range(4):
        cols = slice(n * part, (n + 1) * part)
        r = (
            base[n] + jnp.dot(a_in[...], wo_oth[:, cols], preferred_element_type=f32)
        ).astype(bf16)
        res[:, cols] = r
        rf = r.astype(f32)
        square = square + jnp.sum(rf * rf, axis=-1, keepdims=True)
    inv = lax.rsqrt(square * (1.0 / width) + norm_eps)
    for n in range(4):
        cols = slice(n * part, (n + 1) * part)
        tok[z, :, cols] = (res[:, cols].astype(f32) * inv * gain_ref[:, cols]).astype(bf16)

    hr = half // 2
    rows_of = lambda r: pl.ds(r * hr, hr)

    def ag_send(b, r, direction, to):
        view = tok.at[b, rows_of(r)]
        send(view, view, ag_s.at[direction, b, r], ag_r.at[b, r], to)

    def ag_sent(b, r, direction):
        sent(tok.at[b, rows_of(r)], ag_s.at[direction, b, r])

    def ag_got(b, r):
        got(tok.at[b, rows_of(r)], ag_r.at[b, r])

    for r in range(2):
        ag_send(z, r, 0, fwd)

        @pl.when(inner)
        def _():
            ag_send(z, r, 1, bck)

    def relay(ob, r):
        b = line(ob)

        @pl.when(inner)
        def _():
            ag_got(b, r)
            if ob == 0:
                ag_send(b, r, 0, fwd)
            else:
                ag_send(b, r, 1, bck)

    def table_columns(b, carry):
        t = tab[b]
        grown = jnp.concatenate([t, jnp.zeros((QB - t.shape[0], t.shape[1]), f32)], axis=0)
        tabt[b] = grown.T
        return carry

    def gated(rows, gate, up):
        a = jnp.dot(rows, gate, preferred_element_type=f32)
        b = jnp.dot(rows, up, preferred_element_type=f32)
        return a / (1.0 + jnp.exp(-a)) * b

    def hidden(b, lo, hi):
        def one(slot, carry):
            e = at(z, jnp.where(slot >= 2, oy, y), jnp.where(lax.rem(slot, 2) == 1, oc, c))
            scale = jnp.sum(jnp.where(lanes == e, tabt[b], 0.0), axis=-1, keepdims=True)
            for h in range(2):
                cols = slice(h * (ff // 2), (h + 1) * (ff // 2))
                v = gated(tok[b], gs[slot, :, cols], us[slot, :, cols]) * scale
                to = pl.ds(pl.multiple_of(slot * ff + h * (ff // 2), ff // 2), ff // 2)
                hid[b, :, to] = v.astype(bf16)
            return carry

        lax.fori_loop(lo, hi, one, 0)

    y_event(1)
    for i in range(LINE - 1):
        got(tab.at[z], tab_r.at[i])
    lax.fori_loop(0, LINE, table_columns, 0)
    got(gs.at[1], sib_r.at[0])
    got(us.at[1], sib_r.at[1])
    hidden(z, 0, 2)
    relay(0, 0)
    relay(2, 0)
    x_event(0)
    y_event(2)
    x_event(1)
    relay(0, 1)
    relay(2, 1)
    y_event(3)
    near, far2, far3 = line(1 - w), line(2), line(3)

    def end_got(b):
        @pl.when(w == 0)
        def _():
            ag_got(b, 0)
            ag_got(b, 1)

    end_got(near)
    hidden(near, 0, 2)
    x_event(2)
    relay(3, 0)
    y_event(4)
    x_event(3)
    relay(3, 1)
    for i in range(4):
        kind, j = y_list[i]
        got(piece(held, kind, j, 3), fy_r.at[i])
        kind, j = x_list[i]
        got(piece(held, kind, j, 3), fx_r.at[i])
    hidden(near, 2, 4)
    for n in range(4):
        got(piece(held, "d", n, 1), sib_r.at[2 + n])
    srow, drow = sg_in.shape[0] // 2, sd_in.shape[0] // 2
    shared_views = lambda core: [
        sg.at[1, pl.ds(core * srow, srow)],
        su.at[1, pl.ds(core * srow, srow)],
        sd.at[pl.ds(sd_in.shape[0] + core * drow, drow)],
    ]
    shared_parts = [
        sg_in.at[pl.ds(c * srow, srow)],
        su_in.at[pl.ds(c * srow, srow)],
        sd_in.at[pl.ds(c * drow, drow)],
    ]

    order = [x, 2 + x, ox, 2 + ox]
    tile = lambda slot, n: rbuf.at[slot, n]

    def down(b, n):
        return jnp.dot(hid[b], ds[n], preferred_element_type=f32)

    def reduce_piece(step, n, place=None):
        b = jnp.where(step == 2, near, line(2 + step))
        slot = jnp.where(step == 0, 3 * w, jnp.where(step == 1, 1 + w, 4 - w))
        zt = jnp.where((step == 2) & inner, zb, zf)

        def add():
            got(tile(step, n), rs_r.at[step, n])
            stage[step, n] = (acc[...] + rbuf[step, n].astype(f32)).astype(bf16)

        if place == "end":
            stage[step, n] = down(b, n).astype(bf16)
        else:
            acc[...] = down(b, n)
            if place == "inner":
                add()
            else:
                pl.when(inner)(add)

                @pl.when(w == 0)
                def _():
                    stage[step, n] = acc[...].astype(bf16)

        send(
            stage.at[step, n], tile(slot, n), rs_s.at[step, n], rs_r.at[slot, n], dev(at(zt, y, c), x)
        )

    def nth(k):
        base_n = jnp.where(k < 2, x, ox)
        return base_n + 2 * lax.rem(k, 2)

    def down_got(k):
        lst, sem = (y_list, fy_r) if k < 2 else (x_list, fx_r)
        kind, j = lst[4 + k % 2]
        got(piece(held, kind, j, 3), sem.at[4 + k % 2])

    def at_end(step, k):
        @pl.when(w == 0)
        def _():
            reduce_piece(step, order[k], "end")

    def at_inner(step, k):
        @pl.when(inner)
        def _():
            reduce_piece(step, order[k], "inner")

    down_got(0)
    at_end(2, 0)
    end_got(far2)
    hidden(far2, 0, 4)
    at_end(0, 0)
    y_event(5)
    for i, (src, dst) in enumerate(zip(shared_parts, shared_views(c))):
        pend.append(send(src, dst, sx_s.at[i], sx_r.at[i], xpar))

    @pl.when(inner)
    def _():
        hidden(far3, 0, 4)

    at_inner(0, 0)
    down_got(1)
    at_end(0, 1)
    x_event(4)
    down_got(2)
    at_end(0, 2)
    at_inner(0, 1)
    hidden(z, 2, 4)
    x_event(5)
    at_inner(0, 2)
    down_got(3)
    at_end(0, 3)
    at_inner(0, 3)

    @pl.when(w == 0)
    def _():
        ag_got(far3, 0)
        ag_got(far3, 1)
        hidden(far3, 0, 4)

    def later(i, carry):
        first_two, odd = i < 2, (lax.rem(i, 2) == 1) & (i < 7)
        in_step = jnp.where(first_two | odd, 1, 2)
        in_k = jnp.where(first_two, i, jnp.where(odd, (i + 1) // 2, (i - 1) // 2))
        step = jnp.where(inner, in_step, jnp.where(i < 4, 1, 2))
        k = jnp.where(inner, in_k, jnp.where(i < 4, i, i - 3))
        reduce_piece(step, nth(k))
        return carry

    def own_sum(n, carry):
        cols = pl.ds(pl.multiple_of(n * part, part), part)
        base[n] = res[:, cols].astype(f32) + down(z, n)
        return carry

    lax.fori_loop(0, 1, later, 0)
    lax.fori_loop(0, 4, own_sum, 0)
    lax.fori_loop(1, 7 + w, later, 0)

    for i, view in enumerate(shared_views(c)):
        got(view, sx_r.at[i])
        pend.append(send(view, view, ss_s.at[i], ss_r.at[i], sib))
    for i, view in enumerate(shared_views(oc)):
        got(view, ss_r.at[i])
    units = sg_in.shape[1]
    for h in range(2):
        sh[:, h * units : (h + 1) * units] = gated(tok[z], sg[h], su[h]).astype(bf16)

    def shared_sum(n, carry):
        cols = pl.ds(pl.multiple_of(n * part, part), part)
        base[n] = base[n] + jnp.dot(sh[...], sd[:, cols], preferred_element_type=f32)
        return carry

    lax.fori_loop(0, 4, shared_sum, 0)

    def final(k, carry):
        n = nth(k)
        cols = pl.ds(pl.multiple_of(n * part, part), part)
        got(tile(3, n), rs_r.at[3, n])
        acc[...] = base[n] + rbuf[3, n].astype(f32)

        @pl.when(inner)
        def _():
            got(tile(4, n), rs_r.at[4, n])
            acc[...] = acc[...] + rbuf[4, n].astype(f32)

        ost[n] = acc[...].astype(bf16)
        load(ost.at[n], out_ref.at[:, cols], out_sem.at[n])
        return carry

    lax.fori_loop(0, 4, final, 0)

    for cp in pend:
        cp.wait_send()
    for r in range(2):
        ag_sent(z, r, 0)

        @pl.when(inner)
        def _():
            ag_sent(z, r, 1)
            ag_sent(line(0), r, 0)
            ag_sent(line(2), r, 1)
            ag_sent(line(3), r, 1)

    for step in range(3):
        for n in range(4):
            sent(stage.at[step, n], rs_s.at[step, n])
    for n in range(4):
        pltpu.make_async_copy(ost.at[n], out_ref.at[:, pl.ds(n * part, part)], out_sem.at[n]).wait()


def fused_shards(
    queries, keys, values, doc_ids, sink_logit, w_out, residual, ffn_gain, expert_ids,
    expert_weight, exp_gate, exp_up, exp_down, shared_gate, shared_up, shared_down,
):
    bf16, f32 = jnp.bfloat16, jnp.float32
    experts = lax.axis_size("sp")
    tokens = queries.shape[0]
    nb = tokens // QB
    marks = doc_ids.reshape(nb, 1, QB)
    half, width = residual.shape
    ff = exp_gate.shape[2]
    part = width // 4
    units = shared_gate.shape[1]
    heads = queries.shape[1]
    vm = pltpu.VMEM
    dma = pltpu.SemaphoreType.DMA
    anyspace = pl.BlockSpec(memory_space=pl.ANY)
    scratch = [
        vm((tokens, heads), bf16),
        vm((tokens + 2 * QB, QB), bf16),
        vm((tokens + 2 * QB, QB), bf16),
        vm((nb + 2, 1, QB), jnp.int32),
        vm((4, tokens + 2 * QB, QB), bf16),
        vm((4, tokens + 2 * QB, QB), bf16),
        vm((half, heads), bf16),
        vm((half, heads), bf16),
        vm((half, heads), bf16),
        vm(w_out.shape, bf16),
        vm(w_out.shape, bf16),
        vm((half, width), bf16),
        vm((LINE, half, width), bf16),
        vm(expert_ids.shape[::-1], jnp.int32),
        vm(expert_weight.shape[::-1], f32),
        vm((LINE, experts, half), f32),
        vm((LINE, half, QB), f32),
        vm((4, width, ff), bf16),
        vm((4, width, ff), bf16),
        vm((4, 4 * ff, part), bf16),
        vm((LINE, half, 4 * ff), bf16),
        vm((half, part), f32),
        vm((4, half, part), f32),
        vm((3, 4, half, part), bf16),
        vm((5, 4, half, part), bf16),
        vm((2, width, units), bf16),
        vm((2, width, units), bf16),
        vm((2 * units, width), bf16),
        vm((half, 2 * units), bf16),
        vm((4, half, part), bf16),
        dma((17,)), dma((6,)), dma((6,)), dma((3,)), dma((3,)),
        *[dma((2,)) for _ in range(10)],
        *[dma((6,)) for _ in range(10)],
        dma((2, LINE, 2)), dma((LINE, 2)), dma((3, 4)), dma((5, 4)),
        dma((3,)), dma((3,)), dma((3,)), dma((3,)), dma((4,)),
    ]
    rows = LINE * half
    return pl.pallas_call(
        layer_kernel,
        out_shape=jax.ShapeDtypeStruct((half, width), bf16),
        in_specs=[anyspace] * 3 + [pl.BlockSpec(memory_space=pltpu.SMEM)]
        + [anyspace] * 5
        + [pl.BlockSpec(memory_space=pltpu.VMEM)]
        + [anyspace] * 6,
        out_specs=anyspace,
        scratch_shapes=scratch,
        compiler_params=pltpu.CompilerParams(
            collective_id=0, has_side_effects=True, vmem_limit_bytes=63 * 1024 * 1024
        ),
        cost_estimate=pl.CostEstimate(
            flops=24 * rows * width * ff, bytes_accessed=32 * width * ff, transcendentals=rows * ff
        ),
    )(
        expert_ids.T, expert_weight.T, marks, sink_logit, queries, keys, values, w_out, residual, ffn_gain.reshape(1, -1),
        exp_gate, exp_up, exp_down, shared_gate, shared_up, shared_down,
    )


def solution(mesh):
    fits = mesh.shape["tp"] == 2 and mesh.shape["sp"] == 4 * LINE
    placed = (
        P("sp", "tp"),
        P("sp", "tp"),
        P("sp", "tp"),
        P("sp"),
        P("tp"),
        P("tp", None),
        P(("sp", "tp"), None),
        P(),
        P(("sp", "tp"), None),
        P(("sp", "tp"), None),
        P("sp", None, None),
        P("sp", None, None),
        P("sp", None, None),
        P(None, "tp"),
        P(None, "tp"),
        P("tp", None),
    )
    return jax.shard_map(
        fused_shards if fits else shards, mesh=mesh, in_specs=placed, out_specs=P(("sp", "tp"), None), check_vma=False
    )
```

```python
import math

import jax
import jax.numpy as jnp
from jax import lax
from jax.experimental import pallas as pl
from jax.experimental.pallas import tpu as pltpu
from jax.sharding import PartitionSpec as P

HD = 64
WINDOW = 128
PARTS = 2


norm_eps = 1e-06


def extended(cells, sides, width):
    for axis, dim in sides:
        count = lax.axis_size(axis)
        ends = count - 1
        head = lax.slice_in_dim(cells, 0, width, axis=dim)
        tail = lax.slice_in_dim(cells, cells.shape[dim] - width, cells.shape[dim], axis=dim)
        cells = jnp.concatenate(
            [
                lax.ppermute(tail, axis, [(i, (i + 1) % count) for i in range(ends)]),
                cells,
                lax.ppermute(head, axis, [((i + 1) % count, i) for i in range(ends)]),
            ],
            axis=dim,
        )
    return cells


def band_blocks(padded, width):
    span_count = padded.shape[0] // width - 2
    shaped = padded.reshape((span_count + 2, width) + padded.shape[1:])
    return jnp.concatenate(
        [
            shaped[0:span_count:2],
            shaped[1 : span_count + 1 : 2],
            shaped[2 : span_count + 2 : 2],
            shaped[3 : span_count + 3 : 2],
        ],
        axis=1,
    )


def attend(queries, ext_keys, ext_values, ext_marks, own_marks, sink_logit):
    tok_count = queries.shape[0]
    head_count = sink_logit.shape[0]
    key_heads = ext_keys.shape[1] // HD
    group_size = head_count // key_heads
    query_span = 2 * WINDOW
    block_count = tok_count // query_span
    query_blocks = queries.reshape(block_count, query_span, key_heads, group_size, HD)
    key_blocks = band_blocks(ext_keys, WINDOW).reshape(block_count, 4 * WINDOW, key_heads, HD)
    value_blocks = band_blocks(ext_values, WINDOW).reshape(block_count, 4 * WINDOW, key_heads, HD)
    mark_blocks = band_blocks(ext_marks, WINDOW)
    query_marks = own_marks.reshape(block_count, query_span)
    scores = jnp.einsum(
        "nqkgd,nmkd->nkgqm", query_blocks, key_blocks, preferred_element_type=jnp.float32
    ) * HD ** (-0.5)
    offset = (
        jnp.arange(query_span, dtype=jnp.int32)[:, None]
        - jnp.arange(4 * WINDOW, dtype=jnp.int32)[None, :]
        + WINDOW
    )
    allowed = (jnp.abs(offset) <= WINDOW)[None] & (
        mark_blocks[:, None, :] == query_marks[:, :, None]
    )
    scores = jnp.where(allowed[:, None, None], scores, -jnp.inf)
    sink_term = sink_logit.reshape(key_heads, group_size)[None, :, :, None, None]
    row_max = jnp.maximum(jnp.max(scores, axis=-1, keepdims=True), sink_term)
    exp_scores = jnp.exp(scores - row_max)
    attn_probs = (
        exp_scores / (jnp.sum(exp_scores, axis=-1, keepdims=True) + jnp.exp(sink_term - row_max))
    ).astype(jnp.bfloat16)
    result = jnp.einsum(
        "nkgqm,nmkd->nqkgd", attn_probs, value_blocks, preferred_element_type=jnp.float32
    )
    return result.astype(jnp.bfloat16).reshape(tok_count, head_count * HD)


def expert_kernel(rows_ref, scale_ref, gate_ref, up_ref, down_ref, side_ref, side_down_ref, out_ref):
    rows = rows_ref[...]
    gated = jnp.dot(rows, gate_ref[...], preferred_element_type=jnp.float32)
    lifted = jnp.dot(rows, up_ref[...], preferred_element_type=jnp.float32)
    hidden = (gated / (1.0 + jnp.exp(-gated)) * lifted).astype(jnp.bfloat16)
    produced = jnp.dot(hidden, down_ref[...], preferred_element_type=jnp.float32)
    side = jnp.dot(rows, side_ref[...], preferred_element_type=jnp.float32)
    width = side.shape[1] // 2
    side_gate, side_up = side[:, :width], side[:, width:]
    side_hidden = (side_gate / (1.0 + jnp.exp(-side_gate)) * side_up).astype(jnp.bfloat16)
    shared = jnp.dot(side_hidden, side_down_ref[...], preferred_element_type=jnp.float32)
    out_ref[...] = (
        scale_ref[...] * produced.astype(jnp.bfloat16).astype(jnp.float32) + shared
    ).astype(jnp.bfloat16)


def run_experts(rows, scale, gate_w, up_w, down_w, side_w, side_down):
    count, width = rows.shape
    tile = math.gcd(count, 256)
    whole = lambda w: pl.BlockSpec(w.shape, lambda i: (0, 0))
    units = gate_w.shape[1] + side_w.shape[1] // 2
    return pl.pallas_call(
        expert_kernel,
        grid=(count // tile,),
        in_specs=[
            pl.BlockSpec((tile, width), lambda i: (i, 0)),
            pl.BlockSpec((tile, 1), lambda i: (i, 0)),
            whole(gate_w),
            whole(up_w),
            whole(down_w),
            whole(side_w),
            whole(side_down),
        ],
        out_specs=pl.BlockSpec((tile, width), lambda i: (i, 0)),
        out_shape=jax.ShapeDtypeStruct((count, width), jnp.bfloat16),
        compiler_params=pltpu.CompilerParams(
            dimension_semantics=("arbitrary",), vmem_limit_bytes=48 * 1024 * 1024
        ),
        cost_estimate=pl.CostEstimate(
            flops=6 * count * width * units,
            bytes_accessed=4 * count * width + 6 * units * width,
            transcendentals=count * units,
        ),
    )(rows, scale, gate_w, up_w, down_w, side_w, side_down)


def shared_slice(shared_gate, shared_up, shared_down):
    sp_count, tp_count = lax.axis_size("sp"), lax.axis_size("tp")
    own, side = lax.axis_index("tp"), lax.axis_index("sp")
    units = shared_gate.shape[1] * tp_count // sp_count
    per_owner = sp_count // tp_count
    owner, offset = side // per_owner, (side % per_owner) * units
    held = jnp.concatenate(
        [
            lax.dynamic_slice_in_dim(shared_gate, offset, units, axis=1).T,
            lax.dynamic_slice_in_dim(shared_up, offset, units, axis=1).T,
            lax.dynamic_slice_in_dim(shared_down, offset, units, axis=0),
        ],
        axis=0,
    )
    chosen = held
    for shift in range(1, tp_count):
        came = lax.ppermute(held, "tp", [(i, (i + shift) % tp_count) for i in range(tp_count)])
        chosen = jnp.where((own - shift) % tp_count == owner, came, chosen)
    padded = -(-units // 128) * 128
    grown = [
        jnp.pad(chosen[i * units : (i + 1) * units], ((0, padded - units), (0, 0))) for i in range(3)
    ]
    return jnp.concatenate(grown[:2], axis=0).T, grown[2]


def shards(
    queries,
    keys,
    values,
    doc_ids,
    sink_logit,
    w_out,
    residual,
    ffn_gain,
    expert_ids,
    expert_weight,
    exp_gate,
    exp_up,
    exp_down,
    shared_gate,
    shared_up,
    shared_down,
):
    marks = (doc_ids + 1).astype(jnp.bfloat16)
    kv = keys.shape[1]
    joined = jnp.concatenate(
        [keys, values, jnp.broadcast_to(marks[:, None], (marks.shape[0], 128))], axis=1
    )
    extended_all = extended(joined, (("sp", 0),), WINDOW)
    ext_keys, ext_values, ext_marks = (
        extended_all[:, :kv],
        extended_all[:, kv : 2 * kv],
        extended_all[:, 2 * kv],
    )
    attended = attend(queries, ext_keys, ext_values, ext_marks, marks, sink_logit)
    row_count = residual.shape[0]
    mixed = lax.psum_scatter(
        jnp.dot(attended, w_out, preferred_element_type=jnp.float32).astype(jnp.bfloat16),
        "tp",
        scatter_dimension=0,
        tiled=True,
    ).astype(jnp.float32)
    resid = (residual.astype(jnp.float32) + mixed).astype(jnp.bfloat16)
    resid_f = resid.astype(jnp.float32)
    normed = (
        resid_f
        * lax.rsqrt(jnp.mean(resid_f * resid_f, axis=-1, keepdims=True) + norm_eps)
        * ffn_gain
    ).astype(jnp.bfloat16)
    side_w, side_down = shared_slice(shared_gate, shared_up, shared_down)
    sp_count = lax.axis_size("sp")
    chosen = expert_ids[:, :, None] == jnp.arange(sp_count, dtype=jnp.int32)
    table = jnp.sum(jnp.where(chosen, expert_weight[:, :, None], 0.0), axis=1)
    scales = lax.all_to_all(table.T, "sp", split_axis=0, concat_axis=0, tiled=True)
    part_rows = row_count // PARTS
    sums = []
    for part in range(PARTS):
        begin = part * part_rows
        gathered = lax.all_gather(normed[begin : begin + part_rows], "sp", axis=0, tiled=True)
        scale = scales[:, begin : begin + part_rows].reshape(-1, 1)
        produced = run_experts(
            gathered, scale, exp_gate[0], exp_up[0], exp_down[0], side_w, side_down
        )
        sums.append(lax.psum_scatter(produced, "sp", scatter_dimension=0, tiled=True))
    added = jnp.concatenate(sums, axis=0)
    return (resid.astype(jnp.float32) + added.astype(jnp.float32)).astype(jnp.bfloat16)


MESH = pl.DeviceIdType.MESH
QB = 128
NEG = -1e30
LINE = 4
WO_PIECES = 4


def layer_kernel(
    ids_in, wts_in, marks_in, sink_ref, q_in, k_in, v_in, wo_in, res_in, gain_ref,
    eg_in, eu_in, ed_in, sg_in, su_in, sd_in,
    out_ref,
    q_s, kx, vx, marks, kk, vv, a_out, a_own, a_in, wo_own, wo_oth, res, tok, ids, wts, tab, tabt,
    gs, us, ds, hid, acc, base, stage, rbuf, sg, su, sd, sh, ost,
    loc, halo_s, halo_r, tab_s, tab_r, wx_s, wx_r, wz_s, wz_r, wf_s, wf_r, wg_s, wg_r, att_s, att_r,
    sib_s, sib_r, y_s, y_r, x_s, x_r, fy_s, fy_r, fx_s, fx_r,
    ag_s, ag_r, rs_s, rs_r, sx_s, sx_r, ss_s, ss_r, out_sem,
):
    f32, bf16 = jnp.float32, jnp.bfloat16
    sp_count, tp_count = lax.axis_size("sp"), lax.axis_size("tp")
    s, x = lax.axis_index("sp"), lax.axis_index("tp")
    z, y, c = s // 4, lax.rem(s // 2, 2), lax.rem(s, 2)
    ox, oy, oc = 1 - x, 1 - y, 1 - c
    at = lambda zz, yy, cc: (zz * 2 + yy) * 2 + cc
    dev = lambda sp, tp: {"sp": sp, "tp": tp}
    sib, ypar, xpar = dev(at(z, y, oc), x), dev(at(z, oy, c), x), dev(s, ox)
    nxt, prv = dev(lax.rem(s + 1, sp_count), x), dev(lax.rem(s + sp_count - 1, sp_count), x)
    low = z < 2
    w = jnp.where(low, z, 3 - z)
    inner = w == 1
    zf = jnp.where(low, z + 1, z - 1)
    zb = jnp.clip(jnp.where(low, z - 1, z + 1), 0, 3)
    fwd, bck = dev(at(zf, y, c), x), dev(at(zb, y, c), x)
    line = lambda ob: jnp.where(low, ob, 3 - ob)
    tokens = q_in.shape[0]
    half = tokens // 2
    width = res_in.shape[1]
    ff = eg_in.shape[2]
    part = width // 4

    def send(src, dst, ss, rs, to):
        cp = pltpu.make_async_remote_copy(
            src_ref=src, dst_ref=dst, send_sem=ss, recv_sem=rs, device_id=to, device_id_type=MESH
        )
        cp.start()
        return cp

    def got(view, rs):
        pltpu.make_async_remote_copy(
            src_ref=view, dst_ref=view, send_sem=rs, recv_sem=rs, device_id=sib, device_id_type=MESH
        ).wait_recv()

    def sent(view, ss):
        pltpu.make_async_remote_copy(
            src_ref=view, dst_ref=view, send_sem=ss, recv_sem=ss, device_id=sib, device_id_type=MESH
        ).wait_send()

    def load(src, dst, sem):
        cp = pltpu.make_async_copy(src, dst, sem)
        cp.start()
        return cp

    rows_own = pl.ds(QB, tokens)
    loads_a = [
        load(q_in, q_s, loc.at[0]),
        load(k_in, kx.at[rows_own], loc.at[1]),
        load(v_in, vx.at[rows_own], loc.at[2]),
        load(marks_in, marks.at[pl.ds(1, tokens // QB)], loc.at[3]),
        load(ids_in, ids, loc.at[6]),
        load(wts_in, wts, loc.at[16]),
    ]
    loads_b = [
        load(wo_in, wo_own, loc.at[4]),
        load(res_in, res, loc.at[5]),
        load(eg_in.at[0], gs.at[0], loc.at[7]),
        load(eu_in.at[0], us.at[0], loc.at[8]),
        load(sg_in, sg.at[0], loc.at[9]),
        load(su_in, su.at[0], loc.at[10]),
        load(sd_in, sd.at[pl.ds(0, sd_in.shape[0])], loc.at[11]),
    ]
    for n in range(4):
        loads_b.append(
            load(ed_in.at[0, :, pl.ds(n * part, part)], ds.at[n, pl.ds(0, ff)], loc.at[12 + n])
        )

    barrier = pltpu.get_barrier_semaphore()
    zs = [lax.rem(z + i, LINE) for i in range(1, LINE)]
    partners = [nxt, prv, sib, ypar, xpar] + [dev(at(zz, y, c), x) for zz in zs]
    for to in partners:
        pl.semaphore_signal(barrier, inc=1, device_id=to, device_id_type=MESH)
    pl.semaphore_wait(barrier, len(partners))

    pend = []
    last, first = pl.ds(tokens - QB, QB), pl.ds(0, QB)
    after = pl.ds(QB + tokens, QB)
    nb = tokens // QB
    for i, (src, dst, lo, hi, a, b) in enumerate(
        [(k_in, kx, first, after, last, first), (v_in, vx, first, after, last, first)]
    ):
        pend.append(send(src.at[a], dst.at[lo], halo_s.at[2 * i], halo_r.at[2 * i], nxt))
        pend.append(send(src.at[b], dst.at[hi], halo_s.at[2 * i + 1], halo_r.at[2 * i + 1], prv))
    pend.append(send(marks_in.at[nb - 1], marks.at[0], halo_s.at[4], halo_r.at[4], nxt))
    pend.append(send(marks_in.at[0], marks.at[nb + 1], halo_s.at[5], halo_r.at[5], prv))

    pair = dev(at(jnp.where(inner, zb, zf), y, c), x)
    wrows = wo_in.shape[0] // (4 * WO_PIECES)
    wpiece = lambda pos, core, i: pl.ds(
        pl.multiple_of(((pos * 2 + core) * WO_PIECES + i) * wrows, wrows), wrows
    )
    for i in range(WO_PIECES):
        rows = wpiece(w, c, i)
        pend.append(send(wo_in.at[rows], wo_oth.at[rows], wx_s.at[i], wx_r.at[i], xpar))

    def wx_event(i):
        view = wo_oth.at[wpiece(w, c, i)]
        got(view, wx_r.at[i])
        pend.append(send(view, view, wz_s.at[i], wz_r.at[i], pair))
        pend.append(send(view, view, wf_s.at[i], wf_r.at[i], sib))

    def wz_event(i):
        view = wo_oth.at[wpiece(1 - w, c, i)]
        got(view, wz_r.at[i])
        pend.append(send(view, view, wg_s.at[i], wg_r.at[i], sib))

    quarter = width // 4

    def piece(refs, kind, i, slot):
        g, u, d = refs
        if kind == "g":
            return g.at[slot, pl.ds(i * quarter, quarter)]
        if kind == "u":
            return u.at[slot, pl.ds(i * quarter, quarter)]
        if slot is None:
            return d.at[0, :, pl.ds(i * part, part)]
        return d.at[i, pl.ds(slot * ff, ff)]

    def hbm_piece(kind, i):
        if kind == "g":
            return eg_in.at[0, pl.ds(i * quarter, quarter)]
        if kind == "u":
            return eu_in.at[0, pl.ds(i * quarter, quarter)]
        return ed_in.at[0, :, pl.ds(pl.multiple_of(i * part, part), part)]

    held = (gs, us, ds)
    own_only = lambda v: [
        ("g", 2 * v), ("g", 2 * v + 1), ("u", 2 * v), ("u", 2 * v + 1), ("d", v), ("d", 2 + v)
    ]
    y_list, x_list = own_only(x), own_only(ox)
    for i, (kind, j) in enumerate(y_list):
        pend.append(send(hbm_piece(kind, j), piece(held, kind, j, 2), y_s.at[i], y_r.at[i], ypar))

    def y_event(i):
        kind, j = y_list[i]
        view = piece(held, kind, j, 2)
        got(view, y_r.at[i])
        pend.append(send(view, view, x_s.at[i], x_r.at[i], xpar))
        pend.append(send(view, piece(held, kind, j, 3), fy_s.at[i], fy_r.at[i], sib))

    def x_event(i):
        kind, j = x_list[i]
        view = piece(held, kind, j, 2)
        got(view, x_r.at[i])
        pend.append(send(view, piece(held, kind, j, 3), fx_s.at[i], fx_r.at[i], sib))

    for cp in loads_a:
        cp.wait()
    named = lax.broadcasted_iota(jnp.int32, tab.shape[1:], 0)
    table = jnp.zeros(tab.shape[1:], f32)
    for k in range(ids.shape[0]):
        table = table + jnp.where(named == ids[k : k + 1], wts[k : k + 1], 0.0)
    tab[z] = table
    for i, zz in enumerate(zs):
        pend.append(
            send(tab.at[z], tab.at[z], tab_s.at[i], tab_r.at[LINE - 2 - i], dev(at(zz, y, c), x))
        )
    for i in range(2):
        dst = (kx, vx)[i]
        got(dst.at[first], halo_r.at[2 * i])
        got(dst.at[after], halo_r.at[2 * i + 1])
    got(marks.at[0], halo_r.at[4])
    got(marks.at[nb + 1], halo_r.at[5])

    @pl.when(s == 0)
    def _():
        marks[0] = jnp.full(marks.shape[1:], -1, jnp.int32)

    @pl.when(s == sp_count - 1)
    def _():
        marks[nb + 1] = jnp.full(marks.shape[1:], -1, jnp.int32)

    ri = lax.broadcasted_iota(jnp.int32, (QB, QB), 0)
    ci = lax.broadcasted_iota(jnp.int32, (QB, QB), 1)
    swap = jnp.where(ci == lax.rem(ri + HD, QB), 1.0, 0.0).astype(bf16)

    def spread(t, carry):
        rows = pl.ds(pl.multiple_of(t * QB, QB), QB)
        for src, dst in ((kx, kk), (vx, vv)):
            cur = src[rows]
            turned = jnp.dot(cur, swap, preferred_element_type=f32)
            cur = cur.astype(f32)
            zero = jnp.zeros_like(cur)
            left = ci < HD
            dst[0, rows] = jnp.where(left, cur, zero).astype(bf16)
            dst[1, rows] = jnp.where(left, zero, turned).astype(bf16)
            dst[2, rows] = jnp.where(left, turned, zero).astype(bf16)
            dst[3, rows] = jnp.where(left, zero, cur).astype(bf16)
        return carry

    lax.fori_loop(0, nb + 2, spread, 0)

    def attend_rows(blk, dst, drow):
        rows = pl.ds(pl.multiple_of(blk * QB, QB), QB)
        span = pl.ds(pl.multiple_of(blk * QB, QB), 3 * QB)
        mine = jnp.broadcast_to(marks[blk + 1][0:1], (QB, QB)).T
        biases = []
        for t in range(3):
            same = mine == jnp.broadcast_to(marks[blk + t][0:1], (QB, QB))
            if t == 0:
                same = same & (ri <= ci)
            if t == 2:
                same = same & (ci <= ri)
            biases.append(jnp.where(same, 0.0, NEG).astype(f32))
        bias = jnp.concatenate(biases, axis=1)
        for j in range(q_s.shape[1] // QB):
            g = j // 2
            keys2 = jnp.concatenate([kk[2 * g, span], kk[2 * g + 1, span]], axis=0)
            vals2 = jnp.concatenate([vv[2 * g, span], vv[2 * g + 1, span]], axis=0)
            sc = lax.dot_general(
                q_s[rows, j * QB : (j + 1) * QB], keys2, (((1,), (1,)), ((), ())),
                preferred_element_type=f32,
            ) * HD ** (-0.5)
            probs = []
            for h in range(2):
                sink = sink_ref[2 * j + h]
                own = sc[:, h * 3 * QB : (h + 1) * 3 * QB] + bias
                top = jnp.maximum(jnp.max(own, axis=-1, keepdims=True), sink)
                e = jnp.exp(own - top)
                total = jnp.sum(e, axis=-1, keepdims=True) + jnp.exp(sink - top)
                probs.append((e * (1.0 / total)).astype(bf16))
            o = jnp.dot(jnp.concatenate(probs, axis=1), vals2, preferred_element_type=f32)
            dst[pl.ds(pl.multiple_of(drow, QB), QB), j * QB : (j + 1) * QB] = o.astype(bf16)

    hb = half // QB

    for i in range(hb):
        attend_rows(ox * hb + i, a_out, i * QB)
        rows = pl.ds(i * QB, QB)
        pend.append(send(a_out.at[rows], a_in.at[rows], att_s.at[i], att_r.at[i], xpar))
        wx_event(i)
    pend.append(send(eg_in.at[0], gs.at[1], sib_s.at[0], sib_r.at[0], sib))
    pend.append(send(eu_in.at[0], us.at[1], sib_s.at[1], sib_r.at[1], sib))
    for n in range(4):
        pend.append(
            send(hbm_piece("d", n), piece(held, "d", n, 1), sib_s.at[2 + n], sib_r.at[2 + n], sib)
        )
    for i in range(hb):
        attend_rows(x * hb + i, a_own, i * QB)
        wx_event(hb + i)

    y_event(0)
    for cp in loads_b:
        cp.wait()
    for n in range(4):
        cols = slice(n * part, (n + 1) * part)
        base[n] = res[:, cols].astype(f32) + jnp.dot(
            a_own[...], wo_own[:, cols], preferred_element_type=f32
        )
    for i in range(WO_PIECES // 2):
        wz_event(i)
    for i in range(hb):
        got(a_in.at[pl.ds(i * QB, QB)], att_r.at[i])
    for i in range(WO_PIECES // 2, WO_PIECES):
        wz_event(i)
    for i in range(WO_PIECES):
        got(wo_oth.at[wpiece(w, oc, i)], wf_r.at[i])
        got(wo_oth.at[wpiece(1 - w, oc, i)], wg_r.at[i])
    square = jnp.zeros((half, 1), f32)
    for n in range(4):
        cols = slice(n * part, (n + 1) * part)
        r = (
            base[n] + jnp.dot(a_in[...], wo_oth[:, cols], preferred_element_type=f32)
        ).astype(bf16)
        res[:, cols] = r
        rf = r.astype(f32)
        square = square + jnp.sum(rf * rf, axis=-1, keepdims=True)
    inv = lax.rsqrt(square * (1.0 / width) + norm_eps)
    for n in range(4):
        cols = slice(n * part, (n + 1) * part)
        tok[z, :, cols] = (res[:, cols].astype(f32) * inv * gain_ref[:, cols]).astype(bf16)

    hr = half // 2
    rows_of = lambda r: pl.ds(r * hr, hr)

    def ag_send(b, r, direction, to):
        view = tok.at[b, rows_of(r)]
        send(view, view, ag_s.at[direction, b, r], ag_r.at[b, r], to)

    def ag_sent(b, r, direction):
        sent(tok.at[b, rows_of(r)], ag_s.at[direction, b, r])

    def ag_got(b, r):
        got(tok.at[b, rows_of(r)], ag_r.at[b, r])

    for r in range(2):
        ag_send(z, r, 0, fwd)

        @pl.when(inner)
        def _():
            ag_send(z, r, 1, bck)

    def relay(ob, r):
        b = line(ob)

        @pl.when(inner)
        def _():
            ag_got(b, r)
            if ob == 0:
                ag_send(b, r, 0, fwd)
            else:
                ag_send(b, r, 1, bck)

    def table_columns(b, carry):
        t = tab[b]
        grown = jnp.concatenate([t, jnp.zeros((QB - t.shape[0], t.shape[1]), f32)], axis=0)
        tabt[b] = grown.T
        return carry

    def gated(rows, gate, up):
        a = jnp.dot(rows, gate, preferred_element_type=f32)
        b = jnp.dot(rows, up, preferred_element_type=f32)
        return a / (1.0 + jnp.exp(-a)) * b

    def hidden(b, lo, hi, rows=slice(None)):
        def one(slot, carry):
            e = at(z, jnp.where(slot >= 2, oy, y), jnp.where(lax.rem(slot, 2) == 1, oc, c))
            weights = tabt[b, rows]
            mine = lax.broadcasted_iota(jnp.int32, weights.shape, 1) == e
            scale = jnp.sum(jnp.where(mine, weights, 0.0), axis=-1, keepdims=True)
            for h in range(2):
                cols = slice(h * (ff // 2), (h + 1) * (ff // 2))
                v = gated(tok[b, rows], gs[slot, :, cols], us[slot, :, cols]) * scale
                to = pl.ds(pl.multiple_of(slot * ff + h * (ff // 2), ff // 2), ff // 2)
                hid[b, rows, to] = v.astype(bf16)
            return carry

        lax.fori_loop(lo, hi, one, 0)

    y_event(1)
    for i in range(LINE - 1):
        got(tab.at[z], tab_r.at[i])
    lax.fori_loop(0, LINE, table_columns, 0)
    got(gs.at[1], sib_r.at[0])
    got(us.at[1], sib_r.at[1])
    hidden(z, 0, 2)
    relay(0, 0)
    relay(2, 0)
    x_event(0)
    y_event(2)
    x_event(1)
    relay(0, 1)
    relay(2, 1)
    y_event(3)
    near, far2, far3 = line(1 - w), line(2), line(3)

    def end_got(b):
        @pl.when(w == 0)
        def _():
            ag_got(b, 0)
            ag_got(b, 1)

    end_got(near)
    hidden(near, 0, 2)
    x_event(2)
    relay(3, 0)

    @pl.when(w == 0)
    def _():
        ag_got(far2, 0)
        hidden(far2, 0, 2, slice(0, hr))

    @pl.when(inner)
    def _():
        hidden(far2, 0, 2)

    y_event(4)
    x_event(3)
    relay(3, 1)
    hidden(near, 2, 3)
    for i in range(4):
        kind, j = y_list[i]
        got(piece(held, kind, j, 3), fy_r.at[i])
        kind, j = x_list[i]
        got(piece(held, kind, j, 3), fx_r.at[i])
    hidden(near, 3, 4)
    for n in range(4):
        got(piece(held, "d", n, 1), sib_r.at[2 + n])
    srow, drow = sg_in.shape[0] // 2, sd_in.shape[0] // 2
    shared_views = lambda core: [
        sg.at[1, pl.ds(core * srow, srow)],
        su.at[1, pl.ds(core * srow, srow)],
        sd.at[pl.ds(sd_in.shape[0] + core * drow, drow)],
    ]
    shared_parts = [
        sg_in.at[pl.ds(c * srow, srow)],
        su_in.at[pl.ds(c * srow, srow)],
        sd_in.at[pl.ds(c * drow, drow)],
    ]

    order = [x, 2 + x, ox, 2 + ox]
    tile = lambda slot, n: rbuf.at[slot, n]

    def down(b, n):
        return jnp.dot(hid[b], ds[n], preferred_element_type=f32)

    def reduce_piece(step, n, place=None):
        b = jnp.where(step == 2, near, line(2 + step))
        slot = jnp.where(step == 0, 3 * w, jnp.where(step == 1, 1 + w, 4 - w))
        zt = jnp.where((step == 2) & inner, zb, zf)

        def add():
            got(tile(step, n), rs_r.at[step, n])
            stage[step, n] = (acc[...] + rbuf[step, n].astype(f32)).astype(bf16)

        if place == "end":
            stage[step, n] = down(b, n).astype(bf16)
        else:
            acc[...] = down(b, n)
            if place == "inner":
                add()
            else:
                pl.when(inner)(add)

                @pl.when(w == 0)
                def _():
                    stage[step, n] = acc[...].astype(bf16)

        send(
            stage.at[step, n], tile(slot, n), rs_s.at[step, n], rs_r.at[slot, n], dev(at(zt, y, c), x)
        )

    def nth(k):
        base_n = jnp.where(k < 2, x, ox)
        return base_n + 2 * lax.rem(k, 2)

    def down_got(k):
        lst, sem = (y_list, fy_r) if k < 2 else (x_list, fx_r)
        kind, j = lst[4 + k % 2]
        got(piece(held, kind, j, 3), sem.at[4 + k % 2])

    def at_end(step, k):
        @pl.when(w == 0)
        def _():
            reduce_piece(step, order[k], "end")

    def at_inner(step, k):
        @pl.when(inner)
        def _():
            reduce_piece(step, order[k], "inner")

    down_got(0)
    at_end(2, 0)

    @pl.when(w == 0)
    def _():
        hidden(far2, 2, 4, slice(0, hr))
        ag_got(far2, 1)
        hidden(far2, 0, 4, slice(hr, half))

    @pl.when(inner)
    def _():
        hidden(far2, 2, 4)

    at_end(0, 0)
    y_event(5)
    for i, (src, dst) in enumerate(zip(shared_parts, shared_views(c))):
        pend.append(send(src, dst, sx_s.at[i], sx_r.at[i], xpar))

    @pl.when(inner)
    def _():
        hidden(far3, 0, 4)

    at_inner(0, 0)
    down_got(1)
    at_end(0, 1)
    x_event(4)
    down_got(2)
    at_end(0, 2)
    at_inner(0, 1)
    hidden(z, 2, 4)
    x_event(5)
    at_inner(0, 2)
    down_got(3)
    at_end(0, 3)
    at_inner(0, 3)

    @pl.when(w == 0)
    def _():
        ag_got(far3, 0)
        ag_got(far3, 1)
        hidden(far3, 0, 4)

    def later(i, carry):
        first_two, odd = i < 2, (lax.rem(i, 2) == 1) & (i < 7)
        in_step = jnp.where(first_two | odd, 1, 2)
        in_k = jnp.where(first_two, i, jnp.where(odd, (i + 1) // 2, (i - 1) // 2))
        step = jnp.where(inner, in_step, jnp.where(i < 4, 1, 2))
        k = jnp.where(inner, in_k, jnp.where(i < 4, i, i - 3))
        reduce_piece(step, nth(k))
        return carry

    def own_sum(n, carry):
        cols = pl.ds(pl.multiple_of(n * part, part), part)
        base[n] = res[:, cols].astype(f32) + down(z, n)
        return carry

    lax.fori_loop(0, 1, later, 0)
    lax.fori_loop(0, 4, own_sum, 0)
    lax.fori_loop(1, 7, later, 0)

    for i, view in enumerate(shared_views(c)):
        got(view, sx_r.at[i])
        pend.append(send(view, view, ss_s.at[i], ss_r.at[i], sib))
    for i, view in enumerate(shared_views(oc)):
        got(view, ss_r.at[i])
    units = sg_in.shape[1]
    for h in range(2):
        sh[:, h * units : (h + 1) * units] = gated(tok[z], sg[h], su[h]).astype(bf16)

    def shared_sum(n, carry):
        cols = pl.ds(pl.multiple_of(n * part, part), part)
        base[n] = base[n] + jnp.dot(sh[...], sd[:, cols], preferred_element_type=f32)
        return carry

    lax.fori_loop(0, 4, shared_sum, 0)
    lax.fori_loop(7, 7 + w, later, 0)

    def final(k, carry):
        n = nth(k)
        cols = pl.ds(pl.multiple_of(n * part, part), part)
        got(tile(3, n), rs_r.at[3, n])
        acc[...] = base[n] + rbuf[3, n].astype(f32)

        @pl.when(inner)
        def _():
            got(tile(4, n), rs_r.at[4, n])
            acc[...] = acc[...] + rbuf[4, n].astype(f32)

        ost[n] = acc[...].astype(bf16)
        load(ost.at[n], out_ref.at[:, cols], out_sem.at[n])
        return carry

    lax.fori_loop(0, 4, final, 0)

    for cp in pend:
        cp.wait_send()
    for r in range(2):
        ag_sent(z, r, 0)

        @pl.when(inner)
        def _():
            ag_sent(z, r, 1)
            ag_sent(line(0), r, 0)
            ag_sent(line(2), r, 1)
            ag_sent(line(3), r, 1)

    for step in range(3):
        for n in range(4):
            sent(stage.at[step, n], rs_s.at[step, n])
    for n in range(4):
        pltpu.make_async_copy(ost.at[n], out_ref.at[:, pl.ds(n * part, part)], out_sem.at[n]).wait()


def fused_shards(
    queries, keys, values, doc_ids, sink_logit, w_out, residual, ffn_gain, expert_ids,
    expert_weight, exp_gate, exp_up, exp_down, shared_gate, shared_up, shared_down,
):
    bf16, f32 = jnp.bfloat16, jnp.float32
    experts = lax.axis_size("sp")
    tokens = queries.shape[0]
    nb = tokens // QB
    marks = doc_ids.reshape(nb, 1, QB)
    half, width = residual.shape
    ff = exp_gate.shape[2]
    part = width // 4
    units = shared_gate.shape[1]
    heads = queries.shape[1]
    vm = pltpu.VMEM
    dma = pltpu.SemaphoreType.DMA
    anyspace = pl.BlockSpec(memory_space=pl.ANY)
    scratch = [
        vm((tokens, heads), bf16),
        vm((tokens + 2 * QB, QB), bf16),
        vm((tokens + 2 * QB, QB), bf16),
        vm((nb + 2, 1, QB), jnp.int32),
        vm((4, tokens + 2 * QB, QB), bf16),
        vm((4, tokens + 2 * QB, QB), bf16),
        vm((half, heads), bf16),
        vm((half, heads), bf16),
        vm((half, heads), bf16),
        vm(w_out.shape, bf16),
        vm(w_out.shape, bf16),
        vm((half, width), bf16),
        vm((LINE, half, width), bf16),
        vm(expert_ids.shape[::-1], jnp.int32),
        vm(expert_weight.shape[::-1], f32),
        vm((LINE, experts, half), f32),
        vm((LINE, half, QB), f32),
        vm((4, width, ff), bf16),
        vm((4, width, ff), bf16),
        vm((4, 4 * ff, part), bf16),
        vm((LINE, half, 4 * ff), bf16),
        vm((half, part), f32),
        vm((4, half, part), f32),
        vm((3, 4, half, part), bf16),
        vm((5, 4, half, part), bf16),
        vm((2, width, units), bf16),
        vm((2, width, units), bf16),
        vm((2 * units, width), bf16),
        vm((half, 2 * units), bf16),
        vm((4, half, part), bf16),
        dma((17,)), dma((6,)), dma((6,)), dma((3,)), dma((3,)),
        *[dma((WO_PIECES,)) for _ in range(8)],
        dma((2,)), dma((2,)),
        *[dma((6,)) for _ in range(10)],
        dma((2, LINE, 2)), dma((LINE, 2)), dma((3, 4)), dma((5, 4)),
        dma((3,)), dma((3,)), dma((3,)), dma((3,)), dma((4,)),
    ]
    rows = LINE * half
    return pl.pallas_call(
        layer_kernel,
        out_shape=jax.ShapeDtypeStruct((half, width), bf16),
        in_specs=[anyspace] * 3 + [pl.BlockSpec(memory_space=pltpu.SMEM)]
        + [anyspace] * 5
        + [pl.BlockSpec(memory_space=pltpu.VMEM)]
        + [anyspace] * 6,
        out_specs=anyspace,
        scratch_shapes=scratch,
        compiler_params=pltpu.CompilerParams(
            collective_id=0, has_side_effects=True, vmem_limit_bytes=63 * 1024 * 1024
        ),
        cost_estimate=pl.CostEstimate(
            flops=24 * rows * width * ff, bytes_accessed=32 * width * ff, transcendentals=rows * ff
        ),
    )(
        expert_ids.T, expert_weight.T, marks, sink_logit, queries, keys, values, w_out, residual, ffn_gain.reshape(1, -1),
        exp_gate, exp_up, exp_down, shared_gate, shared_up, shared_down,
    )


def solution(mesh):
    fits = mesh.shape["tp"] == 2 and mesh.shape["sp"] == 4 * LINE
    placed = (
        P("sp", "tp"),
        P("sp", "tp"),
        P("sp", "tp"),
        P("sp"),
        P("tp"),
        P("tp", None),
        P(("sp", "tp"), None),
        P(),
        P(("sp", "tp"), None),
        P(("sp", "tp"), None),
        P("sp", None, None),
        P("sp", None, None),
        P("sp", None, None),
        P(None, "tp"),
        P(None, "tp"),
        P("tp", None),
    )
    return jax.shard_map(
        fused_shards if fits else shards, mesh=mesh, in_specs=placed, out_specs=P(("sp", "tp"), None), check_vma=False
    )
```

```python
import math

import jax
import jax.numpy as jnp
from jax import lax
from jax.experimental import pallas as pl
from jax.experimental.pallas import tpu as pltpu
from jax.sharding import PartitionSpec as P

HD = 64
WINDOW = 128
PARTS = 2


norm_eps = 1e-06


def extended(cells, sides, width):
    for axis, dim in sides:
        count = lax.axis_size(axis)
        ends = count - 1
        head = lax.slice_in_dim(cells, 0, width, axis=dim)
        tail = lax.slice_in_dim(cells, cells.shape[dim] - width, cells.shape[dim], axis=dim)
        cells = jnp.concatenate(
            [
                lax.ppermute(tail, axis, [(i, (i + 1) % count) for i in range(ends)]),
                cells,
                lax.ppermute(head, axis, [((i + 1) % count, i) for i in range(ends)]),
            ],
            axis=dim,
        )
    return cells


def band_blocks(padded, width):
    span_count = padded.shape[0] // width - 2
    shaped = padded.reshape((span_count + 2, width) + padded.shape[1:])
    return jnp.concatenate(
        [
            shaped[0:span_count:2],
            shaped[1 : span_count + 1 : 2],
            shaped[2 : span_count + 2 : 2],
            shaped[3 : span_count + 3 : 2],
        ],
        axis=1,
    )


def attend(queries, ext_keys, ext_values, ext_marks, own_marks, sink_logit):
    tok_count = queries.shape[0]
    head_count = sink_logit.shape[0]
    key_heads = ext_keys.shape[1] // HD
    group_size = head_count // key_heads
    query_span = 2 * WINDOW
    block_count = tok_count // query_span
    query_blocks = queries.reshape(block_count, query_span, key_heads, group_size, HD)
    key_blocks = band_blocks(ext_keys, WINDOW).reshape(block_count, 4 * WINDOW, key_heads, HD)
    value_blocks = band_blocks(ext_values, WINDOW).reshape(block_count, 4 * WINDOW, key_heads, HD)
    mark_blocks = band_blocks(ext_marks, WINDOW)
    query_marks = own_marks.reshape(block_count, query_span)
    scores = jnp.einsum(
        "nqkgd,nmkd->nkgqm", query_blocks, key_blocks, preferred_element_type=jnp.float32
    ) * HD ** (-0.5)
    offset = (
        jnp.arange(query_span, dtype=jnp.int32)[:, None]
        - jnp.arange(4 * WINDOW, dtype=jnp.int32)[None, :]
        + WINDOW
    )
    allowed = (jnp.abs(offset) <= WINDOW)[None] & (
        mark_blocks[:, None, :] == query_marks[:, :, None]
    )
    scores = jnp.where(allowed[:, None, None], scores, -jnp.inf)
    sink_term = sink_logit.reshape(key_heads, group_size)[None, :, :, None, None]
    row_max = jnp.maximum(jnp.max(scores, axis=-1, keepdims=True), sink_term)
    exp_scores = jnp.exp(scores - row_max)
    attn_probs = (
        exp_scores / (jnp.sum(exp_scores, axis=-1, keepdims=True) + jnp.exp(sink_term - row_max))
    ).astype(jnp.bfloat16)
    result = jnp.einsum(
        "nkgqm,nmkd->nqkgd", attn_probs, value_blocks, preferred_element_type=jnp.float32
    )
    return result.astype(jnp.bfloat16).reshape(tok_count, head_count * HD)


def expert_kernel(rows_ref, scale_ref, gate_ref, up_ref, down_ref, side_ref, side_down_ref, out_ref):
    rows = rows_ref[...]
    gated = jnp.dot(rows, gate_ref[...], preferred_element_type=jnp.float32)
    lifted = jnp.dot(rows, up_ref[...], preferred_element_type=jnp.float32)
    hidden = (gated / (1.0 + jnp.exp(-gated)) * lifted).astype(jnp.bfloat16)
    produced = jnp.dot(hidden, down_ref[...], preferred_element_type=jnp.float32)
    side = jnp.dot(rows, side_ref[...], preferred_element_type=jnp.float32)
    width = side.shape[1] // 2
    side_gate, side_up = side[:, :width], side[:, width:]
    side_hidden = (side_gate / (1.0 + jnp.exp(-side_gate)) * side_up).astype(jnp.bfloat16)
    shared = jnp.dot(side_hidden, side_down_ref[...], preferred_element_type=jnp.float32)
    out_ref[...] = (
        scale_ref[...] * produced.astype(jnp.bfloat16).astype(jnp.float32) + shared
    ).astype(jnp.bfloat16)


def run_experts(rows, scale, gate_w, up_w, down_w, side_w, side_down):
    count, width = rows.shape
    tile = math.gcd(count, 256)
    whole = lambda w: pl.BlockSpec(w.shape, lambda i: (0, 0))
    units = gate_w.shape[1] + side_w.shape[1] // 2
    return pl.pallas_call(
        expert_kernel,
        grid=(count // tile,),
        in_specs=[
            pl.BlockSpec((tile, width), lambda i: (i, 0)),
            pl.BlockSpec((tile, 1), lambda i: (i, 0)),
            whole(gate_w),
            whole(up_w),
            whole(down_w),
            whole(side_w),
            whole(side_down),
        ],
        out_specs=pl.BlockSpec((tile, width), lambda i: (i, 0)),
        out_shape=jax.ShapeDtypeStruct((count, width), jnp.bfloat16),
        compiler_params=pltpu.CompilerParams(
            dimension_semantics=("arbitrary",), vmem_limit_bytes=48 * 1024 * 1024
        ),
        cost_estimate=pl.CostEstimate(
            flops=6 * count * width * units,
            bytes_accessed=4 * count * width + 6 * units * width,
            transcendentals=count * units,
        ),
    )(rows, scale, gate_w, up_w, down_w, side_w, side_down)


def shared_slice(shared_gate, shared_up, shared_down):
    sp_count, tp_count = lax.axis_size("sp"), lax.axis_size("tp")
    own, side = lax.axis_index("tp"), lax.axis_index("sp")
    units = shared_gate.shape[1] * tp_count // sp_count
    per_owner = sp_count // tp_count
    owner, offset = side // per_owner, (side % per_owner) * units
    held = jnp.concatenate(
        [
            lax.dynamic_slice_in_dim(shared_gate, offset, units, axis=1).T,
            lax.dynamic_slice_in_dim(shared_up, offset, units, axis=1).T,
            lax.dynamic_slice_in_dim(shared_down, offset, units, axis=0),
        ],
        axis=0,
    )
    chosen = held
    for shift in range(1, tp_count):
        came = lax.ppermute(held, "tp", [(i, (i + shift) % tp_count) for i in range(tp_count)])
        chosen = jnp.where((own - shift) % tp_count == owner, came, chosen)
    padded = -(-units // 128) * 128
    grown = [
        jnp.pad(chosen[i * units : (i + 1) * units], ((0, padded - units), (0, 0))) for i in range(3)
    ]
    return jnp.concatenate(grown[:2], axis=0).T, grown[2]


def shards(
    queries,
    keys,
    values,
    doc_ids,
    sink_logit,
    w_out,
    residual,
    ffn_gain,
    expert_ids,
    expert_weight,
    exp_gate,
    exp_up,
    exp_down,
    shared_gate,
    shared_up,
    shared_down,
):
    marks = (doc_ids + 1).astype(jnp.bfloat16)
    kv = keys.shape[1]
    joined = jnp.concatenate(
        [keys, values, jnp.broadcast_to(marks[:, None], (marks.shape[0], 128))], axis=1
    )
    extended_all = extended(joined, (("sp", 0),), WINDOW)
    ext_keys, ext_values, ext_marks = (
        extended_all[:, :kv],
        extended_all[:, kv : 2 * kv],
        extended_all[:, 2 * kv],
    )
    attended = attend(queries, ext_keys, ext_values, ext_marks, marks, sink_logit)
    row_count = residual.shape[0]
    mixed = lax.psum_scatter(
        jnp.dot(attended, w_out, preferred_element_type=jnp.float32).astype(jnp.bfloat16),
        "tp",
        scatter_dimension=0,
        tiled=True,
    ).astype(jnp.float32)
    resid = (residual.astype(jnp.float32) + mixed).astype(jnp.bfloat16)
    resid_f = resid.astype(jnp.float32)
    normed = (
        resid_f
        * lax.rsqrt(jnp.mean(resid_f * resid_f, axis=-1, keepdims=True) + norm_eps)
        * ffn_gain
    ).astype(jnp.bfloat16)
    side_w, side_down = shared_slice(shared_gate, shared_up, shared_down)
    sp_count = lax.axis_size("sp")
    chosen = expert_ids[:, :, None] == jnp.arange(sp_count, dtype=jnp.int32)
    table = jnp.sum(jnp.where(chosen, expert_weight[:, :, None], 0.0), axis=1)
    scales = lax.all_to_all(table.T, "sp", split_axis=0, concat_axis=0, tiled=True)
    part_rows = row_count // PARTS
    sums = []
    for part in range(PARTS):
        begin = part * part_rows
        gathered = lax.all_gather(normed[begin : begin + part_rows], "sp", axis=0, tiled=True)
        scale = scales[:, begin : begin + part_rows].reshape(-1, 1)
        produced = run_experts(
            gathered, scale, exp_gate[0], exp_up[0], exp_down[0], side_w, side_down
        )
        sums.append(lax.psum_scatter(produced, "sp", scatter_dimension=0, tiled=True))
    added = jnp.concatenate(sums, axis=0)
    return (resid.astype(jnp.float32) + added.astype(jnp.float32)).astype(jnp.bfloat16)


MESH = pl.DeviceIdType.MESH
QB = 128
NEG = -1e30
LINE = 4
WO_PIECES = 4
TILES = 8
CUTS = 8


def layer_kernel(
    ids_in, wts_in, marks_in, sink_ref, q_in, k_in, v_in, wo_in, res_in, gain_ref,
    eg_in, eu_in, ed_in, sg_in, su_in, sd_in,
    out_ref,
    q_s, kx, vx, marks, kk, vv, a_out, a_own, a_in, wo_own, wo_oth, res, tok, ids, wts, tab, tabt,
    gs, us, ds, hid, acc, base, stage, rbuf, sg, su, sd, sh, ost,
    loc, halo_s, halo_r, tab_s, tab_r, wx_s, wx_r, wz_s, wz_r, wf_s, wf_r, wg_s, wg_r, att_s, att_r,
    sib_s, sib_r, y_s, y_r, x_s, x_r, fy_s, fy_r, fx_s, fx_r,
    ag_s, ag_r, rs_s, rs_r, sx_s, sx_r, ss_s, ss_r, out_sem,
):
    f32, bf16 = jnp.float32, jnp.bfloat16
    sp_count, tp_count = lax.axis_size("sp"), lax.axis_size("tp")
    s, x = lax.axis_index("sp"), lax.axis_index("tp")
    z, y, c = s // 4, lax.rem(s // 2, 2), lax.rem(s, 2)
    ox, oy, oc = 1 - x, 1 - y, 1 - c
    at = lambda zz, yy, cc: (zz * 2 + yy) * 2 + cc
    dev = lambda sp, tp: {"sp": sp, "tp": tp}
    sib, ypar, xpar = dev(at(z, y, oc), x), dev(at(z, oy, c), x), dev(s, ox)
    nxt, prv = dev(lax.rem(s + 1, sp_count), x), dev(lax.rem(s + sp_count - 1, sp_count), x)
    low = z < 2
    w = jnp.where(low, z, 3 - z)
    inner = w == 1
    zf = jnp.where(low, z + 1, z - 1)
    zb = jnp.clip(jnp.where(low, z - 1, z + 1), 0, 3)
    fwd, bck = dev(at(zf, y, c), x), dev(at(zb, y, c), x)
    line = lambda ob: jnp.where(low, ob, 3 - ob)
    tokens = q_in.shape[0]
    half = tokens // 2
    width = res_in.shape[1]
    ff = eg_in.shape[2]
    part = width // TILES

    def send(src, dst, ss, rs, to):
        cp = pltpu.make_async_remote_copy(
            src_ref=src, dst_ref=dst, send_sem=ss, recv_sem=rs, device_id=to, device_id_type=MESH
        )
        cp.start()
        return cp

    def got(view, rs):
        pltpu.make_async_remote_copy(
            src_ref=view, dst_ref=view, send_sem=rs, recv_sem=rs, device_id=sib, device_id_type=MESH
        ).wait_recv()

    def sent(view, ss):
        pltpu.make_async_remote_copy(
            src_ref=view, dst_ref=view, send_sem=ss, recv_sem=ss, device_id=sib, device_id_type=MESH
        ).wait_send()

    def amount(elements):
        return ds.at[:, pl.ds(0, elements // (TILES * part))]

    def load(src, dst, sem):
        cp = pltpu.make_async_copy(src, dst, sem)
        cp.start()
        return cp

    rows_own = pl.ds(QB, tokens)
    loads_a = [
        load(q_in, q_s, loc.at[0]),
        load(k_in, kx.at[rows_own], loc.at[1]),
        load(v_in, vx.at[rows_own], loc.at[2]),
        load(marks_in, marks.at[pl.ds(1, tokens // QB)], loc.at[3]),
        load(ids_in, ids, loc.at[4]),
        load(wts_in, wts, loc.at[5]),
    ]
    loads_b = [
        load(wo_in, wo_own, loc.at[6]),
        load(res_in, res, loc.at[7]),
        load(eg_in.at[0], gs.at[0], loc.at[6]),
        load(eu_in.at[0], us.at[0], loc.at[6]),
        load(sg_in, sg.at[0], loc.at[7]),
        load(su_in, su.at[0], loc.at[7]),
        load(sd_in, sd.at[pl.ds(0, sd_in.shape[0])], loc.at[7]),
    ]
    for n in range(TILES):
        loads_b.append(
            load(ed_in.at[0, :, pl.ds(n * part, part)], ds.at[n, pl.ds(0, ff)], loc.at[6])
        )

    barrier = pltpu.get_barrier_semaphore()
    zs = [lax.rem(z + i, LINE) for i in range(1, LINE)]
    partners = [nxt, prv, sib, ypar, xpar] + [dev(at(zz, y, c), x) for zz in zs]
    for to in partners:
        pl.semaphore_signal(barrier, inc=1, device_id=to, device_id_type=MESH)
    pl.semaphore_wait(barrier, len(partners))

    pend = []
    last, first = pl.ds(tokens - QB, QB), pl.ds(0, QB)
    after = pl.ds(QB + tokens, QB)
    nb = tokens // QB
    for i, (src, dst, lo, hi, a, b) in enumerate(
        [(k_in, kx, first, after, last, first), (v_in, vx, first, after, last, first)]
    ):
        pend.append(send(src.at[a], dst.at[lo], halo_s.at[2 * i], halo_r.at[2 * i], nxt))
        pend.append(send(src.at[b], dst.at[hi], halo_s.at[2 * i + 1], halo_r.at[2 * i + 1], prv))
    pend.append(send(marks_in.at[nb - 1], marks.at[0], halo_s.at[4], halo_r.at[4], nxt))
    pend.append(send(marks_in.at[0], marks.at[nb + 1], halo_s.at[5], halo_r.at[5], prv))

    pair = dev(at(jnp.where(inner, zb, zf), y, c), x)
    wrows = wo_in.shape[0] // (4 * WO_PIECES)
    wpiece = lambda pos, core, i: pl.ds(
        pl.multiple_of(((pos * 2 + core) * WO_PIECES + i) * wrows, wrows), wrows
    )
    for i in range(WO_PIECES):
        rows = wpiece(w, c, i)
        send(wo_in.at[rows], wo_oth.at[rows], wx_s.at[0], wx_r.at[i], xpar)

    def wx_event(i):
        view = wo_oth.at[wpiece(w, c, i)]
        got(view, wx_r.at[i])
        send(view, view, wz_s.at[0], wz_r.at[i], pair)
        send(view, view, wf_s.at[0], wf_r.at[0], sib)

    def wz_event(i):
        view = wo_oth.at[wpiece(1 - w, c, i)]
        got(view, wz_r.at[i])
        send(view, view, wg_s.at[0], wg_r.at[0], sib)

    quarter = width // CUTS

    def piece(refs, kind, i, slot):
        g, u, d = refs
        if kind == "g":
            return g.at[slot, pl.ds(i * quarter, quarter)]
        if kind == "u":
            return u.at[slot, pl.ds(i * quarter, quarter)]
        if slot is None:
            return d.at[0, :, pl.ds(i * part, part)]
        return d.at[i, pl.ds(slot * ff, ff)]

    def hbm_piece(kind, i):
        if kind == "g":
            return eg_in.at[0, pl.ds(i * quarter, quarter)]
        if kind == "u":
            return eu_in.at[0, pl.ds(i * quarter, quarter)]
        return ed_in.at[0, :, pl.ds(pl.multiple_of(i * part, part), part)]

    held = (gs, us, ds)
    gates, ups = CUTS // 2, CUTS // 2 - 1
    own_only = lambda v: [("g", gates * v + i) for i in range(gates)] + [
        ("u", ups * v + i) for i in range(ups)
    ]
    tiles_of = lambda v: [("d", 2 * i + v) for i in range(TILES // 2)]
    both = [("u", i) for i in range(2 * ups, CUTS)]
    y_list = own_only(x) + both + tiles_of(x)
    x_list = own_only(ox) + tiles_of(ox)
    x_gu = gates + ups
    y_gu = x_gu + len(both)
    relayed = {i: i if i < x_gu else i - len(both) for i in range(len(y_list)) if i < x_gu or i >= y_gu}
    for i, (kind, j) in enumerate(y_list):
        send(hbm_piece(kind, j), piece(held, kind, j, 2), y_s.at[0], y_r.at[i], ypar)

    def y_event(i):
        kind, j = y_list[i]
        view = piece(held, kind, j, 2)
        got(view, y_r.at[i])
        if i in relayed:
            k = relayed[i]
            send(view, view, x_s.at[0], x_r.at[k], xpar)
        send(view, piece(held, kind, j, 3), fy_s.at[0], fy_r.at[max(0, i - y_gu + 1)], sib)

    def x_event(i):
        kind, j = x_list[i]
        view = piece(held, kind, j, 2)
        got(view, x_r.at[i])
        send(view, piece(held, kind, j, 3), fx_s.at[0], fx_r.at[max(0, i - x_gu + 1)], sib)

    for cp in loads_a:
        cp.wait()
    named = lax.broadcasted_iota(jnp.int32, tab.shape[1:], 0)
    table = jnp.zeros(tab.shape[1:], f32)
    for k in range(ids.shape[0]):
        table = table + jnp.where(named == ids[k : k + 1], wts[k : k + 1], 0.0)
    tab[z] = table
    for i, zz in enumerate(zs):
        pend.append(
            send(tab.at[z], tab.at[z], tab_s.at[i], tab_r.at[LINE - 2 - i], dev(at(zz, y, c), x))
        )
    for i in range(2):
        dst = (kx, vx)[i]
        got(dst.at[first], halo_r.at[2 * i])
        got(dst.at[after], halo_r.at[2 * i + 1])
    got(marks.at[0], halo_r.at[4])
    got(marks.at[nb + 1], halo_r.at[5])

    @pl.when(s == 0)
    def _():
        marks[0] = jnp.full(marks.shape[1:], -1, jnp.int32)

    @pl.when(s == sp_count - 1)
    def _():
        marks[nb + 1] = jnp.full(marks.shape[1:], -1, jnp.int32)

    ri = lax.broadcasted_iota(jnp.int32, (QB, QB), 0)
    ci = lax.broadcasted_iota(jnp.int32, (QB, QB), 1)
    swap = jnp.where(ci == lax.rem(ri + HD, QB), 1.0, 0.0).astype(bf16)

    def spread(t, carry):
        rows = pl.ds(pl.multiple_of(t * QB, QB), QB)
        for src, dst in ((kx, kk), (vx, vv)):
            cur = src[rows]
            turned = jnp.dot(cur, swap, preferred_element_type=f32)
            cur = cur.astype(f32)
            zero = jnp.zeros_like(cur)
            left = ci < HD
            dst[0, rows] = jnp.where(left, cur, zero).astype(bf16)
            dst[1, rows] = jnp.where(left, zero, turned).astype(bf16)
            dst[2, rows] = jnp.where(left, turned, zero).astype(bf16)
            dst[3, rows] = jnp.where(left, zero, cur).astype(bf16)
        return carry

    lax.fori_loop(0, nb + 2, spread, 0)

    def attend_rows(blk, dst, drow):
        rows = pl.ds(pl.multiple_of(blk * QB, QB), QB)
        span = pl.ds(pl.multiple_of(blk * QB, QB), 3 * QB)
        mine = jnp.broadcast_to(marks[blk + 1][0:1], (QB, QB)).T
        biases = []
        for t in range(3):
            same = mine == jnp.broadcast_to(marks[blk + t][0:1], (QB, QB))
            if t == 0:
                same = same & (ri <= ci)
            if t == 2:
                same = same & (ci <= ri)
            biases.append(jnp.where(same, 0.0, NEG).astype(f32))
        bias = jnp.concatenate(biases, axis=1)
        for j in range(q_s.shape[1] // QB):
            g = j // 2
            keys2 = jnp.concatenate([kk[2 * g, span], kk[2 * g + 1, span]], axis=0)
            vals2 = jnp.concatenate([vv[2 * g, span], vv[2 * g + 1, span]], axis=0)
            sc = lax.dot_general(
                q_s[rows, j * QB : (j + 1) * QB], keys2, (((1,), (1,)), ((), ())),
                preferred_element_type=f32,
            ) * HD ** (-0.5)
            probs = []
            for h in range(2):
                sink = sink_ref[2 * j + h]
                own = sc[:, h * 3 * QB : (h + 1) * 3 * QB] + bias
                top = jnp.maximum(jnp.max(own, axis=-1, keepdims=True), sink)
                e = jnp.exp(own - top)
                total = jnp.sum(e, axis=-1, keepdims=True) + jnp.exp(sink - top)
                probs.append((e * (1.0 / total)).astype(bf16))
            o = jnp.dot(jnp.concatenate(probs, axis=1), vals2, preferred_element_type=f32)
            dst[pl.ds(pl.multiple_of(drow, QB), QB), j * QB : (j + 1) * QB] = o.astype(bf16)

    hb = half // QB

    for i in range(hb):
        attend_rows(ox * hb + i, a_out, i * QB)
        rows = pl.ds(i * QB, QB)
        send(a_out.at[rows], a_in.at[rows], att_s.at[0], att_r.at[0], xpar)
        wx_event(i)
    send(eg_in.at[0], gs.at[1], sib_s.at[0], sib_r.at[0], sib)
    send(eu_in.at[0], us.at[1], sib_s.at[0], sib_r.at[1], sib)
    for n in range(TILES):
        send(hbm_piece("d", n), piece(held, "d", n, 1), sib_s.at[0], sib_r.at[2], sib)
    for i in range(hb):
        attend_rows(x * hb + i, a_own, i * QB)
        wx_event(hb + i)

    y_event(0)
    first_loads = wo_in.size + 3 * eg_in.size
    for i, elements in ((6, first_loads), (7, res_in.size + 3 * sg_in.size)):
        view = amount(elements)
        pltpu.make_async_copy(view, view, loc.at[i]).wait()
    for n in range(TILES):
        cols = slice(n * part, (n + 1) * part)
        base[n] = res[:, cols].astype(f32) + jnp.dot(
            a_own[...], wo_own[:, cols], preferred_element_type=f32
        )
    for i in range(WO_PIECES):
        wz_event(i)
    got(a_in, att_r.at[0])
    got(amount(wo_in.size // 4), wf_r.at[0])
    got(amount(wo_in.size // 4), wg_r.at[0])
    square = jnp.zeros((half, 1), f32)
    for n in range(TILES):
        cols = slice(n * part, (n + 1) * part)
        r = (
            base[n] + jnp.dot(a_in[...], wo_oth[:, cols], preferred_element_type=f32)
        ).astype(bf16)
        res[:, cols] = r
        rf = r.astype(f32)
        square = square + jnp.sum(rf * rf, axis=-1, keepdims=True)
    inv = lax.rsqrt(square * (1.0 / width) + norm_eps)
    for n in range(4):
        cols = slice(n * (width // 4), (n + 1) * (width // 4))
        tok[z, :, cols] = (res[:, cols].astype(f32) * inv * gain_ref[:, cols]).astype(bf16)

    hr = half // 2
    rows_of = lambda r: pl.ds(r * hr, hr)

    def ag_send(b, r, direction, to):
        view = tok.at[b, rows_of(r)]
        send(view, view, ag_s.at[direction], ag_r.at[b, r], to)

    def ag_got(b, r):
        got(tok.at[b, rows_of(r)], ag_r.at[b, r])

    for r in range(2):
        ag_send(z, r, 0, fwd)

        @pl.when(inner)
        def _():
            ag_send(z, r, 1, bck)

    def relay(ob, r):
        b = line(ob)

        @pl.when(inner)
        def _():
            ag_got(b, r)
            if ob == 0:
                ag_send(b, r, 2, fwd)
            else:
                ag_send(b, r, 3, bck)

    def table_columns(b, carry):
        t = tab[b]
        grown = jnp.concatenate([t, jnp.zeros((QB - t.shape[0], t.shape[1]), f32)], axis=0)
        tabt[b] = grown.T
        return carry

    def gated(rows, gate, up):
        a = jnp.dot(rows, gate, preferred_element_type=f32)
        b = jnp.dot(rows, up, preferred_element_type=f32)
        return a / (1.0 + jnp.exp(-a)) * b

    def hidden(b, lo, hi, rows=slice(None)):
        def one(slot, carry):
            e = at(z, jnp.where(slot >= 2, oy, y), jnp.where(lax.rem(slot, 2) == 1, oc, c))
            weights = tabt[b, rows]
            mine = lax.broadcasted_iota(jnp.int32, weights.shape, 1) == e
            scale = jnp.sum(jnp.where(mine, weights, 0.0), axis=-1, keepdims=True)
            for h in range(2):
                cols = slice(h * (ff // 2), (h + 1) * (ff // 2))
                v = gated(tok[b, rows], gs[slot, :, cols], us[slot, :, cols]) * scale
                to = pl.ds(pl.multiple_of(slot * ff + h * (ff // 2), ff // 2), ff // 2)
                hid[b, rows, to] = v.astype(bf16)
            return carry

        lax.fori_loop(lo, hi, one, 0)

    y_event(1)
    for i in range(LINE - 1):
        got(tab.at[z], tab_r.at[i])
    lax.fori_loop(0, LINE, table_columns, 0)
    got(gs.at[1], sib_r.at[0])
    got(us.at[1], sib_r.at[1])
    y_event(2)
    hidden(z, 0, 2)
    y_event(3)
    x_event(0)
    relay(0, 0)
    relay(2, 0)
    x_event(1)
    y_event(4)
    x_event(2)
    y_event(5)
    relay(0, 1)
    relay(2, 1)
    x_event(3)
    y_event(6)
    near, far2, far3 = line(1 - w), line(2), line(3)

    def end_got(b):
        @pl.when(w == 0)
        def _():
            ag_got(b, 0)
            ag_got(b, 1)

    end_got(near)
    hidden(near, 0, 2)
    x_event(4)
    y_event(7)
    x_event(5)
    y_event(8)
    relay(3, 0)

    @pl.when(w == 0)
    def _():
        ag_got(far2, 0)
        hidden(far2, 0, 2, slice(0, hr))

    @pl.when(inner)
    def _():
        hidden(far2, 0, 2)

    x_event(6)
    y_event(9)
    hidden(near, 2, 3)
    cut = quarter * ff
    got(amount(y_gu * cut), fy_r.at[0])
    got(amount(x_gu * cut), fx_r.at[0])
    hidden(near, 3, 4)
    got(amount(ed_in.size), sib_r.at[2])
    srow, drow = sg_in.shape[0] // 2, sd_in.shape[0] // 2
    shared_views = lambda core: [
        sg.at[1, pl.ds(core * srow, srow)],
        su.at[1, pl.ds(core * srow, srow)],
        sd.at[pl.ds(sd_in.shape[0] + core * drow, drow)],
    ]
    shared_parts = [
        sg_in.at[pl.ds(c * srow, srow)],
        su_in.at[pl.ds(c * srow, srow)],
        sd_in.at[pl.ds(c * drow, drow)],
    ]

    order = [2 * (k // 2) + (x if k % 2 == 0 else ox) for k in range(TILES)]
    tile = lambda slot, n: rbuf.at[slot, n]

    def down(b, n):
        return jnp.dot(hid[b], ds[n], preferred_element_type=f32)

    def reduce_piece(step, n, place=None):
        b = jnp.where(step == 2, near, line(2 + step))
        slot = jnp.where(step == 0, 3 * w, jnp.where(step == 1, 1 + w, 4 - w))
        zt = jnp.where((step == 2) & inner, zb, zf)

        def add():
            got(tile(step, n), rs_r.at[step, n])
            stage[step, n] = (acc[...] + rbuf[step, n].astype(f32)).astype(bf16)

        if place == "end":
            stage[step, n] = down(b, n).astype(bf16)
        else:
            acc[...] = down(b, n)
            if place == "inner":
                add()
            else:
                pl.when(inner)(add)

                @pl.when(w == 0)
                def _():
                    stage[step, n] = acc[...].astype(bf16)

        send(
            stage.at[step, n], tile(slot, n), rs_s.at[step], rs_r.at[slot, n], dev(at(zt, y, c), x)
        )

    def nth(k):
        return 2 * (k // 2) + jnp.where(lax.rem(k, 2) == 0, x, ox)

    def down_got(k):
        lst, sem, first_d = (y_list, fy_r, y_gu) if k % 2 == 0 else (x_list, fx_r, x_gu)
        kind, j = lst[first_d + k // 2]
        got(piece(held, kind, j, 3), sem.at[1 + k // 2])

    def at_end(step, k):
        @pl.when(w == 0)
        def _():
            reduce_piece(step, order[k], "end")

    def at_inner(step, k):
        @pl.when(inner)
        def _():
            reduce_piece(step, order[k], "inner")

    early = TILES // 2
    down_got(0)
    at_end(2, 0)

    @pl.when(w == 0)
    def _():
        hidden(far2, 2, 4, slice(0, hr))

    x_event(7)
    down_got(1)
    at_end(2, 1)
    y_event(10)
    down_got(2)
    at_end(2, 2)
    relay(3, 1)

    @pl.when(w == 0)
    def _():
        ag_got(far2, 1)
        hidden(far2, 0, 4, slice(hr, half))

    @pl.when(inner)
    def _():
        hidden(far2, 2, 4)

    for k in range(early - 1):
        at_end(0, k)
    x_event(8)
    y_event(11)
    down_got(3)
    at_end(2, 3)
    at_end(0, 3)

    @pl.when(inner)
    def _():
        hidden(far3, 0, 4)

    y_event(12)
    for i, (src, dst) in enumerate(zip(shared_parts, shared_views(c))):
        send(src, dst, sx_s.at[0], sx_r.at[0], xpar)
    x_event(9)

    def a_tiles(k, carry):
        reduce_piece(0, nth(k), "inner")
        return carry

    @pl.when(inner)
    def _():
        lax.fori_loop(0, 2, a_tiles, 0)

    for k in range(4, 7):
        down_got(k)
        at_end(0, k)

    @pl.when(inner)
    def _():
        lax.fori_loop(2, 4, a_tiles, 0)

    hidden(z, 2, 4)

    @pl.when(w == 0)
    def _():
        ag_got(far3, 0)
        hidden(far3, 0, 4, slice(0, hr))

    x_event(10)
    down_got(7)
    at_end(0, 7)

    @pl.when(inner)
    def _():
        lax.fori_loop(4, TILES, a_tiles, 0)

    @pl.when(w == 0)
    def _():
        ag_got(far3, 1)
        hidden(far3, 0, 4, slice(hr, half))

    lag = 3
    turns = 2 * TILES - lag

    def later(i, carry):
        odd = lax.rem(i - lag, 2) == 0
        far = (i < lag) | ((i < turns) & ~odd)
        in_step = jnp.where(far, 1, 2)
        far_k = jnp.where(i < lag, i, (i + lag - 1) // 2)
        near_k = jnp.where(i < turns, (i - lag) // 2, i - TILES)
        step = jnp.where(inner, in_step, jnp.where(i < TILES, 1, 2))
        k = jnp.where(inner, jnp.where(far, far_k, near_k), jnp.where(i < TILES, i, i - TILES + early))
        reduce_piece(step, nth(k))
        return carry

    def own_sum(n, carry):
        cols = pl.ds(pl.multiple_of(n * part, part), part)
        base[n] = res[:, cols].astype(f32) + down(z, n)
        return carry

    at_once = 2 * TILES - early

    block = half * width

    def drain():
        for cp in pend:
            cp.wait_send()
        for sem, elements in (
            (wx_s, wo_in.size // 4), (wz_s, wo_in.size // 4), (wf_s, wo_in.size // 4),
            (wg_s, wo_in.size // 4), (att_s, a_out.size), (sib_s, 3 * eg_in.size),
            (y_s, len(y_list) * cut), (x_s, len(x_list) * cut), (fy_s, len(y_list) * cut),
            (fx_s, len(x_list) * cut), (ag_s, block),
        ):
            sent(amount(elements), sem.at[0])

    @pl.when(inner)
    def _():
        drain()
        for i, elements in ((1, block), (2, block), (3, 2 * block)):
            sent(amount(elements), ag_s.at[i])

    lax.fori_loop(0, 2, later, 0)
    lax.fori_loop(0, TILES, own_sum, 0)
    middle = at_once + w
    lax.fori_loop(2, middle, later, 0)
    pl.when(w == 0)(drain)

    shared_size = 3 * sg_in.size // 2
    got(amount(shared_size), sx_r.at[0])
    for view in shared_views(c):
        send(view, view, ss_s.at[0], ss_r.at[0], sib)
    lax.fori_loop(middle, at_once + early * w, later, 0)
    got(amount(shared_size), ss_r.at[0])
    units = sg_in.shape[1]
    for h in range(2):
        sh[:, h * units : (h + 1) * units] = gated(tok[z], sg[h], su[h]).astype(bf16)

    def shared_sum(n, carry):
        cols = pl.ds(pl.multiple_of(n * part, part), part)
        base[n] = base[n] + jnp.dot(sh[...], sd[:, cols], preferred_element_type=f32)
        return carry

    lax.fori_loop(0, TILES, shared_sum, 0)

    def final(k, carry):
        n = nth(k)
        cols = pl.ds(pl.multiple_of(n * part, part), part)
        got(tile(3, n), rs_r.at[3, n])
        acc[...] = base[n] + rbuf[3, n].astype(f32)

        @pl.when(inner)
        def _():
            got(tile(4, n), rs_r.at[4, n])
            acc[...] = acc[...] + rbuf[4, n].astype(f32)

        ost[n] = acc[...].astype(bf16)
        load(ost.at[n], out_ref.at[:, cols], out_sem.at[0])
        return carry

    def steps_sent(steps):
        for step in steps:
            sent(amount(block), rs_s.at[step])

    steps_sent((0, 1))
    lax.fori_loop(0, TILES, final, 0)

    sent(amount(shared_size), sx_s.at[0])
    sent(amount(shared_size), ss_s.at[0])
    steps_sent((2,))
    pltpu.make_async_copy(amount(block), amount(block), out_sem.at[0]).wait()


def fused_shards(
    queries, keys, values, doc_ids, sink_logit, w_out, residual, ffn_gain, expert_ids,
    expert_weight, exp_gate, exp_up, exp_down, shared_gate, shared_up, shared_down,
):
    bf16, f32 = jnp.bfloat16, jnp.float32
    experts = lax.axis_size("sp")
    tokens = queries.shape[0]
    nb = tokens // QB
    marks = doc_ids.reshape(nb, 1, QB)
    half, width = residual.shape
    ff = exp_gate.shape[2]
    part = width // TILES
    units = shared_gate.shape[1]
    heads = queries.shape[1]
    vm = pltpu.VMEM
    dma = pltpu.SemaphoreType.DMA
    anyspace = pl.BlockSpec(memory_space=pl.ANY)
    scratch = [
        vm((tokens, heads), bf16),
        vm((tokens + 2 * QB, QB), bf16),
        vm((tokens + 2 * QB, QB), bf16),
        vm((nb + 2, 1, QB), jnp.int32),
        vm((4, tokens + 2 * QB, QB), bf16),
        vm((4, tokens + 2 * QB, QB), bf16),
        vm((half, heads), bf16),
        vm((half, heads), bf16),
        vm((half, heads), bf16),
        vm(w_out.shape, bf16),
        vm(w_out.shape, bf16),
        vm((half, width), bf16),
        vm((LINE, half, width), bf16),
        vm(expert_ids.shape[::-1], jnp.int32),
        vm(expert_weight.shape[::-1], f32),
        vm((LINE, experts, half), f32),
        vm((LINE, half, QB), f32),
        vm((4, width, ff), bf16),
        vm((4, width, ff), bf16),
        vm((TILES, 4 * ff, part), bf16),
        vm((LINE, half, 4 * ff), bf16),
        vm((half, part), f32),
        vm((TILES, half, part), f32),
        vm((3, TILES, half, part), bf16),
        vm((5, TILES, half, part), bf16),
        vm((2, width, units), bf16),
        vm((2, width, units), bf16),
        vm((2 * units, width), bf16),
        vm((half, 2 * units), bf16),
        vm((TILES, half, part), bf16),
        dma((8,)), dma((6,)), dma((6,)), dma((3,)), dma((3,)),
        dma((1,)), dma((WO_PIECES,)), dma((1,)), dma((WO_PIECES,)),
        *[dma((1,)) for _ in range(6)],
        dma((1,)), dma((3,)),
        dma((1,)), dma((CUTS + 1 + TILES // 2,)), dma((1,)), dma((CUTS - 1 + TILES // 2,)),
        dma((1,)), dma((1 + TILES // 2,)), dma((1,)), dma((1 + TILES // 2,)),
        dma((4,)), dma((LINE, 2)), dma((3,)), dma((5, TILES)),
        dma((1,)), dma((1,)), dma((1,)), dma((1,)), dma((1,)),
    ]
    rows = LINE * half
    return pl.pallas_call(
        layer_kernel,
        out_shape=jax.ShapeDtypeStruct((half, width), bf16),
        in_specs=[anyspace] * 3 + [pl.BlockSpec(memory_space=pltpu.SMEM)]
        + [anyspace] * 5
        + [pl.BlockSpec(memory_space=pltpu.VMEM)]
        + [anyspace] * 6,
        out_specs=anyspace,
        scratch_shapes=scratch,
        compiler_params=pltpu.CompilerParams(
            collective_id=0, has_side_effects=True, vmem_limit_bytes=63 * 1024 * 1024
        ),
        cost_estimate=pl.CostEstimate(
            flops=24 * rows * width * ff, bytes_accessed=32 * width * ff, transcendentals=rows * ff
        ),
    )(
        expert_ids.T, expert_weight.T, marks, sink_logit, queries, keys, values, w_out, residual, ffn_gain.reshape(1, -1),
        exp_gate, exp_up, exp_down, shared_gate, shared_up, shared_down,
    )


def solution(mesh):
    fits = mesh.shape["tp"] == 2 and mesh.shape["sp"] == 4 * LINE
    placed = (
        P("sp", "tp"),
        P("sp", "tp"),
        P("sp", "tp"),
        P("sp"),
        P("tp"),
        P("tp", None),
        P(("sp", "tp"), None),
        P(),
        P(("sp", "tp"), None),
        P(("sp", "tp"), None),
        P("sp", None, None),
        P("sp", None, None),
        P("sp", None, None),
        P(None, "tp"),
        P(None, "tp"),
        P("tp", None),
    )
    return jax.shard_map(
        fused_shards if fits else shards, mesh=mesh, in_specs=placed, out_specs=P(("sp", "tp"), None), check_vma=False
    )
```

```python
import math

import jax
import jax.numpy as jnp
from jax import lax
from jax.experimental import pallas as pl
from jax.experimental.pallas import tpu as pltpu
from jax.sharding import PartitionSpec as P

HD = 64
WINDOW = 128
PARTS = 2


norm_eps = 1e-06


def extended(cells, sides, width):
    for axis, dim in sides:
        count = lax.axis_size(axis)
        ends = count - 1
        head = lax.slice_in_dim(cells, 0, width, axis=dim)
        tail = lax.slice_in_dim(cells, cells.shape[dim] - width, cells.shape[dim], axis=dim)
        cells = jnp.concatenate(
            [
                lax.ppermute(tail, axis, [(i, (i + 1) % count) for i in range(ends)]),
                cells,
                lax.ppermute(head, axis, [((i + 1) % count, i) for i in range(ends)]),
            ],
            axis=dim,
        )
    return cells


def band_blocks(padded, width):
    span_count = padded.shape[0] // width - 2
    shaped = padded.reshape((span_count + 2, width) + padded.shape[1:])
    return jnp.concatenate(
        [
            shaped[0:span_count:2],
            shaped[1 : span_count + 1 : 2],
            shaped[2 : span_count + 2 : 2],
            shaped[3 : span_count + 3 : 2],
        ],
        axis=1,
    )


def attend(queries, ext_keys, ext_values, ext_marks, own_marks, sink_logit):
    tok_count = queries.shape[0]
    head_count = sink_logit.shape[0]
    key_heads = ext_keys.shape[1] // HD
    group_size = head_count // key_heads
    query_span = 2 * WINDOW
    block_count = tok_count // query_span
    query_blocks = queries.reshape(block_count, query_span, key_heads, group_size, HD)
    key_blocks = band_blocks(ext_keys, WINDOW).reshape(block_count, 4 * WINDOW, key_heads, HD)
    value_blocks = band_blocks(ext_values, WINDOW).reshape(block_count, 4 * WINDOW, key_heads, HD)
    mark_blocks = band_blocks(ext_marks, WINDOW)
    query_marks = own_marks.reshape(block_count, query_span)
    scores = jnp.einsum(
        "nqkgd,nmkd->nkgqm", query_blocks, key_blocks, preferred_element_type=jnp.float32
    ) * HD ** (-0.5)
    offset = (
        jnp.arange(query_span, dtype=jnp.int32)[:, None]
        - jnp.arange(4 * WINDOW, dtype=jnp.int32)[None, :]
        + WINDOW
    )
    allowed = (jnp.abs(offset) <= WINDOW)[None] & (
        mark_blocks[:, None, :] == query_marks[:, :, None]
    )
    scores = jnp.where(allowed[:, None, None], scores, -jnp.inf)
    sink_term = sink_logit.reshape(key_heads, group_size)[None, :, :, None, None]
    row_max = jnp.maximum(jnp.max(scores, axis=-1, keepdims=True), sink_term)
    exp_scores = jnp.exp(scores - row_max)
    attn_probs = (
        exp_scores / (jnp.sum(exp_scores, axis=-1, keepdims=True) + jnp.exp(sink_term - row_max))
    ).astype(jnp.bfloat16)
    result = jnp.einsum(
        "nkgqm,nmkd->nqkgd", attn_probs, value_blocks, preferred_element_type=jnp.float32
    )
    return result.astype(jnp.bfloat16).reshape(tok_count, head_count * HD)


def expert_kernel(rows_ref, scale_ref, gate_ref, up_ref, down_ref, side_ref, side_down_ref, out_ref):
    rows = rows_ref[...]
    gated = jnp.dot(rows, gate_ref[...], preferred_element_type=jnp.float32)
    lifted = jnp.dot(rows, up_ref[...], preferred_element_type=jnp.float32)
    hidden = (gated / (1.0 + jnp.exp(-gated)) * lifted).astype(jnp.bfloat16)
    produced = jnp.dot(hidden, down_ref[...], preferred_element_type=jnp.float32)
    side = jnp.dot(rows, side_ref[...], preferred_element_type=jnp.float32)
    width = side.shape[1] // 2
    side_gate, side_up = side[:, :width], side[:, width:]
    side_hidden = (side_gate / (1.0 + jnp.exp(-side_gate)) * side_up).astype(jnp.bfloat16)
    shared = jnp.dot(side_hidden, side_down_ref[...], preferred_element_type=jnp.float32)
    out_ref[...] = (
        scale_ref[...] * produced.astype(jnp.bfloat16).astype(jnp.float32) + shared
    ).astype(jnp.bfloat16)


def run_experts(rows, scale, gate_w, up_w, down_w, side_w, side_down):
    count, width = rows.shape
    tile = math.gcd(count, 256)
    whole = lambda w: pl.BlockSpec(w.shape, lambda i: (0, 0))
    units = gate_w.shape[1] + side_w.shape[1] // 2
    return pl.pallas_call(
        expert_kernel,
        grid=(count // tile,),
        in_specs=[
            pl.BlockSpec((tile, width), lambda i: (i, 0)),
            pl.BlockSpec((tile, 1), lambda i: (i, 0)),
            whole(gate_w),
            whole(up_w),
            whole(down_w),
            whole(side_w),
            whole(side_down),
        ],
        out_specs=pl.BlockSpec((tile, width), lambda i: (i, 0)),
        out_shape=jax.ShapeDtypeStruct((count, width), jnp.bfloat16),
        compiler_params=pltpu.CompilerParams(
            dimension_semantics=("arbitrary",), vmem_limit_bytes=48 * 1024 * 1024
        ),
        cost_estimate=pl.CostEstimate(
            flops=6 * count * width * units,
            bytes_accessed=4 * count * width + 6 * units * width,
            transcendentals=count * units,
        ),
    )(rows, scale, gate_w, up_w, down_w, side_w, side_down)


def shared_slice(shared_gate, shared_up, shared_down):
    sp_count, tp_count = lax.axis_size("sp"), lax.axis_size("tp")
    own, side = lax.axis_index("tp"), lax.axis_index("sp")
    units = shared_gate.shape[1] * tp_count // sp_count
    per_owner = sp_count // tp_count
    owner, offset = side // per_owner, (side % per_owner) * units
    held = jnp.concatenate(
        [
            lax.dynamic_slice_in_dim(shared_gate, offset, units, axis=1).T,
            lax.dynamic_slice_in_dim(shared_up, offset, units, axis=1).T,
            lax.dynamic_slice_in_dim(shared_down, offset, units, axis=0),
        ],
        axis=0,
    )
    chosen = held
    for shift in range(1, tp_count):
        came = lax.ppermute(held, "tp", [(i, (i + shift) % tp_count) for i in range(tp_count)])
        chosen = jnp.where((own - shift) % tp_count == owner, came, chosen)
    padded = -(-units // 128) * 128
    grown = [
        jnp.pad(chosen[i * units : (i + 1) * units], ((0, padded - units), (0, 0))) for i in range(3)
    ]
    return jnp.concatenate(grown[:2], axis=0).T, grown[2]


def shards(
    queries,
    keys,
    values,
    doc_ids,
    sink_logit,
    w_out,
    residual,
    ffn_gain,
    expert_ids,
    expert_weight,
    exp_gate,
    exp_up,
    exp_down,
    shared_gate,
    shared_up,
    shared_down,
):
    marks = (doc_ids + 1).astype(jnp.bfloat16)
    kv = keys.shape[1]
    joined = jnp.concatenate(
        [keys, values, jnp.broadcast_to(marks[:, None], (marks.shape[0], 128))], axis=1
    )
    extended_all = extended(joined, (("sp", 0),), WINDOW)
    ext_keys, ext_values, ext_marks = (
        extended_all[:, :kv],
        extended_all[:, kv : 2 * kv],
        extended_all[:, 2 * kv],
    )
    attended = attend(queries, ext_keys, ext_values, ext_marks, marks, sink_logit)
    row_count = residual.shape[0]
    mixed = lax.psum_scatter(
        jnp.dot(attended, w_out, preferred_element_type=jnp.float32).astype(jnp.bfloat16),
        "tp",
        scatter_dimension=0,
        tiled=True,
    ).astype(jnp.float32)
    resid = (residual.astype(jnp.float32) + mixed).astype(jnp.bfloat16)
    resid_f = resid.astype(jnp.float32)
    normed = (
        resid_f
        * lax.rsqrt(jnp.mean(resid_f * resid_f, axis=-1, keepdims=True) + norm_eps)
        * ffn_gain
    ).astype(jnp.bfloat16)
    side_w, side_down = shared_slice(shared_gate, shared_up, shared_down)
    sp_count = lax.axis_size("sp")
    chosen = expert_ids[:, :, None] == jnp.arange(sp_count, dtype=jnp.int32)
    table = jnp.sum(jnp.where(chosen, expert_weight[:, :, None], 0.0), axis=1)
    scales = lax.all_to_all(table.T, "sp", split_axis=0, concat_axis=0, tiled=True)
    part_rows = row_count // PARTS
    sums = []
    for part in range(PARTS):
        begin = part * part_rows
        gathered = lax.all_gather(normed[begin : begin + part_rows], "sp", axis=0, tiled=True)
        scale = scales[:, begin : begin + part_rows].reshape(-1, 1)
        produced = run_experts(
            gathered, scale, exp_gate[0], exp_up[0], exp_down[0], side_w, side_down
        )
        sums.append(lax.psum_scatter(produced, "sp", scatter_dimension=0, tiled=True))
    added = jnp.concatenate(sums, axis=0)
    return (resid.astype(jnp.float32) + added.astype(jnp.float32)).astype(jnp.bfloat16)


MESH = pl.DeviceIdType.MESH
QB = 128
NEG = -1e30
LINE = 4
WO_PIECES = 4
TILES = 8
CUTS = 8


def layer_kernel(
    ids_in, wts_in, marks_in, sink_ref, q_in, k_in, v_in, wo_in, res_in, gain_ref,
    eg_in, eu_in, ed_in, sg_in, su_in, sd_in,
    out_ref,
    q_s, kx, vx, marks, kk, vv, a_out, a_own, a_in, wo_own, wo_oth, res, tok, ids, wts, tab, tabt,
    gs, us, ds, hid, acc, base, stage, rbuf, sg, su, sd, sh, ost,
    loc, halo_s, halo_r, tab_s, tab_r, wx_s, wx_r, wz_s, wz_r, wf_s, wf_r, wg_s, wg_r, att_s, att_r,
    sib_s, sib_r, y_s, y_r, x_s, x_r, fy_s, fy_r, fx_s, fx_r,
    ag_s, ag_r, rs_s, rs_r, sx_s, sx_r, ss_s, ss_r, out_sem,
):
    f32, bf16 = jnp.float32, jnp.bfloat16
    sp_count, tp_count = lax.axis_size("sp"), lax.axis_size("tp")
    s, x = lax.axis_index("sp"), lax.axis_index("tp")
    z, y, c = s // 4, lax.rem(s // 2, 2), lax.rem(s, 2)
    ox, oy, oc = 1 - x, 1 - y, 1 - c
    at = lambda zz, yy, cc: (zz * 2 + yy) * 2 + cc
    dev = lambda sp, tp: {"sp": sp, "tp": tp}
    sib, ypar, xpar = dev(at(z, y, oc), x), dev(at(z, oy, c), x), dev(s, ox)
    nxt, prv = dev(lax.rem(s + 1, sp_count), x), dev(lax.rem(s + sp_count - 1, sp_count), x)
    low = z < 2
    w = jnp.where(low, z, 3 - z)
    inner = w == 1
    zf = jnp.where(low, z + 1, z - 1)
    zb = jnp.clip(jnp.where(low, z - 1, z + 1), 0, 3)
    fwd, bck = dev(at(zf, y, c), x), dev(at(zb, y, c), x)
    line = lambda ob: jnp.where(low, ob, 3 - ob)
    tokens = q_in.shape[0]
    half = tokens // 2
    width = res_in.shape[1]
    ff = eg_in.shape[2]
    part = width // TILES

    def send(src, dst, ss, rs, to):
        cp = pltpu.make_async_remote_copy(
            src_ref=src, dst_ref=dst, send_sem=ss, recv_sem=rs, device_id=to, device_id_type=MESH
        )
        cp.start()
        return cp

    def got(view, rs):
        pltpu.make_async_remote_copy(
            src_ref=view, dst_ref=view, send_sem=rs, recv_sem=rs, device_id=sib, device_id_type=MESH
        ).wait_recv()

    def sent(view, ss):
        pltpu.make_async_remote_copy(
            src_ref=view, dst_ref=view, send_sem=ss, recv_sem=ss, device_id=sib, device_id_type=MESH
        ).wait_send()

    def amount(elements):
        return ds.at[:, pl.ds(0, elements // (TILES * part))]

    def load(src, dst, sem):
        cp = pltpu.make_async_copy(src, dst, sem)
        cp.start()
        return cp

    rows_own = pl.ds(QB, tokens)
    loads_a = [
        load(q_in, q_s, loc.at[0]),
        load(k_in, kx.at[rows_own], loc.at[1]),
        load(v_in, vx.at[rows_own], loc.at[2]),
        load(marks_in, marks.at[pl.ds(1, tokens // QB)], loc.at[3]),
        load(ids_in, ids, loc.at[4]),
        load(wts_in, wts, loc.at[5]),
    ]
    loads_b = [
        load(wo_in, wo_own, loc.at[6]),
        load(res_in, res, loc.at[7]),
        load(eg_in.at[0], gs.at[0], loc.at[6]),
        load(eu_in.at[0], us.at[0], loc.at[6]),
        load(sg_in, sg.at[0], loc.at[7]),
        load(su_in, su.at[0], loc.at[7]),
        load(sd_in, sd.at[pl.ds(0, sd_in.shape[0])], loc.at[7]),
    ]
    for n in range(TILES):
        loads_b.append(
            load(ed_in.at[0, :, pl.ds(n * part, part)], ds.at[n, pl.ds(0, ff)], loc.at[6])
        )

    barrier = pltpu.get_barrier_semaphore()
    zs = [lax.rem(z + i, LINE) for i in range(1, LINE)]
    partners = [nxt, prv, sib, ypar, xpar] + [dev(at(zz, y, c), x) for zz in zs]
    for to in partners:
        pl.semaphore_signal(barrier, inc=1, device_id=to, device_id_type=MESH)
    pl.semaphore_wait(barrier, len(partners))

    pend = []
    last, first = pl.ds(tokens - QB, QB), pl.ds(0, QB)
    after = pl.ds(QB + tokens, QB)
    nb = tokens // QB
    for i, (src, dst, lo, hi, a, b) in enumerate(
        [(k_in, kx, first, after, last, first), (v_in, vx, first, after, last, first)]
    ):
        pend.append(send(src.at[a], dst.at[lo], halo_s.at[2 * i], halo_r.at[2 * i], nxt))
        pend.append(send(src.at[b], dst.at[hi], halo_s.at[2 * i + 1], halo_r.at[2 * i + 1], prv))
    pend.append(send(marks_in.at[nb - 1], marks.at[0], halo_s.at[4], halo_r.at[4], nxt))
    pend.append(send(marks_in.at[0], marks.at[nb + 1], halo_s.at[5], halo_r.at[5], prv))

    pair = dev(at(jnp.where(inner, zb, zf), y, c), x)
    wrows = wo_in.shape[0] // (4 * WO_PIECES)
    wpiece = lambda pos, core, i: pl.ds(
        pl.multiple_of(((pos * 2 + core) * WO_PIECES + i) * wrows, wrows), wrows
    )
    for i in range(WO_PIECES):
        rows = wpiece(w, c, i)
        send(wo_in.at[rows], wo_oth.at[rows], wx_s.at[0], wx_r.at[i], xpar)

    def wx_event(i):
        view = wo_oth.at[wpiece(w, c, i)]
        got(view, wx_r.at[i])
        send(view, view, wz_s.at[0], wz_r.at[i], pair)
        send(view, view, wf_s.at[0], wf_r.at[0], sib)

    def wz_event(i):
        view = wo_oth.at[wpiece(1 - w, c, i)]
        got(view, wz_r.at[i])
        send(view, view, wg_s.at[0], wg_r.at[0], sib)

    quarter = width // CUTS

    def piece(refs, kind, i, slot):
        g, u, d = refs
        if kind == "g":
            return g.at[slot, pl.ds(i * quarter, quarter)]
        if kind == "u":
            return u.at[slot, pl.ds(i * quarter, quarter)]
        if slot is None:
            return d.at[0, :, pl.ds(i * part, part)]
        return d.at[i, pl.ds(slot * ff, ff)]

    def hbm_piece(kind, i):
        if kind == "g":
            return eg_in.at[0, pl.ds(i * quarter, quarter)]
        if kind == "u":
            return eu_in.at[0, pl.ds(i * quarter, quarter)]
        return ed_in.at[0, :, pl.ds(pl.multiple_of(i * part, part), part)]

    held = (gs, us, ds)
    gates, ups = CUTS // 2, CUTS // 2 - 1
    own_only = lambda v: [("g", gates * v + i) for i in range(gates)] + [
        ("u", ups * v + i) for i in range(ups)
    ]
    tiles_of = lambda v: [("d", 2 * i + v) for i in range(TILES // 2)]
    both = [("u", i) for i in range(2 * ups, CUTS)]
    y_list = own_only(x) + both + tiles_of(x)
    x_list = own_only(ox) + tiles_of(ox)
    x_gu = gates + ups
    y_gu = x_gu + len(both)
    relayed = {i: i if i < x_gu else i - len(both) for i in range(len(y_list)) if i < x_gu or i >= y_gu}
    for i, (kind, j) in enumerate(y_list):
        send(hbm_piece(kind, j), piece(held, kind, j, 2), y_s.at[0], y_r.at[i], ypar)

    def y_event(i):
        kind, j = y_list[i]
        view = piece(held, kind, j, 2)
        got(view, y_r.at[i])
        if i in relayed:
            k = relayed[i]
            send(view, view, x_s.at[0], x_r.at[k], xpar)
        send(view, piece(held, kind, j, 3), fy_s.at[0], fy_r.at[max(0, i - y_gu + 1)], sib)

    def x_event(i):
        kind, j = x_list[i]
        view = piece(held, kind, j, 2)
        got(view, x_r.at[i])
        send(view, piece(held, kind, j, 3), fx_s.at[0], fx_r.at[max(0, i - x_gu + 1)], sib)

    for cp in loads_a:
        cp.wait()
    named = lax.broadcasted_iota(jnp.int32, tab.shape[1:], 0)
    table = jnp.zeros(tab.shape[1:], f32)
    for k in range(ids.shape[0]):
        table = table + jnp.where(named == ids[k : k + 1], wts[k : k + 1], 0.0)
    tab[z] = table
    for i, zz in enumerate(zs):
        pend.append(
            send(tab.at[z], tab.at[z], tab_s.at[i], tab_r.at[LINE - 2 - i], dev(at(zz, y, c), x))
        )
    for i in range(2):
        dst = (kx, vx)[i]
        got(dst.at[first], halo_r.at[2 * i])
        got(dst.at[after], halo_r.at[2 * i + 1])
    got(marks.at[0], halo_r.at[4])
    got(marks.at[nb + 1], halo_r.at[5])

    @pl.when(s == 0)
    def _():
        marks[0] = jnp.full(marks.shape[1:], -1, jnp.int32)

    @pl.when(s == sp_count - 1)
    def _():
        marks[nb + 1] = jnp.full(marks.shape[1:], -1, jnp.int32)

    ri = lax.broadcasted_iota(jnp.int32, (QB, QB), 0)
    ci = lax.broadcasted_iota(jnp.int32, (QB, QB), 1)
    swap = jnp.where(ci == lax.rem(ri + HD, QB), 1.0, 0.0).astype(bf16)

    def spread(t, carry):
        rows = pl.ds(pl.multiple_of(t * QB, QB), QB)
        for src, dst in ((kx, kk), (vx, vv)):
            cur = src[rows]
            turned = jnp.dot(cur, swap, preferred_element_type=f32)
            cur = cur.astype(f32)
            zero = jnp.zeros_like(cur)
            left = ci < HD
            dst[0, rows] = jnp.where(left, cur, zero).astype(bf16)
            dst[1, rows] = jnp.where(left, zero, turned).astype(bf16)
            dst[2, rows] = jnp.where(left, turned, zero).astype(bf16)
            dst[3, rows] = jnp.where(left, zero, cur).astype(bf16)
        return carry

    lax.fori_loop(0, nb + 2, spread, 0)

    def attend_rows(blk, dst, drow):
        rows = pl.ds(pl.multiple_of(blk * QB, QB), QB)
        span = pl.ds(pl.multiple_of(blk * QB, QB), 3 * QB)
        mine = jnp.broadcast_to(marks[blk + 1][0:1], (QB, QB)).T
        biases = []
        for t in range(3):
            same = mine == jnp.broadcast_to(marks[blk + t][0:1], (QB, QB))
            if t == 0:
                same = same & (ri <= ci)
            if t == 2:
                same = same & (ci <= ri)
            biases.append(jnp.where(same, 0.0, NEG).astype(f32))
        bias = jnp.concatenate(biases, axis=1)
        for j in range(q_s.shape[1] // QB):
            g = j // 2
            keys2 = jnp.concatenate([kk[2 * g, span], kk[2 * g + 1, span]], axis=0)
            vals2 = jnp.concatenate([vv[2 * g, span], vv[2 * g + 1, span]], axis=0)
            sc = lax.dot_general(
                q_s[rows, j * QB : (j + 1) * QB], keys2, (((1,), (1,)), ((), ())),
                preferred_element_type=f32,
            ) * HD ** (-0.5)
            probs = []
            for h in range(2):
                sink = sink_ref[2 * j + h]
                own = sc[:, h * 3 * QB : (h + 1) * 3 * QB] + bias
                top = jnp.maximum(jnp.max(own, axis=-1, keepdims=True), sink)
                e = jnp.exp(own - top)
                total = jnp.sum(e, axis=-1, keepdims=True) + jnp.exp(sink - top)
                probs.append((e * (1.0 / total)).astype(bf16))
            o = jnp.dot(jnp.concatenate(probs, axis=1), vals2, preferred_element_type=f32)
            dst[pl.ds(pl.multiple_of(drow, QB), QB), j * QB : (j + 1) * QB] = o.astype(bf16)

    hb = half // QB

    for i in range(hb):
        attend_rows(ox * hb + i, a_out, i * QB)
        rows = pl.ds(i * QB, QB)
        send(a_out.at[rows], a_in.at[rows], att_s.at[0], att_r.at[0], xpar)
        wx_event(i)
    send(eg_in.at[0], gs.at[1], sib_s.at[0], sib_r.at[0], sib)
    send(eu_in.at[0], us.at[1], sib_s.at[0], sib_r.at[1], sib)
    for n in range(TILES):
        send(hbm_piece("d", n), piece(held, "d", n, 1), sib_s.at[0], sib_r.at[2], sib)
    for i in range(hb):
        attend_rows(x * hb + i, a_own, i * QB)
        wx_event(hb + i)

    y_event(0)
    first_loads = wo_in.size + 3 * eg_in.size
    for i, elements in ((6, first_loads), (7, res_in.size + 3 * sg_in.size)):
        view = amount(elements)
        pltpu.make_async_copy(view, view, loc.at[i]).wait()
    for n in range(TILES):
        cols = slice(n * part, (n + 1) * part)
        base[n] = res[:, cols].astype(f32) + jnp.dot(
            a_own[...], wo_own[:, cols], preferred_element_type=f32
        )
    for i in range(WO_PIECES):
        wz_event(i)
    got(a_in, att_r.at[0])
    got(amount(wo_in.size // 4), wf_r.at[0])
    got(amount(wo_in.size // 4), wg_r.at[0])
    square = jnp.zeros((half, 1), f32)
    for n in range(TILES):
        cols = slice(n * part, (n + 1) * part)
        r = (
            base[n] + jnp.dot(a_in[...], wo_oth[:, cols], preferred_element_type=f32)
        ).astype(bf16)
        res[:, cols] = r
        rf = r.astype(f32)
        square = square + jnp.sum(rf * rf, axis=-1, keepdims=True)
    inv = lax.rsqrt(square * (1.0 / width) + norm_eps)
    for n in range(4):
        cols = slice(n * (width // 4), (n + 1) * (width // 4))
        tok[z, :, cols] = (res[:, cols].astype(f32) * inv * gain_ref[:, cols]).astype(bf16)

    hr = half // 2
    rows_of = lambda r: pl.ds(r * hr, hr)

    def ag_send(b, r, direction, to):
        view = tok.at[b, rows_of(r)]
        send(view, view, ag_s.at[direction], ag_r.at[b, r], to)

    def ag_got(b, r):
        got(tok.at[b, rows_of(r)], ag_r.at[b, r])

    for r in range(2):
        ag_send(z, r, 0, fwd)

        @pl.when(inner)
        def _():
            ag_send(z, r, 1, bck)

    def relay(ob, r):
        b = line(ob)

        @pl.when(inner)
        def _():
            ag_got(b, r)
            if ob == 0:
                ag_send(b, r, 2, fwd)
            else:
                ag_send(b, r, 3, bck)

    def table_columns(b, carry):
        t = tab[b]
        grown = jnp.concatenate([t, jnp.zeros((QB - t.shape[0], t.shape[1]), f32)], axis=0)
        tabt[b] = grown.T
        return carry

    def gated(rows, gate, up):
        a = jnp.dot(rows, gate, preferred_element_type=f32)
        b = jnp.dot(rows, up, preferred_element_type=f32)
        return a / (1.0 + jnp.exp(-a)) * b

    def hidden(b, lo, hi, rows=slice(None)):
        def one(slot, carry):
            e = at(z, jnp.where(slot >= 2, oy, y), jnp.where(lax.rem(slot, 2) == 1, oc, c))
            weights = tabt[b, rows]
            mine = lax.broadcasted_iota(jnp.int32, weights.shape, 1) == e
            scale = jnp.sum(jnp.where(mine, weights, 0.0), axis=-1, keepdims=True)
            for h in range(2):
                cols = slice(h * (ff // 2), (h + 1) * (ff // 2))
                v = gated(tok[b, rows], gs[slot, :, cols], us[slot, :, cols]) * scale
                to = pl.ds(pl.multiple_of(slot * ff + h * (ff // 2), ff // 2), ff // 2)
                hid[b, rows, to] = v.astype(bf16)
            return carry

        lax.fori_loop(lo, hi, one, 0)

    y_event(1)
    for i in range(LINE - 1):
        got(tab.at[z], tab_r.at[i])
    lax.fori_loop(0, LINE, table_columns, 0)
    got(gs.at[1], sib_r.at[0])
    got(us.at[1], sib_r.at[1])
    y_event(2)
    hidden(z, 0, 2)
    y_event(3)
    x_event(0)
    relay(0, 0)
    relay(2, 0)
    x_event(1)
    y_event(4)
    x_event(2)
    y_event(5)
    relay(0, 1)
    relay(2, 1)
    x_event(3)
    y_event(6)
    near, far2, far3 = line(1 - w), line(2), line(3)

    def end_got(b):
        @pl.when(w == 0)
        def _():
            ag_got(b, 0)
            ag_got(b, 1)

    end_got(near)
    hidden(near, 0, 2)
    x_event(4)
    y_event(7)
    x_event(5)
    y_event(8)
    relay(3, 0)

    @pl.when(w == 0)
    def _():
        ag_got(far2, 0)
        hidden(far2, 0, 2, slice(0, hr))

    @pl.when(inner)
    def _():
        hidden(far2, 0, 2)

    x_event(6)
    y_event(9)
    hidden(near, 2, 3)
    cut = quarter * ff
    got(amount(y_gu * cut), fy_r.at[0])
    got(amount(x_gu * cut), fx_r.at[0])
    hidden(near, 3, 4)
    got(amount(ed_in.size), sib_r.at[2])
    srow, drow = sg_in.shape[0] // 2, sd_in.shape[0] // 2
    shared_views = lambda core: [
        sg.at[1, pl.ds(core * srow, srow)],
        su.at[1, pl.ds(core * srow, srow)],
        sd.at[pl.ds(sd_in.shape[0] + core * drow, drow)],
    ]
    shared_parts = [
        sg_in.at[pl.ds(c * srow, srow)],
        su_in.at[pl.ds(c * srow, srow)],
        sd_in.at[pl.ds(c * drow, drow)],
    ]

    order = [2 * (k // 2) + (x if k % 2 == 0 else ox) for k in range(TILES)]
    tile = lambda slot, n: rbuf.at[slot, n]

    def down(b, n):
        return jnp.dot(hid[b], ds[n], preferred_element_type=f32)

    def reduce_piece(step, n, place=None):
        b = jnp.where(step == 2, near, line(2 + step))
        slot = jnp.where(step == 0, 3 * w, jnp.where(step == 1, 1 + w, 4 - w))
        zt = jnp.where((step == 2) & inner, zb, zf)

        def add():
            got(tile(step, n), rs_r.at[step, n])
            stage[step, n] = (acc[...] + rbuf[step, n].astype(f32)).astype(bf16)

        if place == "end":
            stage[step, n] = down(b, n).astype(bf16)
        else:
            acc[...] = down(b, n)
            if place == "inner":
                add()
            else:
                pl.when(inner)(add)

                @pl.when(w == 0)
                def _():
                    stage[step, n] = acc[...].astype(bf16)

        send(
            stage.at[step, n], tile(slot, n), rs_s.at[step], rs_r.at[slot, n], dev(at(zt, y, c), x)
        )

    def nth(k):
        return 2 * (k // 2) + jnp.where(lax.rem(k, 2) == 0, x, ox)

    def down_got(k):
        lst, sem, first_d = (y_list, fy_r, y_gu) if k % 2 == 0 else (x_list, fx_r, x_gu)
        kind, j = lst[first_d + k // 2]
        got(piece(held, kind, j, 3), sem.at[1 + k // 2])

    def at_end(step, k):
        @pl.when(w == 0)
        def _():
            reduce_piece(step, order[k], "end")

    def at_inner(step, k):
        @pl.when(inner)
        def _():
            reduce_piece(step, order[k], "inner")

    early = TILES // 2
    down_got(0)
    at_end(2, 0)

    @pl.when(w == 0)
    def _():
        hidden(far2, 2, 4, slice(0, hr))

    x_event(7)
    down_got(1)
    at_end(2, 1)
    y_event(10)
    down_got(2)
    at_end(2, 2)
    relay(3, 1)

    @pl.when(w == 0)
    def _():
        ag_got(far2, 1)
        hidden(far2, 0, 4, slice(hr, half))

    @pl.when(inner)
    def _():
        hidden(far2, 2, 4)

    for k in range(early - 1):
        at_end(0, k)
    x_event(8)
    y_event(11)
    down_got(3)
    at_end(2, 3)
    at_end(0, 3)

    @pl.when(inner)
    def _():
        hidden(far3, 0, 4)

    y_event(12)
    for i, (src, dst) in enumerate(zip(shared_parts, shared_views(c))):
        send(src, dst, sx_s.at[0], sx_r.at[0], xpar)
    x_event(9)

    def a_tiles(k, carry):
        reduce_piece(0, nth(k), "inner")
        return carry

    @pl.when(inner)
    def _():
        lax.fori_loop(0, 2, a_tiles, 0)

    for k in range(4, 7):
        down_got(k)
        at_end(0, k)

    @pl.when(inner)
    def _():
        lax.fori_loop(2, 4, a_tiles, 0)

    hidden(z, 2, 4)

    @pl.when(w == 0)
    def _():
        ag_got(far3, 0)
        hidden(far3, 0, 4, slice(0, hr))

    x_event(10)
    down_got(7)
    at_end(0, 7)

    def own_sum(n, carry):
        cols = pl.ds(pl.multiple_of(n * part, part), part)
        base[n] = res[:, cols].astype(f32) + down(z, n)
        return carry

    @pl.when(inner)
    def _():
        lax.fori_loop(4, 5, a_tiles, 0)
        lax.fori_loop(0, TILES, own_sum, 0)
        lax.fori_loop(5, TILES, a_tiles, 0)

    @pl.when(w == 0)
    def _():
        ag_got(far3, 1)
        hidden(far3, 0, 4, slice(hr, half))

    lag = 3
    turns = 2 * TILES - lag

    def later(i, carry):
        odd = lax.rem(i - lag, 2) == 0
        far = (i < lag) | ((i < turns) & ~odd)
        in_step = jnp.where(far, 1, 2)
        far_k = jnp.where(i < lag, i, (i + lag - 1) // 2)
        near_k = jnp.where(i < turns, (i - lag) // 2, i - TILES)
        step = jnp.where(inner, in_step, jnp.where(i < TILES, 1, 2))
        k = jnp.where(inner, jnp.where(far, far_k, near_k), jnp.where(i < TILES, i, i - TILES + early))
        reduce_piece(step, nth(k))
        return carry

    at_once = 2 * TILES - early

    block = half * width

    def drain():
        for cp in pend:
            cp.wait_send()
        for sem, elements in (
            (wx_s, wo_in.size // 4), (wz_s, wo_in.size // 4), (wf_s, wo_in.size // 4),
            (wg_s, wo_in.size // 4), (att_s, a_out.size), (sib_s, 3 * eg_in.size),
            (y_s, len(y_list) * cut), (x_s, len(x_list) * cut), (fy_s, len(y_list) * cut),
            (fx_s, len(x_list) * cut), (ag_s, block),
        ):
            sent(amount(elements), sem.at[0])

    @pl.when(inner)
    def _():
        drain()
        for i, elements in ((1, block), (2, block), (3, 2 * block)):
            sent(amount(elements), ag_s.at[i])

    lax.fori_loop(0, 2, later, 0)

    @pl.when(w == 0)
    def _():
        lax.fori_loop(0, TILES, own_sum, 0)

    middle = at_once + w
    lax.fori_loop(2, middle, later, 0)
    pl.when(w == 0)(drain)

    shared_size = 3 * sg_in.size // 2
    got(amount(shared_size), sx_r.at[0])
    for view in shared_views(c):
        send(view, view, ss_s.at[0], ss_r.at[0], sib)
    lax.fori_loop(middle, at_once + early * w, later, 0)
    got(amount(shared_size), ss_r.at[0])
    units = sg_in.shape[1]
    for h in range(2):
        sh[:, h * units : (h + 1) * units] = gated(tok[z], sg[h], su[h]).astype(bf16)

    def shared_sum(n, carry):
        cols = pl.ds(pl.multiple_of(n * part, part), part)
        base[n] = base[n] + jnp.dot(sh[...], sd[:, cols], preferred_element_type=f32)
        return carry

    lax.fori_loop(0, TILES, shared_sum, 0)

    def final(k, carry):
        n = nth(k)
        cols = pl.ds(pl.multiple_of(n * part, part), part)
        got(tile(3, n), rs_r.at[3, n])
        acc[...] = base[n] + rbuf[3, n].astype(f32)

        @pl.when(inner)
        def _():
            got(tile(4, n), rs_r.at[4, n])
            acc[...] = acc[...] + rbuf[4, n].astype(f32)

        ost[n] = acc[...].astype(bf16)
        load(ost.at[n], out_ref.at[:, cols], out_sem.at[0])
        return carry

    def steps_sent(steps):
        for step in steps:
            sent(amount(block), rs_s.at[step])

    steps_sent((0, 1))
    lax.fori_loop(0, TILES, final, 0)

    sent(amount(shared_size), sx_s.at[0])
    sent(amount(shared_size), ss_s.at[0])
    steps_sent((2,))
    pltpu.make_async_copy(amount(block), amount(block), out_sem.at[0]).wait()


def fused_shards(
    queries, keys, values, doc_ids, sink_logit, w_out, residual, ffn_gain, expert_ids,
    expert_weight, exp_gate, exp_up, exp_down, shared_gate, shared_up, shared_down,
):
    bf16, f32 = jnp.bfloat16, jnp.float32
    experts = lax.axis_size("sp")
    tokens = queries.shape[0]
    nb = tokens // QB
    marks = doc_ids.reshape(nb, 1, QB)
    half, width = residual.shape
    ff = exp_gate.shape[2]
    part = width // TILES
    units = shared_gate.shape[1]
    heads = queries.shape[1]
    vm = pltpu.VMEM
    dma = pltpu.SemaphoreType.DMA
    anyspace = pl.BlockSpec(memory_space=pl.ANY)
    scratch = [
        vm((tokens, heads), bf16),
        vm((tokens + 2 * QB, QB), bf16),
        vm((tokens + 2 * QB, QB), bf16),
        vm((nb + 2, 1, QB), jnp.int32),
        vm((4, tokens + 2 * QB, QB), bf16),
        vm((4, tokens + 2 * QB, QB), bf16),
        vm((half, heads), bf16),
        vm((half, heads), bf16),
        vm((half, heads), bf16),
        vm(w_out.shape, bf16),
        vm(w_out.shape, bf16),
        vm((half, width), bf16),
        vm((LINE, half, width), bf16),
        vm(expert_ids.shape[::-1], jnp.int32),
        vm(expert_weight.shape[::-1], f32),
        vm((LINE, experts, half), f32),
        vm((LINE, half, QB), f32),
        vm((4, width, ff), bf16),
        vm((4, width, ff), bf16),
        vm((TILES, 4 * ff, part), bf16),
        vm((LINE, half, 4 * ff), bf16),
        vm((half, part), f32),
        vm((TILES, half, part), f32),
        vm((3, TILES, half, part), bf16),
        vm((5, TILES, half, part), bf16),
        vm((2, width, units), bf16),
        vm((2, width, units), bf16),
        vm((2 * units, width), bf16),
        vm((half, 2 * units), bf16),
        vm((TILES, half, part), bf16),
        dma((8,)), dma((6,)), dma((6,)), dma((3,)), dma((3,)),
        dma((1,)), dma((WO_PIECES,)), dma((1,)), dma((WO_PIECES,)),
        *[dma((1,)) for _ in range(6)],
        dma((1,)), dma((3,)),
        dma((1,)), dma((CUTS + 1 + TILES // 2,)), dma((1,)), dma((CUTS - 1 + TILES // 2,)),
        dma((1,)), dma((1 + TILES // 2,)), dma((1,)), dma((1 + TILES // 2,)),
        dma((4,)), dma((LINE, 2)), dma((3,)), dma((5, TILES)),
        dma((1,)), dma((1,)), dma((1,)), dma((1,)), dma((1,)),
    ]
    rows = LINE * half
    return pl.pallas_call(
        layer_kernel,
        out_shape=jax.ShapeDtypeStruct((half, width), bf16),
        in_specs=[anyspace] * 3 + [pl.BlockSpec(memory_space=pltpu.SMEM)]
        + [anyspace] * 5
        + [pl.BlockSpec(memory_space=pltpu.VMEM)]
        + [anyspace] * 6,
        out_specs=anyspace,
        scratch_shapes=scratch,
        compiler_params=pltpu.CompilerParams(
            collective_id=0, has_side_effects=True, vmem_limit_bytes=63 * 1024 * 1024
        ),
        cost_estimate=pl.CostEstimate(
            flops=24 * rows * width * ff, bytes_accessed=32 * width * ff, transcendentals=rows * ff
        ),
    )(
        expert_ids.T, expert_weight.T, marks, sink_logit, queries, keys, values, w_out, residual, ffn_gain.reshape(1, -1),
        exp_gate, exp_up, exp_down, shared_gate, shared_up, shared_down,
    )


def solution(mesh):
    fits = mesh.shape["tp"] == 2 and mesh.shape["sp"] == 4 * LINE
    placed = (
        P("sp", "tp"),
        P("sp", "tp"),
        P("sp", "tp"),
        P("sp"),
        P("tp"),
        P("tp", None),
        P(("sp", "tp"), None),
        P(),
        P(("sp", "tp"), None),
        P(("sp", "tp"), None),
        P("sp", None, None),
        P("sp", None, None),
        P("sp", None, None),
        P(None, "tp"),
        P(None, "tp"),
        P("tp", None),
    )
    return jax.shard_map(
        fused_shards if fits else shards, mesh=mesh, in_specs=placed, out_specs=P(("sp", "tp"), None), check_vma=False
    )
```
